256 devices in a mesh: gr: 2 (over z_hi), sp: 16 (over z_lo, y), tp: 8 (over x, core).
Axes of the slice: x: 4, y: 4, z: 8 (z_hi: 2, z_lo: 4; z = z_hi * 4 + z_lo), core: 2. Of those that a mesh axis runs over, the one named last changes fastest.
Arguments:
- prompt: bfloat16 [256, 256, 1024], P('gr', 'sp'), parts along dimension 0, may hold values from -6 to 6
- w_key: bfloat16 [1024, 8, 128], P(None, 'tp'), may hold values from -0.1875 to 0.1875
- w_value: bfloat16 [1024, 8, 128], P(None, 'tp'), may hold values from -0.1875 to 0.1875
- w_in_gate: bfloat16 [2, 1024, 8], P(None, None, 'tp'), may hold values from -0.1875 to 0.1875
- w_forget_gate: bfloat16 [2, 1024, 8], P(None, None, 'tp'), may hold values from -0.1875 to 0.1875
- in_bias: float32 [2, 8], P(None, 'tp'), may hold values from -6 to 0, as said below
- forget_bias: float32 [2, 8], P(None, 'tp'), may hold values from 1 to 10, as said below
- query: bfloat16 [256, 8, 128], P(('gr', 'sp'), 'tp'), parts along dimension 0, may hold values from -6 to 6
- w_out: bfloat16 [8, 128, 1024], P('tp'), may hold values from -0.5 to 0.5
Outputs:
- memory: bfloat16 [2, 256, 8, 128, 128], P(None, ('gr', 'sp'), 'tp'), parts along dimension 1
- normalizer: float32 [2, 256, 8, 128], P(None, ('gr', 'sp'), 'tp'), parts along dimension 1
- stabilizer: float32 [2, 256, 8], P(None, ('gr', 'sp'), 'tp'), parts along dimension 1
- read: bfloat16 [256, 1024], P(('gr', 'sp'), 'tp'), parts along dimension 0
The draws below stay inside these ranges and needn't reach their ends.
There are 2 independent parts, one for each index of `gr`. The reference program is written for one: setup_inputs(seed, part) draws one part's arguments, and reference() takes and returns one part's arrays. A program takes and returns all parts, laid end to end along the dimension named above; an argument that names none is the same for every part. Nothing has to cross between parts.
Inputs may be any that keep to these rules, and one draw needn't show every extreme that they name: forget_bias lies between 1 and 10; the per-head share of memory kept over the whole prompt is spread between a few and some ninety percent. in_bias lies between -6 and 0.
All inputs are finite; a program needn't handle non-finite values.
Results may differ from the reference program's by a relative error of at most 0.015.
Values may be sent and summed in bfloat16 or wider, within the bound.
No kernel may reach another device: no remote copies, remote signals or barrier semaphores. Data moves between devices by JAX's collectives and lax.ppermute only.
A program may use at most 64 MiB of HBM per device.

```python
import math
import jax
import jax.numpy as jnp
from jax import lax

D = 1024
HEADS = 8
HEAD_DIM = 128
SEQS = 128
SEQ_LEN = 256


def draw_forget_bias(key, part):
    kept_share = jnp.exp(jax.random.uniform(key, (2, HEADS), jnp.float32, math.log(0.05), math.log(0.9)))
    chain_loss = -jnp.log(kept_share) / 1.65
    return -jnp.log(jnp.expm1(chain_loss / SEQ_LEN))


def draw_in_bias(key, part):
    centre = -0.5 * math.log(SEQ_LEN) - 1.0
    offset = jax.random.uniform(key, (2, HEADS), jnp.float32, -1.0, 1.0)
    return offset + centre


def block_scale(stream_key, dims, shards, smallest, high):
    loudness, own = 1.0, jax.random.fold_in(stream_key, 6)
    for position, shards_of in shards:
        steps = jnp.exp(jax.random.uniform(jax.random.fold_in(own, position), (shards_of,), jnp.float32, smallest / len(shards), high / len(shards)))
        loudness = loudness * jnp.repeat(steps, dims[position] // shards_of).reshape([-1 if axis == position else 1 for axis in range(len(dims))])
    return loudness


def gaussian(key, extent, scale, reach, pieces=(), kind=jnp.bfloat16):
    loudness = block_scale(key, extent, pieces, -0.22, 0.18) if pieces else 1.0
    array = jax.random.normal(key, extent, jnp.float32) * scale * loudness
    return jnp.minimum(jnp.maximum(array, -reach), reach).astype(kind)


def setup_inputs(seed: int = 0, part: int = 0) -> dict:
    keys = jax.random.split(jax.random.key(seed), 10)
    part_keys = jax.random.split(jax.random.fold_in(keys[9], part), 10)
    prompt = gaussian(part_keys[0], (SEQS, SEQ_LEN, D), 1.0, 6.0, ((1, 16),))
    w_key = gaussian(keys[1], (D, HEADS, HEAD_DIM), D ** -0.5, 0.1875, ((1, 8),))
    w_value = gaussian(keys[2], (D, HEADS, HEAD_DIM), D ** -0.5, 0.1875, ((1, 8),))
    w_in_gate = gaussian(keys[3], (2, D, HEADS), D ** -0.5, 0.1875, ((2, 8),))
    w_forget_gate = gaussian(keys[4], (2, D, HEADS), D ** -0.5, 0.1875, ((2, 8),))
    in_bias = draw_in_bias(jax.random.fold_in(keys[9], 71), part)
    forget_bias = draw_forget_bias(jax.random.fold_in(keys[9], 71), part)
    query = gaussian(part_keys[7], (SEQS, HEADS, HEAD_DIM), 1.0, 6.0, ((0, 16), (1, 8)))
    w_out = gaussian(keys[8], (HEADS, HEAD_DIM, D), (HEADS * HEAD_DIM // 9) ** -0.5, 0.5, ((0, 8),))
    return dict(prompt=prompt, w_key=w_key, w_value=w_value, w_in_gate=w_in_gate, w_forget_gate=w_forget_gate, in_bias=in_bias, forget_bias=forget_bias, query=query, w_out=w_out)


highest = lax.Precision.HIGHEST


def summary(scaled, float_values, in_log, forget_log, backward):
    total_forget = jnp.sum(forget_log, axis=1)
    running = jnp.cumsum(forget_log, axis=1)
    if backward:
        log_weight = in_log + running - forget_log
    else:
        log_weight = in_log + total_forget[:, None, :] - running
    stable = jnp.maximum(total_forget, jnp.max(log_weight, axis=1))
    weight = jnp.exp(log_weight - stable[:, None, :])
    weighted = scaled * weight[..., None]
    memory = jnp.einsum('bshd,bshe->bhde', weighted, float_values, precision=highest)
    normal = jnp.sum(weighted, axis=1)
    return memory, normal, stable


def read_out(memory_bf, normal, stable, query_f):
    cells = memory_bf.astype(jnp.float32)
    numerator = jnp.sum(query_f[..., :, None] * cells, axis=-2)
    denominator = jnp.sum(query_f * normal, axis=-1)
    floor_value = jnp.maximum(jnp.maximum(jnp.abs(denominator), jnp.exp(-stable)), 1.0)
    return numerator / floor_value[..., None]


def reference(prompt, w_key, w_value, w_in_gate, w_forget_gate, in_bias, forget_bias, query, w_out):
    token_rows = prompt.astype(jnp.float32)
    key_rows = jnp.einsum('bsd,dhe->bshe', token_rows, w_key.astype(jnp.float32), precision=highest).astype(jnp.bfloat16)
    value_rows = jnp.einsum('bsd,dhe->bshe', token_rows, w_value.astype(jnp.float32), precision=highest).astype(jnp.bfloat16)
    in_pre = jnp.einsum('bsd,gdh->bsgh', token_rows, w_in_gate.astype(jnp.float32), precision=highest) + in_bias
    forget_pre = jnp.einsum('bsd,gdh->bsgh', token_rows, w_forget_gate.astype(jnp.float32), precision=highest) + forget_bias
    scaled = key_rows.astype(jnp.float32) * (key_rows.shape[-1] ** -0.5)
    float_values = value_rows.astype(jnp.float32)
    query_f = query.astype(jnp.float32)
    memories = []
    normals = []
    stables = []
    reads = []
    for course in range(2):
        memory, normal, stable = summary(scaled, float_values, in_pre[:, :, course, :],
                                         jax.nn.log_sigmoid(forget_pre[:, :, course, :]), course == 1)
        memory_bf = memory.astype(jnp.bfloat16)
        memories.append(memory_bf)
        normals.append(normal)
        stables.append(stable)
        reads.append(read_out(memory_bf, normal, stable, query_f))
    hidden = (reads[0] + reads[1]).astype(jnp.bfloat16)
    read = jnp.einsum('bhd,hde->be', hidden.astype(jnp.float32), w_out.astype(jnp.float32), precision=highest).astype(jnp.bfloat16)
    return (jnp.stack(memories), jnp.stack(normals), jnp.stack(stables), read)
```

```python
import jax
import jax.numpy as jnp
from jax import lax
from jax.experimental import pallas as pl
from jax.experimental.pallas import tpu as pltpu
from jax.sharding import Mesh
from jax.sharding import PartitionSpec as P

TP = ("tp_0", "tp_1")
BF = jnp.bfloat16
F32 = jnp.float32
SP = 16
TPN = 8
OWN = 8
POS = 16
ROWS = OWN * POS
HD = 128
D = 1024
SEND = 2 * ROWS + 8


def dot(a, b, dims=((1,), (0,))):
    return lax.dot_general(a, b, (dims, ((), ())), preferred_element_type=F32)


def project_kernel(x_ref, wk_ref, wv_ref, wi_ref, wf_ref, out_ref, w_ref, g_ref):
    @pl.when(pl.program_id(0) == 0)
    def _():
        w_ref[:, :HD] = wk_ref[...]
        w_ref[:, HD:] = wv_ref[...]
        gates = jnp.concatenate((wi_ref[...].astype(F32), wf_ref[...].astype(F32), jnp.zeros((4, D), F32)), axis=0)
        g_ref[...] = gates.astype(BF)

    for k in range(out_ref.shape[0]):
        rows = x_ref[k * OWN : (k + 1) * OWN].reshape(ROWS, D)
        both = dot(rows, w_ref[...]).astype(BF)
        out_ref[k, :ROWS, :] = both[:, :HD]
        out_ref[k, ROWS : 2 * ROWS, :] = both[:, HD:]
        pre = dot(g_ref[...], rows, ((1,), (1,)))[:4]
        high = pre.astype(BF).astype(F32)
        out_ref[k, 2 * ROWS :, :] = jnp.concatenate((high, pre - high), axis=0).astype(BF)


def project(prompt, w_key, w_value, w_in, w_forget, blocks=4):
    whole = lambda a: pl.BlockSpec(a.shape, lambda i: (0,) * a.ndim)
    return pl.pallas_call(
        project_kernel,
        grid=(SP // blocks,),
        in_specs=[
            pl.BlockSpec((blocks * OWN, POS, D), lambda i: (i, 0, 0)),
            whole(w_key), whole(w_value), whole(w_in), whole(w_forget),
        ],
        out_specs=pl.BlockSpec((blocks, SEND, HD), lambda i: (i, 0, 0)),
        out_shape=jax.ShapeDtypeStruct((SP, SEND, HD), BF),
        scratch_shapes=[pltpu.VMEM((D, 2 * HD), BF), pltpu.VMEM((8, D), BF)],
        name="project",
    )(prompt, w_key, w_value, w_in, w_forget)


def three_parts(a):
    first = a.astype(BF)
    rest = a - first.astype(F32)
    second = rest.astype(BF)
    return first, second, (rest - second.astype(F32)).astype(BF)


def group_max(a, lane):
    for k in (1, 2, 4, 8):
        inside = (lane % POS) + k < POS
        a = jnp.maximum(a, jnp.where(inside, pltpu.roll(a, HD - k, 1), pltpu.roll(a, POS - k, 1)))
    return a


def log_sigmoid(a):
    return jnp.minimum(a, 0.0) - jnp.log1p(jnp.exp(-jnp.abs(a)))


def memory_kernel(recv_ref, q_ref, wo_ref, ib_ref, fb_ref, mem_ref, norm_ref, stab_ref, term_ref, vw_ref):
    scale = HD ** -0.5
    gates = recv_ref[:, 2 * ROWS :, :].astype(F32)
    part = lambda c: gates[:, c, :] + gates[:, c + 4, :]
    in_pre = [part(g) + ib_ref[0:1, g : g + 1] for g in range(2)]
    forget = [log_sigmoid(part(2 + g) + fb_ref[0:1, g : g + 1]) for g in range(2)]

    r = lax.broadcasted_iota(jnp.int32, (HD, HD), 0)
    c = lax.broadcasted_iota(jnp.int32, (HD, HD), 1)
    same = (r // POS) == (c // POS)
    ones = lambda m: jnp.where(m, 1.0, 0.0).astype(BF)
    jr = lax.broadcasted_iota(jnp.int32, (2 * SP, SP), 0)
    jc = lax.broadcasted_iota(jnp.int32, (2 * SP, SP), 1)
    lane = lax.broadcasted_iota(jnp.int32, (1, HD), 1)
    log_weight = []
    total = []
    for g in range(2):
        order = (r > c) if g == 0 else (r < c)
        inside = jnp.concatenate((ones(same & order), ones(same)), axis=1)
        sums = sum(dot(p, inside) for p in three_parts(forget[g]))
        block = sums[:, HD:]
        across = ones(((jc > jr) if g == 0 else (jc < jr)) | (jr >= SP))
        outside = sum(dot(across, p) for p in three_parts(block))
        log_weight.append(in_pre[g] + sums[:, :HD] + outside[:SP])
        total.append(outside[SP : SP + 1])
    stab = [
        jnp.maximum(total[g], group_max(jnp.max(log_weight[g], axis=0, keepdims=True), lane)) for g in range(2)
    ]
    weight = [jnp.exp(log_weight[g] - stab[g]) for g in range(2)]

    row8 = lax.broadcasted_iota(jnp.int32, (OWN, HD), 0)
    lane8 = lax.broadcasted_iota(jnp.int32, (OWN, HD), 1)
    mine = (lane8 // POS) == row8
    norm = jnp.zeros((4 * OWN, HD), F32)
    for j in range(SP):
        spread = jnp.concatenate([jnp.where(mine, weight[g][j : j + 1], 0.0) for g in range(2)], axis=0)
        high = spread.astype(BF)
        low = (spread - high.astype(F32)).astype(BF)
        norm += dot(jnp.concatenate((high, low), axis=0), recv_ref[j, :ROWS, :])
    norm = (norm[: 2 * OWN] + norm[2 * OWN :]) * scale
    norm_ref[...] = norm

    turned = jnp.concatenate(weight, axis=0).T
    for j in range(SP):
        value = recv_ref[j, ROWS : 2 * ROWS, :].astype(F32)
        for g in range(2):
            k = g * SP + j
            vw_ref[j, :, g * HD : (g + 1) * HD] = (value * turned[:, k : k + 1]).astype(BF)

    query = q_ref[...]
    row16 = lax.broadcasted_iota(jnp.int32, (OWN, 2 * HD), 0)
    numerator = jnp.zeros((OWN, 2 * HD), F32)
    for s in range(OWN):
        at = slice(s * POS, (s + 1) * POS)
        keys = recv_ref[:, at, :].reshape(SP * POS, HD)
        values = vw_ref[:, at, :].reshape(SP * POS, 2 * HD)
        memory = (dot(keys, values, ((0,), (0,))) * scale).astype(BF)
        mem_ref[0, s] = memory[:, :HD]
        mem_ref[1, s] = memory[:, HD:]
        numerator = jnp.where(row16 == s, dot(query, memory), numerator)

    query_f = query.astype(F32)
    hidden = jnp.zeros((OWN, HD), F32)
    for g in range(2):
        column = jnp.max(jnp.where(mine, stab[g], -jnp.inf), axis=1, keepdims=True)
        stab_ref[g] = jnp.sum(jnp.where(lane8 == row8, column, 0.0), axis=0, keepdims=True)[:, :OWN]
        denominator = jnp.sum(query_f * norm[g * OWN : (g + 1) * OWN], axis=1, keepdims=True)
        floor = jnp.maximum(jnp.maximum(jnp.abs(denominator), jnp.exp(-column)), 1.0)
        hidden += numerator[:, g * HD : (g + 1) * HD] / floor
    hidden = hidden.astype(BF)
    for t in range(TPN):
        term_ref[t] = dot(hidden, wo_ref[:, t * HD : (t + 1) * HD])


def memories(recv, query, w_out, in_bias, forget_bias):
    return pl.pallas_call(
        memory_kernel,
        out_shape=(
            jax.ShapeDtypeStruct((2, OWN, HD, HD), BF),
            jax.ShapeDtypeStruct((2 * OWN, HD), F32),
            jax.ShapeDtypeStruct((2, 1, OWN), F32),
            jax.ShapeDtypeStruct((TPN, OWN, HD), F32),
        ),
        scratch_shapes=[pltpu.VMEM((SP, ROWS, 2 * HD), BF)],
        name="memories",
    )(recv, query, w_out, in_bias, forget_bias)


def shards(prompt, w_key, w_value, w_in_gate, w_forget_gate, in_bias, forget_bias, query, w_out):
    send = project(
        prompt, w_key.reshape(D, HD), w_value.reshape(D, HD), w_in_gate.reshape(2, D), w_forget_gate.reshape(2, D)
    )
    recv = lax.all_to_all(send, "sp", 0, 0, tiled=True)
    memory, norm, stab, terms = memories(
        recv, query.reshape(OWN, HD), w_out.reshape(HD, D), in_bias.reshape(1, 2), forget_bias.reshape(1, 2)
    )
    terms = lax.all_to_all(terms, TP, 0, 0, tiled=True)
    read = jnp.sum(terms, axis=0).astype(BF)
    return (
        memory.reshape(2, OWN, 1, HD, HD),
        norm.reshape(2, OWN, 1, HD),
        stab.reshape(2, OWN, 1),
        read,
    )


def solution(mesh):
    torus = Mesh(
        mesh.devices.reshape(mesh.shape["gr"], mesh.shape["sp"], 4, 2), ("gr", "sp", "tp_0", "tp_1")
    )
    return jax.shard_map(
        shards,
        mesh=torus,
        in_specs=(
            P("gr", "sp", None),
            P(None, TP, None),
            P(None, TP, None),
            P(None, None, TP),
            P(None, None, TP),
            P(None, TP),
            P(None, TP),
            P(("gr", "sp"), TP, None),
            P(TP, None, None),
        ),
        out_specs=(
            P(None, ("gr", "sp"), TP, None, None),
            P(None, ("gr", "sp"), TP, None),
            P(None, ("gr", "sp"), TP),
            P(("gr", "sp"), TP),
        ),
        check_vma=False,
    )
```

```python
import jax
import jax.numpy as jnp
from jax import lax
from jax.experimental import pallas as pl
from jax.experimental.pallas import tpu as pltpu
from jax.sharding import Mesh
from jax.sharding import PartitionSpec as P


TP = ("tp_0", "tp_1")
BF = jnp.bfloat16
F32 = jnp.float32
SP = 16
TPN = 8
OWN = 8
POS = 16
ROWS = OWN * POS
HD = 128
D = 1024
SEND = 2 * ROWS + 8
ROW = 4


def dot(a, b, dims=((1,), (0,))):
    return lax.dot_general(a, b, (dims, ((), ())), preferred_element_type=F32)


def here():
    at = lax.axis_index("sp")
    return at // ROW, at % ROW


def take(x_ref, buf_ref, sem_ref, blocks):
    z, y = here()
    copies = []
    for i, (dz, dy) in enumerate(blocks):
        dest = ((z + dz) % ROW) * ROW + (y + dy) % ROW
        copies.append(pltpu.make_async_copy(x_ref.at[pl.ds(dest * OWN, OWN)], buf_ref.at[i], sem_ref.at[i]))
    for copy in copies:
        copy.start()
    return copies


def project_blocks(buf_ref, first, w, gates, outs):
    rows = buf_ref[first : first + ROW].reshape(ROW * ROWS, D)
    both = dot(rows, w).astype(BF)
    pre = dot(gates, rows, ((1,), (1,)))[:4]
    high = pre.astype(BF).astype(F32)
    coded = jnp.concatenate((high, pre - high), axis=0).astype(BF)
    for k, out in enumerate(outs):
        at = slice(k * ROWS, (k + 1) * ROWS)
        out[:ROWS, :] = both[at, :HD]
        out[ROWS : 2 * ROWS, :] = both[at, HD:]
        out[2 * ROWS :, :] = coded[:, at]


def near_kernel(x_ref, wk_ref, wv_ref, wi_ref, wf_ref, up_ref, down_ref, w_ref, g_ref, buf_ref, sem_ref):
    copies = take(x_ref, buf_ref, sem_ref, [(dz, dy) for dz in (1, 3) for dy in range(ROW)])
    w_ref[:, :HD] = wk_ref[...]
    w_ref[:, HD:] = wv_ref[...]
    gates = jnp.concatenate((wi_ref[...].astype(F32), wf_ref[...].astype(F32), jnp.zeros((4, D), F32)), axis=0)
    g_ref[...] = gates.astype(BF)
    for half, out_ref in enumerate((up_ref, down_ref)):
        for copy in copies[half * ROW : (half + 1) * ROW]:
            copy.wait()
        project_blocks(buf_ref, half * ROW, w_ref[...], g_ref[...], [out_ref.at[k] for k in range(ROW)])


def far_kernel(x_ref, w_ref, g_ref, *refs):
    outs, (buf_ref, sem_ref) = refs[:ROW], refs[ROW:]
    for copy in take(x_ref, buf_ref, sem_ref, [(2, dy) for dy in range(ROW)]):
        copy.wait()
    project_blocks(buf_ref, 0, w_ref[...], g_ref[...], outs)


def own_kernel(x_ref, w_ref, g_ref, out_ref, buf_ref, sem_ref):
    for copy in take(x_ref, buf_ref, sem_ref, [(0, dy) for dy in range(ROW)]):
        copy.wait()
    project_blocks(buf_ref, 0, w_ref[...], g_ref[...], [out_ref.at[k] for k in range(ROW)])


ANY = pl.BlockSpec(memory_space=pl.ANY)
VM = pl.BlockSpec(memory_space=pltpu.VMEM)


def scratch(blocks):
    return [pltpu.VMEM((blocks, OWN, POS, D), BF), pltpu.SemaphoreType.DMA((blocks,))]


def block(*lead):
    return jax.ShapeDtypeStruct((*lead, SEND, HD), BF)


def project_near(*args):
    return pl.pallas_call(
        near_kernel,
        in_specs=[ANY, VM, VM, VM, VM],
        out_shape=(block(ROW), block(ROW), jax.ShapeDtypeStruct((D, 2 * HD), BF), jax.ShapeDtypeStruct((8, D), BF)),
        scratch_shapes=scratch(2 * ROW),
        name="near",
    )(*args)


def project_far(*args):
    return pl.pallas_call(
        far_kernel, in_specs=[ANY, VM, VM], out_shape=(block(),) * ROW, scratch_shapes=scratch(ROW), name="far"
    )(*args)


def project_own(*args):
    return pl.pallas_call(
        own_kernel, in_specs=[ANY, VM, VM], out_shape=block(ROW), scratch_shapes=scratch(ROW), name="own"
    )(*args)


def stack_kernel(a_ref, b_ref, c_ref, *outs):
    for k, out in enumerate(outs):
        for i, ref in enumerate((a_ref, b_ref, c_ref)):
            out[i] = ref[k + 1]


def stack(*args):
    return pl.pallas_call(stack_kernel, out_shape=(block(3),) * 3, name="stack")(*args)


def three_parts(a):
    first = a.astype(BF)
    rest = a - first.astype(F32)
    second = rest.astype(BF)
    return first, second, (rest - second.astype(F32)).astype(BF)


def group_max(a, lane):
    for k in (1, 2, 4, 8):
        inside = (lane % POS) + k < POS
        a = jnp.maximum(a, jnp.where(inside, pltpu.roll(a, HD - k, 1), pltpu.roll(a, POS - k, 1)))
    return a


def log_sigmoid(a):
    return jnp.minimum(a, 0.0) - jnp.log1p(jnp.exp(-jnp.abs(a)))


def memory_kernel(own_ref, up_ref, down_ref, y1_ref, y2_ref, y3_ref, f0_ref, f1_ref, f2_ref, f3_ref,
                  q_ref, wo_ref, ib_ref, fb_ref, mem_ref, norm_ref, stab_ref, term_ref, vw_ref, recv_ref):
    for i, (dz, ref) in enumerate(((0, own_ref), (1, up_ref), (3, down_ref))):
        recv_ref[dz * ROW] = ref[0]
        for dy, far_ref in ((1, y1_ref), (2, y2_ref), (3, y3_ref)):
            recv_ref[dz * ROW + dy] = far_ref[i]
    for dy, ref in enumerate((f0_ref, f1_ref, f2_ref, f3_ref)):
        recv_ref[2 * ROW + dy] = ref[...]
    z, y = here()
    place = lambda j: ((z - j // ROW) & 3) * ROW + ((y - j % ROW) & 3)
    scale = HD ** -0.5
    gates = recv_ref[:, 2 * ROWS :, :].astype(F32)
    part = lambda c: gates[:, c, :] + gates[:, c + 4, :]
    in_pre = [part(g) + ib_ref[0:1, g : g + 1] for g in range(2)]
    forget = [log_sigmoid(part(2 + g) + fb_ref[0:1, g : g + 1]) for g in range(2)]

    r = lax.broadcasted_iota(jnp.int32, (HD, HD), 0)
    c = lax.broadcasted_iota(jnp.int32, (HD, HD), 1)
    same = (r // POS) == (c // POS)
    ones = lambda m: jnp.where(m, 1.0, 0.0).astype(BF)
    jr = lax.broadcasted_iota(jnp.int32, (2 * SP, SP), 0)
    jc = lax.broadcasted_iota(jnp.int32, (2 * SP, SP), 1)
    lane = lax.broadcasted_iota(jnp.int32, (1, HD), 1)
    log_weight = []
    total = []
    for g in range(2):
        order = (r > c) if g == 0 else (r < c)
        inside = jnp.concatenate((ones(same & order), ones(same)), axis=1)
        sums = sum(dot(p, inside) for p in three_parts(forget[g]))
        block = sums[:, HD:]
        across = ones(((place(jc) > place(jr)) if g == 0 else (place(jc) < place(jr))) | (jr >= SP))
        outside = sum(dot(across, p) for p in three_parts(block))
        log_weight.append(in_pre[g] + sums[:, :HD] + outside[:SP])
        total.append(outside[SP : SP + 1])
    stab = [
        jnp.maximum(total[g], group_max(jnp.max(log_weight[g], axis=0, keepdims=True), lane)) for g in range(2)
    ]
    weight = [jnp.exp(log_weight[g] - stab[g]) for g in range(2)]

    row8 = lax.broadcasted_iota(jnp.int32, (OWN, HD), 0)
    lane8 = lax.broadcasted_iota(jnp.int32, (OWN, HD), 1)
    mine = (lane8 // POS) == row8
    norm = jnp.zeros((4 * OWN, HD), F32)
    for j in range(SP):
        spread = jnp.concatenate([jnp.where(mine, weight[g][j : j + 1], 0.0) for g in range(2)], axis=0)
        high = spread.astype(BF)
        low = (spread - high.astype(F32)).astype(BF)
        norm += dot(jnp.concatenate((high, low), axis=0), recv_ref[j, :ROWS, :])
    norm = (norm[: 2 * OWN] + norm[2 * OWN :]) * scale
    norm_ref[...] = norm

    turned = jnp.concatenate(weight, axis=0).T
    for j in range(SP):
        value = recv_ref[j, ROWS : 2 * ROWS, :].astype(F32)
        for g in range(2):
            k = g * SP + j
            vw_ref[j, :, g * HD : (g + 1) * HD] = (value * turned[:, k : k + 1]).astype(BF)

    query = q_ref[...]
    row16 = lax.broadcasted_iota(jnp.int32, (OWN, 2 * HD), 0)
    numerator = jnp.zeros((OWN, 2 * HD), F32)
    for s in range(OWN):
        at = slice(s * POS, (s + 1) * POS)
        keys = recv_ref[:, at, :].reshape(SP * POS, HD)
        values = vw_ref[:, at, :].reshape(SP * POS, 2 * HD)
        memory = (dot(keys, values, ((0,), (0,))) * scale).astype(BF)
        mem_ref[0, s] = memory[:, :HD]
        mem_ref[1, s] = memory[:, HD:]
        numerator = jnp.where(row16 == s, dot(query, memory), numerator)

    query_f = query.astype(F32)
    hidden = jnp.zeros((OWN, HD), F32)
    for g in range(2):
        column = jnp.max(jnp.where(mine, stab[g], -jnp.inf), axis=1, keepdims=True)
        stab_ref[g] = jnp.sum(jnp.where(lane8 == row8, column, 0.0), axis=0, keepdims=True)[:, :OWN]
        denominator = jnp.sum(query_f * norm[g * OWN : (g + 1) * OWN], axis=1, keepdims=True)
        floor = jnp.maximum(jnp.maximum(jnp.abs(denominator), jnp.exp(-column)), 1.0)
        hidden += numerator[:, g * HD : (g + 1) * HD] / floor
    hidden = hidden.astype(BF)
    for t in range(TPN):
        term_ref[t] = dot(hidden, wo_ref[:, t * HD : (t + 1) * HD])


def memories(own, up, down, *rest):
    first = pl.BlockSpec((1, SEND, HD), lambda i: (0, 0, 0))
    return pl.pallas_call(
        memory_kernel,
        grid=(1,),
        in_specs=[first] * 3 + [VM] * len(rest),
        out_shape=(
            jax.ShapeDtypeStruct((2, OWN, HD, HD), BF),
            jax.ShapeDtypeStruct((2 * OWN, HD), F32),
            jax.ShapeDtypeStruct((2, 1, OWN), F32),
            jax.ShapeDtypeStruct((TPN, OWN, HD), F32),
        ),
        scratch_shapes=[pltpu.VMEM((SP, ROWS, 2 * HD), BF), pltpu.VMEM((SP, SEND, HD), BF)],
        name="memories",
    )(own, up, down, *rest)


def shift(array, dz, dy):
    spots = [(z, y) for z in range(ROW) for y in range(ROW)]
    pairs = [(z * ROW + y, ((z + dz) % ROW) * ROW + (y + dy) % ROW) for z, y in spots]
    return lax.ppermute(array, "sp", pairs)


def step(prompt, w_key, w_value, w_in_gate, w_forget_gate, in_bias, forget_bias, query, w_out):
    up, down, w, gates = project_near(
        prompt, w_key.reshape(D, HD), w_value.reshape(D, HD), w_in_gate.reshape(2, D), w_forget_gate.reshape(2, D)
    )
    up = shift(up, 1, 0)
    down = shift(down, 3, 0)
    far = project_far(prompt, w, gates)
    far = [shift(block, 2, dy) for dy, block in enumerate(far)]
    own = project_own(prompt, w, gates)
    aside = stack(own, up, down)
    aside = [shift(blocks, 0, dy + 1) for dy, blocks in enumerate(aside)]
    memory, norm, stab, terms = memories(
        own, up, down, *aside, *far,
        query.reshape(OWN, HD), w_out.reshape(HD, D), in_bias.reshape(1, 2), forget_bias.reshape(1, 2),
    )
    terms = lax.all_to_all(terms, TP, 0, 0, tiled=True)
    read = jnp.sum(terms, axis=0).astype(BF)
    return (
        memory.reshape(2, OWN, 1, HD, HD),
        norm.reshape(2, OWN, 1, HD),
        stab.reshape(2, OWN, 1),
        read,
    )


def solution(mesh):
    torus = Mesh(
        mesh.devices.reshape(mesh.shape["gr"], mesh.shape["sp"], 4, 2), ("gr", "sp", "tp_0", "tp_1")
    )
    return jax.shard_map(
        step,
        mesh=torus,
        in_specs=(
            P("gr", "sp", None),
            P(None, TP, None),
            P(None, TP, None),
            P(None, None, TP),
            P(None, None, TP),
            P(None, TP),
            P(None, TP),
            P(("gr", "sp"), TP, None),
            P(TP, None, None),
        ),
        out_specs=(
            P(None, ("gr", "sp"), TP, None, None),
            P(None, ("gr", "sp"), TP, None),
            P(None, ("gr", "sp"), TP),
            P(("gr", "sp"), TP),
        ),
        check_vma=False,
    )
```

```python
import jax
import jax.numpy as jnp
from jax import lax
from jax.experimental import pallas as pl
from jax.experimental.pallas import tpu as pltpu
from jax.sharding import Mesh
from jax.sharding import PartitionSpec as P


TP = ("tp_0", "tp_1")
BF = jnp.bfloat16
F32 = jnp.float32
SP = 16
TPN = 8
OWN = 8
POS = 16
ROWS = OWN * POS
HD = 128
D = 1024
SEND = 2 * ROWS + 8
ROW = 4


def dot(a, b, dims=((1,), (0,))):
    return lax.dot_general(a, b, (dims, ((), ())), preferred_element_type=F32)


def here():
    at = lax.axis_index("sp")
    return at // ROW, at % ROW


def take(x_ref, buf_ref, sem_ref, sem, blocks):
    z, y = here()
    copies = []
    for i, (dz, dy) in enumerate(blocks):
        dest = ((z + dz) % ROW) * ROW + (y + dy) % ROW
        copies.append(pltpu.make_async_copy(x_ref.at[pl.ds(dest * OWN, OWN)], buf_ref.at[i], sem_ref.at[sem + i]))
    for copy in copies:
        copy.start()
    return copies


def project_blocks(buf_ref, first, w, gates, outs):
    rows = buf_ref[first : first + ROW].reshape(ROW * ROWS, D)
    both = dot(rows, w).astype(BF)
    pre = dot(gates, rows, ((1,), (1,)))[:4]
    high = pre.astype(BF).astype(F32)
    coded = jnp.concatenate((high, pre - high), axis=0).astype(BF)
    for k, out in enumerate(outs):
        at = slice(k * ROWS, (k + 1) * ROWS)
        out[:ROWS, :] = both[at, :HD]
        out[ROWS : 2 * ROWS, :] = both[at, HD:]
        out[2 * ROWS :, :] = coded[:, at]


def near_kernel(x_ref, wk_ref, wv_ref, wi_ref, wf_ref, up_ref, down_ref, w_ref, g_ref, rest_ref, buf_ref, wi_buf, wf_buf, sem_ref):
    key_copy = pltpu.make_async_copy(wk_ref, w_ref.at[:, :HD], sem_ref.at[SP])
    value_copy = pltpu.make_async_copy(wv_ref, w_ref.at[:, HD:], sem_ref.at[SP + 1])
    gate_copies = [
        pltpu.make_async_copy(wi_ref, wi_buf, sem_ref.at[SP + 2]),
        pltpu.make_async_copy(wf_ref, wf_buf, sem_ref.at[SP + 3]),
    ]
    for copy in (*gate_copies, key_copy, value_copy):
        copy.start()
    copies = take(x_ref, buf_ref, sem_ref, 0, [(dz, dy) for dz in (1, 3) for dy in range(ROW)])
    later = take(x_ref, rest_ref, sem_ref, 2 * ROW, [(dz, dy) for dz in (2, 0) for dy in range(ROW)])
    for copy in gate_copies:
        copy.wait()
    gates = jnp.concatenate((wi_buf[...].astype(F32), wf_buf[...].astype(F32), jnp.zeros((4, D), F32)), axis=0)
    g_ref[...] = gates.astype(BF)
    key_copy.wait()
    value_copy.wait()
    for half, out_ref in enumerate((up_ref, down_ref)):
        for copy in copies[half * ROW : (half + 1) * ROW]:
            copy.wait()
        project_blocks(buf_ref, half * ROW, w_ref[...], g_ref[...], [out_ref.at[k] for k in range(ROW)])
    for copy in later:
        copy.wait()


def rest_kernel(rest_ref, w_ref, g_ref, *outs):
    for half in range(2):
        project_blocks(rest_ref, half * ROW, w_ref[...], g_ref[...], outs[half * ROW : (half + 1) * ROW])


ANY = pl.BlockSpec(memory_space=pl.ANY)
VM = pl.BlockSpec(memory_space=pltpu.VMEM)


def vm(array):
    return pltpu.with_memory_space_constraint(array, pltpu.VMEM)


def grant(mib):
    return pltpu.CompilerParams(vmem_limit_bytes=mib << 20)


def block(*lead):
    return pltpu.VMEM((*lead, SEND, HD), BF)


def project_near(*args):
    return pl.pallas_call(
        near_kernel,
        in_specs=[ANY] * 5,
        out_specs=[VM] * 5,
        out_shape=(
            block(ROW), block(ROW), pltpu.VMEM((D, 2 * HD), BF), pltpu.VMEM((8, D), BF),
            pltpu.VMEM((2 * ROW, OWN, POS, D), BF),
        ),
        scratch_shapes=[
            pltpu.VMEM((2 * ROW, OWN, POS, D), BF), pltpu.VMEM((2, D), BF), pltpu.VMEM((2, D), BF),
            pltpu.SemaphoreType.DMA((SP + 4,)),
        ],
        compiler_params=grant(16),
        name="near",
    )(*[pltpu.with_memory_space_constraint(a, pltpu.HBM) for a in args])


def project_rest(*args):
    return pl.pallas_call(
        rest_kernel, in_specs=[VM] * 3, out_specs=[VM] * 8, out_shape=(block(),) * 8, compiler_params=grant(16), name="rest"
    )(*[vm(a) for a in args])


def gather_kernel(*refs):
    for i in range(ROW):
        refs[ROW][i] = refs[i][...]


def gather(*args):
    return pl.pallas_call(
        gather_kernel, in_specs=[VM] * ROW, out_specs=VM, out_shape=block(ROW), compiler_params=grant(4), name="gather"
    )(*[vm(a) for a in args])


def pair_kernel(a_ref, b_ref, *outs):
    for k, out in enumerate(outs):
        out[0] = a_ref[k + 1]
        out[1] = b_ref[k + 1]


def pair(*args):
    return pl.pallas_call(
        pair_kernel, in_specs=[VM] * 2, out_specs=[VM] * 3, out_shape=(block(2),) * 3, compiler_params=grant(4), name="pair"
    )(*[vm(a) for a in args])


def three_parts(a):
    first = a.astype(BF)
    rest = a - first.astype(F32)
    second = rest.astype(BF)
    return first, second, (rest - second.astype(F32)).astype(BF)


def group_max(a, lane):
    for k in (1, 2, 4, 8):
        inside = (lane % POS) + k < POS
        a = jnp.maximum(a, jnp.where(inside, pltpu.roll(a, HD - k, 1), pltpu.roll(a, POS - k, 1)))
    return a


def log_sigmoid(a):
    return jnp.minimum(a, 0.0) - jnp.log1p(jnp.exp(-jnp.abs(a)))


def memory_kernel(
    o0_ref, o1_ref, o2_ref, o3_ref, up_ref, down_ref, y1_ref, y2_ref, y3_ref, far_ref,
    q_ref, wo_ref, ib_ref, fb_ref, mem_ref, norm_ref, stab_ref, term_ref, vw_ref, recv_ref,
):
    for dy, ref in enumerate((o0_ref, o1_ref, o2_ref, o3_ref)):
        recv_ref[dy] = ref[...]
        recv_ref[2 * ROW + dy] = far_ref[dy]
    for i, (dz, ref) in enumerate(((1, up_ref), (3, down_ref))):
        recv_ref[dz * ROW] = ref[0]
        for dy, side_ref in ((1, y1_ref), (2, y2_ref), (3, y3_ref)):
            recv_ref[dz * ROW + dy] = side_ref[i]
    z, y = here()
    place = lambda j: ((z - j // ROW) & 3) * ROW + ((y - j % ROW) & 3)
    scale = HD ** -0.5
    gates = recv_ref[:, 2 * ROWS :, :].astype(F32)
    part = lambda c: gates[:, c, :] + gates[:, c + 4, :]
    in_pre = [part(g) + ib_ref[0:1, g : g + 1] for g in range(2)]
    forget = [log_sigmoid(part(2 + g) + fb_ref[0:1, g : g + 1]) for g in range(2)]

    r = lax.broadcasted_iota(jnp.int32, (HD, HD), 0)
    c = lax.broadcasted_iota(jnp.int32, (HD, HD), 1)
    same = (r // POS) == (c // POS)
    ones = lambda m: jnp.where(m, 1.0, 0.0).astype(BF)
    jr = lax.broadcasted_iota(jnp.int32, (2 * SP, SP), 0)
    jc = lax.broadcasted_iota(jnp.int32, (2 * SP, SP), 1)
    lane = lax.broadcasted_iota(jnp.int32, (1, HD), 1)
    log_weight = []
    total = []
    for g in range(2):
        order = (r > c) if g == 0 else (r < c)
        inside = jnp.concatenate((ones(same & order), ones(same)), axis=1)
        sums = sum(dot(p, inside) for p in three_parts(forget[g]))
        block = sums[:, HD:]
        across = ones(((place(jc) > place(jr)) if g == 0 else (place(jc) < place(jr))) | (jr >= SP))
        outside = sum(dot(across, p) for p in three_parts(block))
        log_weight.append(in_pre[g] + sums[:, :HD] + outside[:SP])
        total.append(outside[SP : SP + 1])
    stab = [
        jnp.maximum(total[g], group_max(jnp.max(log_weight[g], axis=0, keepdims=True), lane)) for g in range(2)
    ]
    weight = [jnp.exp(log_weight[g] - stab[g]) for g in range(2)]

    row8 = lax.broadcasted_iota(jnp.int32, (OWN, HD), 0)
    lane8 = lax.broadcasted_iota(jnp.int32, (OWN, HD), 1)
    mine = (lane8 // POS) == row8
    norm = jnp.zeros((4 * OWN, HD), F32)
    for j in range(SP):
        spread = jnp.concatenate([jnp.where(mine, weight[g][j : j + 1], 0.0) for g in range(2)], axis=0)
        high = spread.astype(BF)
        low = (spread - high.astype(F32)).astype(BF)
        norm += dot(jnp.concatenate((high, low), axis=0), recv_ref[j, :ROWS, :])
    norm = (norm[: 2 * OWN] + norm[2 * OWN :]) * scale
    norm_ref[...] = norm

    turned = jnp.concatenate(weight, axis=0).T
    for j in range(SP):
        value = recv_ref[j, ROWS : 2 * ROWS, :].astype(F32)
        for g in range(2):
            k = g * SP + j
            vw_ref[j, :, g * HD : (g + 1) * HD] = (value * turned[:, k : k + 1]).astype(BF)

    query = q_ref[...]
    row16 = lax.broadcasted_iota(jnp.int32, (OWN, 2 * HD), 0)
    numerator = jnp.zeros((OWN, 2 * HD), F32)
    for s in range(OWN):
        at = slice(s * POS, (s + 1) * POS)
        keys = recv_ref[:, at, :].reshape(SP * POS, HD)
        values = vw_ref[:, at, :].reshape(SP * POS, 2 * HD)
        memory = (dot(keys, values, ((0,), (0,))) * scale).astype(BF)
        mem_ref[0, s] = memory[:, :HD]
        mem_ref[1, s] = memory[:, HD:]
        numerator = jnp.where(row16 == s, dot(query, memory), numerator)

    query_f = query.astype(F32)
    hidden = jnp.zeros((OWN, HD), F32)
    for g in range(2):
        column = jnp.max(jnp.where(mine, stab[g], -jnp.inf), axis=1, keepdims=True)
        stab_ref[g] = jnp.sum(jnp.where(lane8 == row8, column, 0.0), axis=0, keepdims=True)[:, :OWN]
        denominator = jnp.sum(query_f * norm[g * OWN : (g + 1) * OWN], axis=1, keepdims=True)
        floor = jnp.maximum(jnp.maximum(jnp.abs(denominator), jnp.exp(-column)), 1.0)
        hidden += numerator[:, g * HD : (g + 1) * HD] / floor
    hidden = hidden.astype(BF)
    for t in range(TPN):
        term_ref[t] = dot(hidden, wo_ref[:, t * HD : (t + 1) * HD])


def memories(blocks, rest):
    return pl.pallas_call(
        memory_kernel,
        in_specs=[VM] * (len(blocks) + len(rest)),
        out_shape=(
            jax.ShapeDtypeStruct((2, OWN, HD, HD), BF),
            jax.ShapeDtypeStruct((2 * OWN, HD), F32),
            jax.ShapeDtypeStruct((2, 1, OWN), F32),
            jax.ShapeDtypeStruct((TPN, OWN, HD), F32),
        ),
        scratch_shapes=[pltpu.VMEM((SP, ROWS, 2 * HD), BF), pltpu.VMEM((SP, SEND, HD), BF)],
        compiler_params=grant(16),
        name="memories",
    )(*[vm(a) for a in blocks], *rest)


def shift(array, dz, dy):
    spots = [(z, y) for z in range(ROW) for y in range(ROW)]
    pairs = [(z * ROW + y, ((z + dz) % ROW) * ROW + (y + dy) % ROW) for z, y in spots]
    return lax.ppermute(array, "sp", pairs)


def step(prompt, w_key, w_value, w_in_gate, w_forget_gate, in_bias, forget_bias, query, w_out):
    up, down, w, gates, later = project_near(
        prompt, w_key.reshape(D, HD), w_value.reshape(D, HD), w_in_gate.reshape(2, D), w_forget_gate.reshape(2, D)
    )
    up = shift(up, 1, 0)
    down = shift(down, 3, 0)
    made = project_rest(later, w, gates)
    far = [made[0]] + [shift(made[k], 0, k) for k in range(1, ROW)]
    own = [made[ROW]] + [shift(made[ROW + k], 0, k) for k in range(1, ROW)]
    far = gather(*far)
    far = shift(far, 2, 0)
    side = pair(up, down)
    side = [shift(blocks, 0, k + 1) for k, blocks in enumerate(side)]
    memory, norm, stab, terms = memories(
        (*own, up, down, *side, far),
        (query.reshape(OWN, HD), w_out.reshape(HD, D), in_bias.reshape(1, 2), forget_bias.reshape(1, 2)),
    )
    terms = lax.all_to_all(terms, TP, 0, 0, tiled=True)
    read = jnp.sum(terms, axis=0).astype(BF)
    return (
        memory.reshape(2, OWN, 1, HD, HD),
        norm.reshape(2, OWN, 1, HD),
        stab.reshape(2, OWN, 1),
        read,
    )


def solution(mesh):
    torus = Mesh(
        mesh.devices.reshape(mesh.shape["gr"], mesh.shape["sp"], 4, 2), ("gr", "sp", "tp_0", "tp_1")
    )
    return jax.shard_map(
        step,
        mesh=torus,
        in_specs=(
            P("gr", "sp", None),
            P(None, TP, None),
            P(None, TP, None),
            P(None, None, TP),
            P(None, None, TP),
            P(None, TP),
            P(None, TP),
            P(("gr", "sp"), TP, None),
            P(TP, None, None),
        ),
        out_specs=(
            P(None, ("gr", "sp"), TP, None, None),
            P(None, ("gr", "sp"), TP, None),
            P(None, ("gr", "sp"), TP),
            P(("gr", "sp"), TP),
        ),
        check_vma=False,
    )
```

```python
import jax
import jax.numpy as jnp
from jax import lax
from jax.experimental import pallas as pl
from jax.experimental.pallas import tpu as pltpu
from jax.sharding import Mesh
from jax.sharding import PartitionSpec as P


TP = ("tp_0", "tp_1")
BF = jnp.bfloat16
F32 = jnp.float32
SP = 16
OWN = 8
POS = 16
ROWS = OWN * POS
HD = 128
D = 1024
SEND = 2 * ROWS + 8
ROW = 4
TPX = 4


def dot(a, b, dims=((1,), (0,))):
    return lax.dot_general(a, b, (dims, ((), ())), preferred_element_type=F32)


def here():
    at = lax.axis_index("sp")
    return at // ROW, at % ROW


def take(x_ref, buf_ref, sem_ref, sem, blocks):
    z, y = here()
    copies = []
    for i, (dz, dy) in enumerate(blocks):
        dest = ((z + dz) % ROW) * ROW + (y + dy) % ROW
        copies.append(pltpu.make_async_copy(x_ref.at[pl.ds(dest * OWN, OWN)], buf_ref.at[i], sem_ref.at[sem + i]))
    for copy in copies:
        copy.start()
    return copies


def project_blocks(buf_ref, first, w, gates, outs):
    rows = buf_ref[first : first + ROW].reshape(ROW * ROWS, D)
    both = dot(rows, w).astype(BF)
    pre = dot(gates, rows, ((1,), (1,)))[:4]
    high = pre.astype(BF).astype(F32)
    coded = jnp.concatenate((high, pre - high), axis=0).astype(BF)
    for k, out in enumerate(outs):
        at = slice(k * ROWS, (k + 1) * ROWS)
        out[:ROWS, :] = both[at, :HD]
        out[ROWS : 2 * ROWS, :] = both[at, HD:]
        out[2 * ROWS :, :] = coded[:, at]


def near_kernel(x_ref, wk_ref, wv_ref, wi_ref, wf_ref, up_ref, w_ref, g_ref, rest_ref, buf_ref, wi_buf, wf_buf, sem_ref):
    key_copy = pltpu.make_async_copy(wk_ref, w_ref.at[:, :HD], sem_ref.at[SP])
    value_copy = pltpu.make_async_copy(wv_ref, w_ref.at[:, HD:], sem_ref.at[SP + 1])
    gate_copies = [
        pltpu.make_async_copy(wi_ref, wi_buf, sem_ref.at[SP + 2]),
        pltpu.make_async_copy(wf_ref, wf_buf, sem_ref.at[SP + 3]),
    ]
    for copy in (*gate_copies, key_copy, value_copy):
        copy.start()
    copies = take(x_ref, buf_ref, sem_ref, 0, [(1, dy) for dy in range(ROW)])
    later = take(x_ref, rest_ref, sem_ref, ROW, [(dz, dy) for dz in (3, 2, 0) for dy in range(ROW)])
    for copy in gate_copies:
        copy.wait()
    gates = jnp.concatenate((wi_buf[...].astype(F32), wf_buf[...].astype(F32), jnp.zeros((4, D), F32)), axis=0)
    g_ref[...] = gates.astype(BF)
    key_copy.wait()
    value_copy.wait()
    for copy in copies:
        copy.wait()
    project_blocks(buf_ref, 0, w_ref[...], g_ref[...], [up_ref.at[k] for k in range(ROW)])
    for copy in later:
        copy.wait()


def second_kernel(rest_ref, w_ref, g_ref, down_ref):
    project_blocks(rest_ref, 0, w_ref[...], g_ref[...], [down_ref.at[k] for k in range(ROW)])


def third_kernel(rest_ref, w_ref, g_ref, *outs):
    for half in range(2):
        project_blocks(rest_ref, (half + 1) * ROW, w_ref[...], g_ref[...], [out.at[half] for out in outs])


ANY = pl.BlockSpec(memory_space=pl.ANY)
VM = pl.BlockSpec(memory_space=pltpu.VMEM)


def vm(array):
    return pltpu.with_memory_space_constraint(array, pltpu.VMEM)


def grant(mib):
    return pltpu.CompilerParams(vmem_limit_bytes=mib << 20)


def block(*lead):
    return pltpu.VMEM((*lead, SEND, HD), BF)


def run(kernel, out_shape, args, mib=16, scratch=()):
    specs = jax.tree.map(lambda _: VM, out_shape, is_leaf=lambda s: hasattr(s, "shape"))
    return pl.pallas_call(
        kernel,
        in_specs=[VM] * len(args),
        out_specs=specs,
        out_shape=out_shape,
        scratch_shapes=list(scratch),
        compiler_params=grant(mib),
    )(*[vm(a) for a in args])


def project_near(*args):
    return pl.pallas_call(
        near_kernel,
        in_specs=[ANY] * 5,
        out_specs=[VM] * 4,
        out_shape=(
            block(ROW), pltpu.VMEM((D, 2 * HD), BF), pltpu.VMEM((8, D), BF), pltpu.VMEM((3 * ROW, OWN, POS, D), BF)
        ),
        scratch_shapes=[
            pltpu.VMEM((ROW, OWN, POS, D), BF), pltpu.VMEM((2, D), BF), pltpu.VMEM((2, D), BF),
            pltpu.SemaphoreType.DMA((SP + 4,)),
        ],
        compiler_params=grant(16),
        name="near",
    )(*[pltpu.with_memory_space_constraint(a, pltpu.HBM) for a in args])


def gather_kernel(*refs):
    for i in range(ROW):
        refs[ROW][i] = refs[i][0]


def pair_kernel(a_ref, b_ref, *outs):
    for k, out in enumerate(outs):
        out[0] = a_ref[k + 1]
        out[1] = b_ref[k + 1]


def three_parts(a):
    first = a.astype(BF)
    rest = a - first.astype(F32)
    second = rest.astype(BF)
    return first, second, (rest - second.astype(F32)).astype(BF)


def group_max(a, lane):
    for k in (1, 2, 4, 8):
        inside = (lane % POS) + k < POS
        a = jnp.maximum(a, jnp.where(inside, pltpu.roll(a, HD - k, 1), pltpu.roll(a, POS - k, 1)))
    return a


def log_sigmoid(a):
    return jnp.minimum(a, 0.0) - jnp.log1p(jnp.exp(-jnp.abs(a)))


def landed(refs):
    c0, c1, c2, c3, up, down, s1, s2, s3, far = refs
    own = [c.at[1] for c in (c0, c1, c2, c3)]
    from_up = [up.at[0]] + [s.at[0] for s in (s1, s2, s3)]
    from_down = [down.at[0]] + [s.at[1] for s in (s1, s2, s3)]
    return own + from_up + [far.at[k] for k in range(ROW)] + from_down


def rows_mine():
    row = lax.broadcasted_iota(jnp.int32, (OWN, HD), 0)
    lane = lax.broadcasted_iota(jnp.int32, (OWN, HD), 1)
    return row, lane, (lane // POS) == row


def two_parts(a):
    high = a.astype(BF)
    return jnp.concatenate((high, (a - high.astype(F32)).astype(BF)), axis=0)


def read_kernel(*refs):
    blocks = landed(refs[:10])
    q_ref, wo_ref, ib_ref, fb_ref, keep_ref, send_ref, weight_ref, turned_ref, stab_ref = refs[10:]
    scale = HD ** -0.5
    row, lane8, mine = rows_mine()
    query = q_ref[...]
    scores = [jnp.where(mine, dot(query, blk[:ROWS, :], ((1,), (1,))), 0.0) for blk in blocks]

    gates = jnp.stack([blk[2 * ROWS :, :].astype(F32) for blk in blocks])
    part = lambda c: gates[:, c, :] + gates[:, c + 4, :]
    in_pre = [part(g) + ib_ref[0:1, g : g + 1] for g in range(2)]
    forget = [log_sigmoid(part(2 + g) + fb_ref[0:1, g : g + 1]) for g in range(2)]

    z, y = here()
    place = lambda j: ((z - j // ROW) & 3) * ROW + ((y - j % ROW) & 3)
    r = lax.broadcasted_iota(jnp.int32, (HD, HD), 0)
    c = lax.broadcasted_iota(jnp.int32, (HD, HD), 1)
    same = (r // POS) == (c // POS)
    ones = lambda m: jnp.where(m, 1.0, 0.0).astype(BF)
    jr = lax.broadcasted_iota(jnp.int32, (2 * SP, SP), 0)
    jc = lax.broadcasted_iota(jnp.int32, (2 * SP, SP), 1)
    lane = lax.broadcasted_iota(jnp.int32, (1, HD), 1)
    log_weight = []
    total = []
    for g in range(2):
        order = (r > c) if g == 0 else (r < c)
        inside = jnp.concatenate((ones(same & order), ones(same)), axis=1)
        sums = sum(dot(p, inside) for p in three_parts(forget[g]))
        block = sums[:, HD:]
        across = ones(((place(jc) > place(jr)) if g == 0 else (place(jc) < place(jr))) | (jr >= SP))
        outside = sum(dot(across, p) for p in three_parts(block))
        log_weight.append(in_pre[g] + sums[:, :HD] + outside[:SP])
        total.append(outside[SP : SP + 1])
    stab = [
        jnp.maximum(total[g], group_max(jnp.max(log_weight[g], axis=0, keepdims=True), lane)) for g in range(2)
    ]
    weight = jnp.concatenate([jnp.exp(log_weight[g] - stab[g]) for g in range(2)], axis=0)
    weight_ref[...] = weight
    turned_ref[...] = weight.T

    shares = jnp.zeros((2 * OWN, HD), F32)
    numerator = jnp.zeros((4 * OWN, HD), F32)
    for j, blk in enumerate(blocks):
        share = jnp.concatenate([scores[j] * weight[g * SP + j : g * SP + j + 1] for g in range(2)], axis=0)
        shares += share
        numerator += dot(two_parts(share), blk[ROWS : 2 * ROWS, :])
    numerator = (numerator[: 2 * OWN] + numerator[2 * OWN :]) * scale
    denominator = jnp.sum(shares, axis=1, keepdims=True) * scale
    hidden = jnp.zeros((OWN, HD), F32)
    for g in range(2):
        at = slice(g * OWN, (g + 1) * OWN)
        column = jnp.max(jnp.where(mine, stab[g], -jnp.inf), axis=1, keepdims=True)
        stab_ref[g] = jnp.sum(jnp.where(lane8 == row, column, 0.0), axis=0, keepdims=True)[:, :OWN]
        hidden += numerator[at] / jnp.maximum(jnp.maximum(jnp.abs(denominator[at]), jnp.exp(-column)), 1.0)
    hidden = hidden.astype(BF)
    x = lax.axis_index("tp_0")
    core = lax.axis_index("tp_1")
    for k in range(TPX):
        first = ((x + k) % TPX) * 2
        for out_ref, which in ((keep_ref, core), (send_ref, 1 - core)):
            at = pl.multiple_of((first + which) * HD, HD)
            out_ref[k] = dot(hidden, wo_ref[:, pl.ds(at, HD)])


def weigh_kernel(*refs):
    blocks = landed(refs[:10])
    weight_ref, turned_ref, vw_ref, norm_ref = refs[10:]
    _, _, mine = rows_mine()
    norm = jnp.zeros((4 * OWN, HD), F32)
    for j, blk in enumerate(blocks):
        spread = [jnp.where(mine, weight_ref[g * SP + j : g * SP + j + 1, :], 0.0) for g in range(2)]
        norm += dot(two_parts(jnp.concatenate(spread, axis=0)), blk[:ROWS, :])
        value = blk[ROWS : 2 * ROWS, :].astype(F32)
        for g in range(2):
            k = g * SP + j
            vw_ref[j, :, g * HD : (g + 1) * HD] = (value * turned_ref[:, k : k + 1]).astype(BF)
    norm_ref[...] = (norm[: 2 * OWN] + norm[2 * OWN :]) * (HD ** -0.5)


def memory_kernel(*refs):
    blocks = landed(refs[:10])
    vw_ref, mem_ref = refs[10:]
    for s in range(OWN):
        at = slice(s * POS, (s + 1) * POS)
        keys = jnp.concatenate([blk[at, :] for blk in blocks], axis=0)
        values = vw_ref[:, at, :].reshape(SP * POS, 2 * HD)
        memory = (dot(keys, values, ((0,), (0,))) * (HD ** -0.5)).astype(BF)
        mem_ref[0, s] = memory[:, :HD]
        mem_ref[1, s] = memory[:, HD:]


def join_kernel(keep_ref, got_ref, *outs):
    for k, out in enumerate(outs):
        out[...] = keep_ref[k] + got_ref[k]


def sum_kernel(a_ref, b_ref, c_ref, d_ref, out_ref):
    out_ref[...] = ((a_ref[...] + b_ref[...]) + (c_ref[...] + d_ref[...])).astype(BF)


def shift(array, dz, dy):
    spots = [(z, y) for z in range(ROW) for y in range(ROW)]
    pairs = [(z * ROW + y, ((z + dz) % ROW) * ROW + (y + dy) % ROW) for z, y in spots]
    return lax.ppermute(array, "sp", pairs)


def across(array, axis, hop):
    size = lax.axis_size(axis)
    return lax.ppermute(array, axis, [(i, (i + hop) % size) for i in range(size)])


def step(prompt, w_key, w_value, w_in_gate, w_forget_gate, in_bias, forget_bias, query, w_out):
    hops = range(1, ROW)
    up, w, gates, later = project_near(
        prompt, w_key.reshape(D, HD), w_value.reshape(D, HD), w_in_gate.reshape(2, D), w_forget_gate.reshape(2, D)
    )
    up = shift(up, 1, 0)
    down = run(second_kernel, block(ROW), (later, w, gates))
    down = shift(down, 3, 0)
    cross = run(third_kernel, (block(2),) * ROW, (later, w, gates))
    cross = [cross[0]] + [shift(cross[k], 0, k) for k in hops]
    far = run(gather_kernel, block(ROW), cross, 4)
    far = shift(far, 2, 0)
    side = run(pair_kernel, (block(2),) * 3, (up, down), 4)
    side = [shift(blocks, 0, k) for k, blocks in zip(hops, side)]
    blocks = (*cross, up, down, *side, far)
    half = pltpu.VMEM((TPX, OWN, HD), F32)
    keep, send, weight, turned, stab = run(
        read_kernel,
        (half, half, pltpu.VMEM((2 * SP, HD), F32), pltpu.VMEM((HD, 2 * SP), F32),
         jax.ShapeDtypeStruct((2, 1, OWN), F32)),
        (*blocks, query.reshape(OWN, HD), w_out.reshape(HD, D), in_bias.reshape(1, 2), forget_bias.reshape(1, 2)),
    )
    got = across(send, "tp_1", 1)
    values, norm = run(
        weigh_kernel,
        (pltpu.VMEM((SP, ROWS, 2 * HD), BF), jax.ShapeDtypeStruct((2 * OWN, HD), F32)),
        (*blocks, weight, turned),
    )
    terms = run(join_kernel, (pltpu.VMEM((OWN, HD), F32),) * TPX, (keep, got), 4)
    terms = [terms[0]] + [across(terms[k], "tp_0", k) for k in range(1, TPX)]
    memory = run(memory_kernel, jax.ShapeDtypeStruct((2, OWN, HD, HD), BF), (*blocks, values))
    read = run(sum_kernel, jax.ShapeDtypeStruct((OWN, HD), BF), terms, 4)
    return (
        memory.reshape(2, OWN, 1, HD, HD),
        norm.reshape(2, OWN, 1, HD),
        stab.reshape(2, OWN, 1),
        read,
    )


def solution(mesh):
    torus = Mesh(
        mesh.devices.reshape(mesh.shape["gr"], mesh.shape["sp"], 4, 2), ("gr", "sp", "tp_0", "tp_1")
    )
    return jax.shard_map(
        step,
        mesh=torus,
        in_specs=(
            P("gr", "sp", None),
            P(None, TP, None),
            P(None, TP, None),
            P(None, None, TP),
            P(None, None, TP),
            P(None, TP),
            P(None, TP),
            P(("gr", "sp"), TP, None),
            P(TP, None, None),
        ),
        out_specs=(
            P(None, ("gr", "sp"), TP, None, None),
            P(None, ("gr", "sp"), TP, None),
            P(None, ("gr", "sp"), TP),
            P(("gr", "sp"), TP),
        ),
        check_vma=False,
    )
```

```python
import jax
import jax.numpy as jnp
from jax import lax
from jax.experimental import pallas as pl
from jax.experimental.pallas import tpu as pltpu
from jax.sharding import Mesh
from jax.sharding import PartitionSpec as P


TP = ("tp_0", "tp_1")
BF = jnp.bfloat16
F32 = jnp.float32
SP = 16
OWN = 8
POS = 16
ROWS = OWN * POS
HD = 128
D = 1024
SEND = 2 * ROWS + 8
ROW = 4
TPX = 4


def dot(a, b, dims=((1,), (0,))):
    return lax.dot_general(a, b, (dims, ((), ())), preferred_element_type=F32)


def here():
    at = lax.axis_index("sp")
    return at // ROW, at % ROW


def take(x_ref, buf_ref, sem_ref, sem, blocks):
    z, y = here()
    copies = []
    for i, (dz, dy) in enumerate(blocks):
        dest = ((z + dz) % ROW) * ROW + (y + dy) % ROW
        copies.append(pltpu.make_async_copy(x_ref.at[pl.ds(dest * OWN, OWN)], buf_ref.at[i], sem_ref.at[sem + i]))
    for copy in copies:
        copy.start()
    return copies


def project_blocks(buf_ref, first, w, gates, outs):
    rows = buf_ref[first : first + ROW].reshape(ROW * ROWS, D)
    both = dot(rows, w).astype(BF)
    pre = dot(gates, rows, ((1,), (1,)))[:4]
    high = pre.astype(BF).astype(F32)
    coded = jnp.concatenate((high, pre - high), axis=0).astype(BF)
    for k, out in enumerate(outs):
        at = slice(k * ROWS, (k + 1) * ROWS)
        out[:ROWS, :] = both[at, :HD]
        out[ROWS : 2 * ROWS, :] = both[at, HD:]
        out[2 * ROWS :, :] = coded[:, at]


def near_kernel(x_ref, wk_ref, wv_ref, wi_ref, wf_ref, up_ref, w_ref, g_ref, rest_ref, buf_ref, wi_buf, wf_buf, sem_ref):
    key_copy = pltpu.make_async_copy(wk_ref, w_ref.at[:, :HD], sem_ref.at[SP])
    value_copy = pltpu.make_async_copy(wv_ref, w_ref.at[:, HD:], sem_ref.at[SP + 1])
    gate_copies = [
        pltpu.make_async_copy(wi_ref, wi_buf, sem_ref.at[SP + 2]),
        pltpu.make_async_copy(wf_ref, wf_buf, sem_ref.at[SP + 3]),
    ]
    for copy in (*gate_copies, key_copy, value_copy):
        copy.start()
    copies = take(x_ref, buf_ref, sem_ref, 0, [(1, dy) for dy in range(ROW)])
    later = take(x_ref, rest_ref, sem_ref, ROW, [(dz, dy) for dz in (3, 2, 0) for dy in range(ROW)])
    for copy in gate_copies:
        copy.wait()
    gates = jnp.concatenate((wi_buf[...].astype(F32), wf_buf[...].astype(F32), jnp.zeros((4, D), F32)), axis=0)
    g_ref[...] = gates.astype(BF)
    key_copy.wait()
    value_copy.wait()
    for copy in copies:
        copy.wait()
    project_blocks(buf_ref, 0, w_ref[...], g_ref[...], [up_ref.at[k] for k in range(ROW)])
    for copy in later:
        copy.wait()


def second_kernel(rest_ref, w_ref, g_ref, down_ref):
    project_blocks(rest_ref, 0, w_ref[...], g_ref[...], [down_ref.at[k] for k in range(ROW)])


def third_kernel(rest_ref, w_ref, g_ref, *outs):
    project_blocks(rest_ref, ROW, w_ref[...], g_ref[...], outs)


def own_kernel(rest_ref, w_ref, g_ref, *outs):
    project_blocks(rest_ref, 2 * ROW, w_ref[...], g_ref[...], outs)


ANY = pl.BlockSpec(memory_space=pl.ANY)
VM = pl.BlockSpec(memory_space=pltpu.VMEM)


def vm(array):
    return pltpu.with_memory_space_constraint(array, pltpu.VMEM)


def grant(mib):
    return pltpu.CompilerParams(vmem_limit_bytes=mib << 20)


def block(*lead):
    return pltpu.VMEM((*lead, SEND, HD), BF)


def run(kernel, out_shape, args, mib=16, scratch=()):
    specs = jax.tree.map(lambda _: VM, out_shape, is_leaf=lambda s: hasattr(s, "shape"))
    return pl.pallas_call(
        kernel,
        in_specs=[VM] * len(args),
        out_specs=specs,
        out_shape=out_shape,
        scratch_shapes=list(scratch),
        compiler_params=grant(mib),
    )(*[vm(a) for a in args])


def project_near(*args):
    return pl.pallas_call(
        near_kernel,
        in_specs=[ANY] * 5,
        out_specs=[VM] * 4,
        out_shape=(
            block(ROW), pltpu.VMEM((D, 2 * HD), BF), pltpu.VMEM((8, D), BF), pltpu.VMEM((3 * ROW, OWN, POS, D), BF)
        ),
        scratch_shapes=[
            pltpu.VMEM((ROW, OWN, POS, D), BF), pltpu.VMEM((2, D), BF), pltpu.VMEM((2, D), BF),
            pltpu.SemaphoreType.DMA((SP + 4,)),
        ],
        compiler_params=grant(16),
        name="near",
    )(*[pltpu.with_memory_space_constraint(a, pltpu.HBM) for a in args])


def gather_kernel(*refs):
    for i in range(ROW):
        refs[ROW][i] = refs[i][...]


def pair_kernel(a_ref, b_ref, *outs):
    for k, out in enumerate(outs):
        out[0] = a_ref[k + 1]
        out[1] = b_ref[k + 1]


def three_parts(a):
    first = a.astype(BF)
    rest = a - first.astype(F32)
    second = rest.astype(BF)
    return first, second, (rest - second.astype(F32)).astype(BF)


def group_max(a, lane):
    for k in (1, 2, 4, 8):
        inside = (lane % POS) + k < POS
        a = jnp.maximum(a, jnp.where(inside, pltpu.roll(a, HD - k, 1), pltpu.roll(a, POS - k, 1)))
    return a


def log_sigmoid(a):
    return jnp.minimum(a, 0.0) - jnp.log1p(jnp.exp(-jnp.abs(a)))


def landed(refs):
    own, (up, down, s1, s2, s3, far) = list(refs[:ROW]), refs[ROW:]
    from_up = [up.at[0]] + [s.at[0] for s in (s1, s2, s3)]
    from_down = [down.at[0]] + [s.at[1] for s in (s1, s2, s3)]
    return own + from_up + [far.at[k] for k in range(ROW)] + from_down


def rows_mine():
    row = lax.broadcasted_iota(jnp.int32, (OWN, HD), 0)
    lane = lax.broadcasted_iota(jnp.int32, (OWN, HD), 1)
    return row, lane, (lane // POS) == row


def two_parts(a):
    high = a.astype(BF)
    return jnp.concatenate((high, (a - high.astype(F32)).astype(BF)), axis=0)


def read_kernel(*refs):
    blocks = landed(refs[:10])
    q_ref, wo_ref, ib_ref, fb_ref, keep_ref, send_ref, weight_ref, turned_ref, stab_ref = refs[10:]
    scale = HD ** -0.5
    row, lane8, mine = rows_mine()
    query = q_ref[...]
    scores = [jnp.where(mine, dot(query, blk[:ROWS, :], ((1,), (1,))), 0.0) for blk in blocks]

    gates = jnp.stack([blk[2 * ROWS :, :].astype(F32) for blk in blocks])
    part = lambda c: gates[:, c, :] + gates[:, c + 4, :]
    in_pre = [part(g) + ib_ref[0:1, g : g + 1] for g in range(2)]
    forget = [log_sigmoid(part(2 + g) + fb_ref[0:1, g : g + 1]) for g in range(2)]

    z, y = here()
    place = lambda j: ((z - j // ROW) & 3) * ROW + ((y - j % ROW) & 3)
    r = lax.broadcasted_iota(jnp.int32, (HD, HD), 0)
    c = lax.broadcasted_iota(jnp.int32, (HD, HD), 1)
    same = (r // POS) == (c // POS)
    ones = lambda m: jnp.where(m, 1.0, 0.0).astype(BF)
    jr = lax.broadcasted_iota(jnp.int32, (2 * SP, SP), 0)
    jc = lax.broadcasted_iota(jnp.int32, (2 * SP, SP), 1)
    lane = lax.broadcasted_iota(jnp.int32, (1, HD), 1)
    log_weight = []
    total = []
    for g in range(2):
        order = (r > c) if g == 0 else (r < c)
        inside = jnp.concatenate((ones(same & order), ones(same)), axis=1)
        sums = sum(dot(p, inside) for p in three_parts(forget[g]))
        block = sums[:, HD:]
        across = ones(((place(jc) > place(jr)) if g == 0 else (place(jc) < place(jr))) | (jr >= SP))
        outside = sum(dot(across, p) for p in three_parts(block))
        log_weight.append(in_pre[g] + sums[:, :HD] + outside[:SP])
        total.append(outside[SP : SP + 1])
    stab = [
        jnp.maximum(total[g], group_max(jnp.max(log_weight[g], axis=0, keepdims=True), lane)) for g in range(2)
    ]
    weight = jnp.concatenate([jnp.exp(log_weight[g] - stab[g]) for g in range(2)], axis=0)
    weight_ref[...] = weight
    turned_ref[...] = weight.T

    shares = jnp.zeros((2 * OWN, HD), F32)
    numerator = jnp.zeros((4 * OWN, HD), F32)
    for j, blk in enumerate(blocks):
        share = jnp.concatenate([scores[j] * weight[g * SP + j : g * SP + j + 1] for g in range(2)], axis=0)
        shares += share
        numerator += dot(two_parts(share), blk[ROWS : 2 * ROWS, :])
    numerator = (numerator[: 2 * OWN] + numerator[2 * OWN :]) * scale
    denominator = jnp.sum(shares, axis=1, keepdims=True) * scale
    hidden = jnp.zeros((OWN, HD), F32)
    for g in range(2):
        at = slice(g * OWN, (g + 1) * OWN)
        column = jnp.max(jnp.where(mine, stab[g], -jnp.inf), axis=1, keepdims=True)
        stab_ref[g] = jnp.sum(jnp.where(lane8 == row, column, 0.0), axis=0, keepdims=True)[:, :OWN]
        hidden += numerator[at] / jnp.maximum(jnp.maximum(jnp.abs(denominator[at]), jnp.exp(-column)), 1.0)
    hidden = hidden.astype(BF)
    x = lax.axis_index("tp_0")
    core = lax.axis_index("tp_1")
    for k in range(TPX):
        first = ((x + k) % TPX) * 2
        for out_ref, which in ((keep_ref, core), (send_ref, 1 - core)):
            at = pl.multiple_of((first + which) * HD, HD)
            out_ref[k] = dot(hidden, wo_ref[:, pl.ds(at, HD)])


def weigh_kernel(*refs):
    blocks = landed(refs[:10])
    weight_ref, turned_ref, vw_ref, norm_ref = refs[10:]
    _, _, mine = rows_mine()
    norm = jnp.zeros((4 * OWN, HD), F32)
    for j, blk in enumerate(blocks):
        spread = [jnp.where(mine, weight_ref[g * SP + j : g * SP + j + 1, :], 0.0) for g in range(2)]
        norm += dot(two_parts(jnp.concatenate(spread, axis=0)), blk[:ROWS, :])
        value = blk[ROWS : 2 * ROWS, :].astype(F32)
        for g in range(2):
            k = g * SP + j
            vw_ref[j, :, g * HD : (g + 1) * HD] = (value * turned_ref[:, k : k + 1]).astype(BF)
    norm_ref[...] = (norm[: 2 * OWN] + norm[2 * OWN :]) * (HD ** -0.5)


def memory_kernel(*refs):
    blocks = landed(refs[:10])
    vw_ref, mem_ref = refs[10:]
    for s in range(OWN):
        at = slice(s * POS, (s + 1) * POS)
        keys = jnp.concatenate([blk[at, :] for blk in blocks], axis=0)
        values = vw_ref[:, at, :].reshape(SP * POS, 2 * HD)
        memory = (dot(keys, values, ((0,), (0,))) * (HD ** -0.5)).astype(BF)
        mem_ref[0, s] = memory[:, :HD]
        mem_ref[1, s] = memory[:, HD:]


def join_kernel(keep_ref, got_ref, *outs):
    for k, out in enumerate(outs):
        out[...] = keep_ref[k] + got_ref[k]


def sum_kernel(a_ref, b_ref, c_ref, d_ref, out_ref):
    out_ref[...] = ((a_ref[...] + b_ref[...]) + (c_ref[...] + d_ref[...])).astype(BF)


def shift(array, dz, dy):
    spots = [(z, y) for z in range(ROW) for y in range(ROW)]
    pairs = [(z * ROW + y, ((z + dz) % ROW) * ROW + (y + dy) % ROW) for z, y in spots]
    return lax.ppermute(array, "sp", pairs)


def across(array, axis, hop):
    size = lax.axis_size(axis)
    return lax.ppermute(array, axis, [(i, (i + hop) % size) for i in range(size)])


def step(prompt, w_key, w_value, w_in_gate, w_forget_gate, in_bias, forget_bias, query, w_out):
    hops = range(1, ROW)
    up, w, gates, later = project_near(
        prompt, w_key.reshape(D, HD), w_value.reshape(D, HD), w_in_gate.reshape(2, D), w_forget_gate.reshape(2, D)
    )
    up = shift(up, 1, 0)
    down = run(second_kernel, block(ROW), (later, w, gates))
    down = shift(down, 3, 0)
    cross = run(third_kernel, (block(),) * ROW, (later, w, gates))
    cross = [cross[0]] + [shift(cross[k], 0, k) for k in hops]
    far = run(gather_kernel, block(ROW), cross, 4)
    far = shift(far, 2, 0)
    own = run(own_kernel, (block(),) * ROW, (later, w, gates))
    own = [own[0]] + [shift(own[k], 0, k) for k in hops]
    side = run(pair_kernel, (block(2),) * 3, (up, down), 4)
    side = [shift(blocks, 0, k) for k, blocks in zip(hops, side)]
    blocks = (*own, up, down, *side, far)
    half = pltpu.VMEM((TPX, OWN, HD), F32)
    keep, send, weight, turned, stab = run(
        read_kernel,
        (half, half, pltpu.VMEM((2 * SP, HD), F32), pltpu.VMEM((HD, 2 * SP), F32),
         jax.ShapeDtypeStruct((2, 1, OWN), F32)),
        (*blocks, query.reshape(OWN, HD), w_out.reshape(HD, D), in_bias.reshape(1, 2), forget_bias.reshape(1, 2)),
    )
    got = across(send, "tp_1", 1)
    values, norm = run(
        weigh_kernel,
        (pltpu.VMEM((SP, ROWS, 2 * HD), BF), jax.ShapeDtypeStruct((2 * OWN, HD), F32)),
        (*blocks, weight, turned),
    )
    terms = run(join_kernel, (pltpu.VMEM((OWN, HD), F32),) * TPX, (keep, got), 4)
    terms = [terms[0]] + [across(terms[k], "tp_0", k) for k in range(1, TPX)]
    memory = run(memory_kernel, jax.ShapeDtypeStruct((2, OWN, HD, HD), BF), (*blocks, values))
    read = run(sum_kernel, jax.ShapeDtypeStruct((OWN, HD), BF), terms, 4)
    return (
        memory.reshape(2, OWN, 1, HD, HD),
        norm.reshape(2, OWN, 1, HD),
        stab.reshape(2, OWN, 1),
        read,
    )


def solution(mesh):
    torus = Mesh(
        mesh.devices.reshape(mesh.shape["gr"], mesh.shape["sp"], 4, 2), ("gr", "sp", "tp_0", "tp_1")
    )
    return jax.shard_map(
        step,
        mesh=torus,
        in_specs=(
            P("gr", "sp", None),
            P(None, TP, None),
            P(None, TP, None),
            P(None, None, TP),
            P(None, None, TP),
            P(None, TP),
            P(None, TP),
            P(("gr", "sp"), TP, None),
            P(TP, None, None),
        ),
        out_specs=(
            P(None, ("gr", "sp"), TP, None, None),
            P(None, ("gr", "sp"), TP, None),
            P(None, ("gr", "sp"), TP),
            P(("gr", "sp"), TP),
        ),
        check_vma=False,
    )
```

```python
import jax
import jax.numpy as jnp
from jax import lax
from jax.experimental import pallas as pl
from jax.experimental.pallas import tpu as pltpu
from jax.sharding import Mesh
from jax.sharding import PartitionSpec as P


TP = ("tp_0", "tp_1")
BF = jnp.bfloat16
F32 = jnp.float32
SP = 16
OWN = 8
POS = 16
ROWS = OWN * POS
HD = 128
D = 1024
SEND = 2 * ROWS + 8
ROW = 4
TPX = 4


def dot(a, b, dims=((1,), (0,))):
    return lax.dot_general(a, b, (dims, ((), ())), preferred_element_type=F32)


def here():
    at = lax.axis_index("sp")
    return at // ROW, at % ROW


def take(x_ref, buf_ref, sem_ref, sem, blocks):
    z, y = here()
    copies = []
    for i, (dz, dy) in enumerate(blocks):
        dest = (z ^ dz) * ROW + (y + dy) % ROW
        copies.append(pltpu.make_async_copy(x_ref.at[pl.ds(dest * OWN, OWN)], buf_ref.at[i], sem_ref.at[sem + i]))
    for copy in copies:
        copy.start()
    return copies


def project_blocks(buf_ref, first, w, gates, outs):
    rows = buf_ref[first : first + ROW].reshape(ROW * ROWS, D)
    both = dot(rows, w).astype(BF)
    pre = dot(gates, rows, ((1,), (1,)))[:4]
    high = pre.astype(BF).astype(F32)
    coded = jnp.concatenate((high, pre - high), axis=0).astype(BF)
    for k, out in enumerate(outs):
        at = slice(k * ROWS, (k + 1) * ROWS)
        out[:ROWS, :] = both[at, :HD]
        out[ROWS : 2 * ROWS, :] = both[at, HD:]
        out[2 * ROWS :, :] = coded[:, at]


def near_kernel(x_ref, wk_ref, wv_ref, wi_ref, wf_ref, mirror_ref, w_ref, g_ref, rest_ref, buf_ref, wi_buf, wf_buf, sem_ref):
    key_copy = pltpu.make_async_copy(wk_ref, w_ref.at[:, :HD], sem_ref.at[SP])
    value_copy = pltpu.make_async_copy(wv_ref, w_ref.at[:, HD:], sem_ref.at[SP + 1])
    gate_copies = [
        pltpu.make_async_copy(wi_ref, wi_buf, sem_ref.at[SP + 2]),
        pltpu.make_async_copy(wf_ref, wf_buf, sem_ref.at[SP + 3]),
    ]
    for copy in (*gate_copies, key_copy, value_copy):
        copy.start()
    copies = take(x_ref, buf_ref, sem_ref, 0, [(3, dy) for dy in range(ROW)])
    later = take(x_ref, rest_ref, sem_ref, ROW, [(dz, dy) for dz in (1, 2, 0) for dy in range(ROW)])
    for copy in gate_copies:
        copy.wait()
    gates = jnp.concatenate((wi_buf[...].astype(F32), wf_buf[...].astype(F32), jnp.zeros((4, D), F32)), axis=0)
    g_ref[...] = gates.astype(BF)
    key_copy.wait()
    value_copy.wait()
    for copy in copies:
        copy.wait()
    project_blocks(buf_ref, 0, w_ref[...], g_ref[...], [mirror_ref.at[k] for k in range(ROW)])
    for copy in later:
        copy.wait()


def second_kernel(rest_ref, w_ref, g_ref, twin_ref):
    project_blocks(rest_ref, 0, w_ref[...], g_ref[...], [twin_ref.at[k] for k in range(ROW)])


def third_kernel(rest_ref, w_ref, g_ref, *outs):
    project_blocks(rest_ref, ROW, w_ref[...], g_ref[...], outs)


def own_kernel(rest_ref, w_ref, g_ref, own_ref):
    project_blocks(rest_ref, 2 * ROW, w_ref[...], g_ref[...], [own_ref.at[k] for k in range(ROW)])


ANY = pl.BlockSpec(memory_space=pl.ANY)
VM = pl.BlockSpec(memory_space=pltpu.VMEM)


def vm(array):
    return pltpu.with_memory_space_constraint(array, pltpu.VMEM)


def grant(mib):
    return pltpu.CompilerParams(vmem_limit_bytes=mib << 20)


def block(*lead):
    return pltpu.VMEM((*lead, SEND, HD), BF)


def run(kernel, out_shape, args, mib=16, scratch=()):
    specs = jax.tree.map(lambda _: VM, out_shape, is_leaf=lambda s: hasattr(s, "shape"))
    return pl.pallas_call(
        kernel,
        in_specs=[VM] * len(args),
        out_specs=specs,
        out_shape=out_shape,
        scratch_shapes=list(scratch),
        compiler_params=grant(mib),
    )(*[vm(a) for a in args])


def project_near(*args):
    return pl.pallas_call(
        near_kernel,
        in_specs=[ANY] * 5,
        out_specs=[VM] * 4,
        out_shape=(
            block(ROW), pltpu.VMEM((D, 2 * HD), BF), pltpu.VMEM((8, D), BF), pltpu.VMEM((3 * ROW, OWN, POS, D), BF)
        ),
        scratch_shapes=[
            pltpu.VMEM((ROW, OWN, POS, D), BF), pltpu.VMEM((2, D), BF), pltpu.VMEM((2, D), BF),
            pltpu.SemaphoreType.DMA((SP + 4,)),
        ],
        compiler_params=grant(16),
        name="near",
    )(*[pltpu.with_memory_space_constraint(a, pltpu.HBM) for a in args])


def gather_kernel(*refs):
    for i in range(ROW):
        refs[ROW][i] = refs[i][...]


def triple_kernel(a_ref, b_ref, c_ref, *outs):
    for k, out in enumerate(outs):
        for i, ref in enumerate((a_ref, b_ref, c_ref)):
            out[i] = ref[k + 1]


def three_parts(a):
    first = a.astype(BF)
    rest = a - first.astype(F32)
    second = rest.astype(BF)
    return first, second, (rest - second.astype(F32)).astype(BF)


def group_max(a, lane):
    for k in (1, 2, 4, 8):
        inside = (lane % POS) + k < POS
        a = jnp.maximum(a, jnp.where(inside, pltpu.roll(a, HD - k, 1), pltpu.roll(a, POS - k, 1)))
    return a


def log_sigmoid(a):
    return jnp.minimum(a, 0.0) - jnp.log1p(jnp.exp(-jnp.abs(a)))


def landed(refs):
    own, mirror, twin, s1, s2, s3, far = refs
    legs = [[kept.at[0]] + [s.at[i] for s in (s1, s2, s3)] for i, kept in enumerate((mirror, twin, own))]
    return legs[2] + legs[1] + [far.at[k] for k in range(ROW)] + legs[0]


def rows_mine():
    row = lax.broadcasted_iota(jnp.int32, (OWN, HD), 0)
    lane = lax.broadcasted_iota(jnp.int32, (OWN, HD), 1)
    return row, lane, (lane // POS) == row


def two_parts(a):
    high = a.astype(BF)
    return jnp.concatenate((high, (a - high.astype(F32)).astype(BF)), axis=0)


def read_kernel(*refs):
    blocks = landed(refs[:7])
    q_ref, wo_ref, ib_ref, fb_ref, keep_ref, send_ref, weight_ref, turned_ref, stab_ref = refs[7:]
    scale = HD ** -0.5
    row, lane8, mine = rows_mine()
    query = q_ref[...]
    scores = [jnp.where(mine, dot(query, blk[:ROWS, :], ((1,), (1,))), 0.0) for blk in blocks]

    gates = jnp.stack([blk[2 * ROWS :, :].astype(F32) for blk in blocks])
    part = lambda c: gates[:, c, :] + gates[:, c + 4, :]
    in_pre = [part(g) + ib_ref[0:1, g : g + 1] for g in range(2)]
    forget = [log_sigmoid(part(2 + g) + fb_ref[0:1, g : g + 1]) for g in range(2)]

    z, y = here()
    place = lambda j: (z ^ (j // ROW)) * ROW + ((y - j % ROW) & 3)
    r = lax.broadcasted_iota(jnp.int32, (HD, HD), 0)
    c = lax.broadcasted_iota(jnp.int32, (HD, HD), 1)
    same = (r // POS) == (c // POS)
    ones = lambda m: jnp.where(m, 1.0, 0.0).astype(BF)
    jr = lax.broadcasted_iota(jnp.int32, (2 * SP, SP), 0)
    jc = lax.broadcasted_iota(jnp.int32, (2 * SP, SP), 1)
    lane = lax.broadcasted_iota(jnp.int32, (1, HD), 1)
    log_weight = []
    total = []
    for g in range(2):
        order = (r > c) if g == 0 else (r < c)
        inside = jnp.concatenate((ones(same & order), ones(same)), axis=1)
        sums = dot(jnp.concatenate(three_parts(forget[g]), axis=0), inside)
        sums = sums[:SP] + sums[SP : 2 * SP] + sums[2 * SP :]
        block = sums[:, HD:]
        across = ones(((place(jc) > place(jr)) if g == 0 else (place(jc) < place(jr))) | (jr >= SP))
        outside = dot(across, jnp.concatenate(three_parts(block), axis=1))
        outside = outside[:, :HD] + outside[:, HD : 2 * HD] + outside[:, 2 * HD :]
        log_weight.append(in_pre[g] + sums[:, :HD] + outside[:SP])
        total.append(outside[SP : SP + 1])
    stab = [
        jnp.maximum(total[g], group_max(jnp.max(log_weight[g], axis=0, keepdims=True), lane)) for g in range(2)
    ]
    weight = jnp.concatenate([jnp.exp(log_weight[g] - stab[g]) for g in range(2)], axis=0)
    weight_ref[...] = weight
    turned_ref[...] = weight.T

    shares = jnp.zeros((2 * OWN, HD), F32)
    numerator = jnp.zeros((4 * OWN, HD), F32)
    for j, blk in enumerate(blocks):
        share = jnp.concatenate([scores[j] * weight[g * SP + j : g * SP + j + 1] for g in range(2)], axis=0)
        shares += share
        numerator += dot(two_parts(share), blk[ROWS : 2 * ROWS, :])
    numerator = (numerator[: 2 * OWN] + numerator[2 * OWN :]) * scale
    denominator = jnp.sum(shares, axis=1, keepdims=True) * scale
    hidden = jnp.zeros((OWN, HD), F32)
    for g in range(2):
        at = slice(g * OWN, (g + 1) * OWN)
        column = jnp.max(jnp.where(mine, stab[g], -jnp.inf), axis=1, keepdims=True)
        stab_ref[g] = jnp.sum(jnp.where(lane8 == row, column, 0.0), axis=0, keepdims=True)[:, :OWN]
        hidden += numerator[at] / jnp.maximum(jnp.maximum(jnp.abs(denominator[at]), jnp.exp(-column)), 1.0)
    hidden = hidden.astype(BF)
    x = lax.axis_index("tp_0")
    core = lax.axis_index("tp_1")
    for k in range(TPX):
        first = ((x + k) % TPX) * 2
        for out_ref, which in ((keep_ref, core), (send_ref, 1 - core)):
            at = pl.multiple_of((first + which) * HD, HD)
            out_ref[k] = dot(hidden, wo_ref[:, pl.ds(at, HD)])


def weigh_kernel(*refs):
    blocks = landed(refs[:7])
    weight_ref, turned_ref, vw_ref, norm_ref = refs[7:]
    _, _, mine = rows_mine()
    norm = jnp.zeros((4 * OWN, HD), F32)
    for j, blk in enumerate(blocks):
        spread = [jnp.where(mine, weight_ref[g * SP + j : g * SP + j + 1, :], 0.0) for g in range(2)]
        norm += dot(two_parts(jnp.concatenate(spread, axis=0)), blk[:ROWS, :])
        value = blk[ROWS : 2 * ROWS, :].astype(F32)
        for g in range(2):
            k = g * SP + j
            vw_ref[j, :, g * HD : (g + 1) * HD] = (value * turned_ref[:, k : k + 1]).astype(BF)
    norm_ref[...] = (norm[: 2 * OWN] + norm[2 * OWN :]) * (HD ** -0.5)


def memory_kernel(*refs):
    blocks = landed(refs[:7])
    vw_ref, mem_ref = refs[7:]
    for s in range(OWN):
        at = slice(s * POS, (s + 1) * POS)
        keys = jnp.concatenate([blk[at, :] for blk in blocks], axis=0)
        values = vw_ref[:, at, :].reshape(SP * POS, 2 * HD)
        memory = (dot(keys, values, ((0,), (0,))) * (HD ** -0.5)).astype(BF)
        mem_ref[0, s] = memory[:, :HD]
        mem_ref[1, s] = memory[:, HD:]


def join_kernel(keep_ref, got_ref, *outs):
    for k, out in enumerate(outs):
        out[...] = keep_ref[k] + got_ref[k]


def sum_kernel(a_ref, b_ref, c_ref, d_ref, out_ref):
    out_ref[...] = ((a_ref[...] + b_ref[...]) + (c_ref[...] + d_ref[...])).astype(BF)


def shift(array, dz, dy):
    spots = [(z, y) for z in range(ROW) for y in range(ROW)]
    pairs = [(z * ROW + y, (z ^ dz) * ROW + (y + dy) % ROW) for z, y in spots]
    return lax.ppermute(array, "sp", pairs)


def across(array, axis, hop):
    size = lax.axis_size(axis)
    return lax.ppermute(array, axis, [(i, (i + hop) % size) for i in range(size)])


def step(prompt, w_key, w_value, w_in_gate, w_forget_gate, in_bias, forget_bias, query, w_out):
    hops = range(1, ROW)
    mirror, w, gates, later = project_near(
        prompt, w_key.reshape(D, HD), w_value.reshape(D, HD), w_in_gate.reshape(2, D), w_forget_gate.reshape(2, D)
    )
    mirror = shift(mirror, 3, 0)
    twin = run(second_kernel, block(ROW), (later, w, gates))
    twin = shift(twin, 1, 0)
    cross = run(third_kernel, (block(),) * ROW, (later, w, gates))
    cross = [cross[0]] + [shift(cross[k], 0, k) for k in hops]
    far = run(gather_kernel, block(ROW), cross, 4)
    far = shift(far, 2, 0)
    own = run(own_kernel, block(ROW), (later, w, gates))
    side = run(triple_kernel, (block(3),) * 3, (mirror, twin, own), 4)
    side = [shift(blocks, 0, k) for k, blocks in zip(hops, side)]
    blocks = (own, mirror, twin, *side, far)
    half = pltpu.VMEM((TPX, OWN, HD), F32)
    keep, send, weight, turned, stab = run(
        read_kernel,
        (half, half, pltpu.VMEM((2 * SP, HD), F32), pltpu.VMEM((HD, 2 * SP), F32),
         jax.ShapeDtypeStruct((2, 1, OWN), F32)),
        (*blocks, query.reshape(OWN, HD), w_out.reshape(HD, D), in_bias.reshape(1, 2), forget_bias.reshape(1, 2)),
    )
    got = across(send, "tp_1", 1)
    values, norm = run(
        weigh_kernel,
        (pltpu.VMEM((SP, ROWS, 2 * HD), BF), jax.ShapeDtypeStruct((2 * OWN, HD), F32)),
        (*blocks, weight, turned),
    )
    terms = run(join_kernel, (pltpu.VMEM((OWN, HD), F32),) * TPX, (keep, got), 4)
    terms = [terms[0]] + [across(terms[k], "tp_0", k) for k in range(1, TPX)]
    memory = run(memory_kernel, jax.ShapeDtypeStruct((2, OWN, HD, HD), BF), (*blocks, values))
    read = run(sum_kernel, jax.ShapeDtypeStruct((OWN, HD), BF), terms, 4)
    return (
        memory.reshape(2, OWN, 1, HD, HD),
        norm.reshape(2, OWN, 1, HD),
        stab.reshape(2, OWN, 1),
        read,
    )


def solution(mesh):
    torus = Mesh(
        mesh.devices.reshape(mesh.shape["gr"], mesh.shape["sp"], 4, 2), ("gr", "sp", "tp_0", "tp_1")
    )
    return jax.shard_map(
        step,
        mesh=torus,
        in_specs=(
            P("gr", "sp", None),
            P(None, TP, None),
            P(None, TP, None),
            P(None, None, TP),
            P(None, None, TP),
            P(None, TP),
            P(None, TP),
            P(("gr", "sp"), TP, None),
            P(TP, None, None),
        ),
        out_specs=(
            P(None, ("gr", "sp"), TP, None, None),
            P(None, ("gr", "sp"), TP, None),
            P(None, ("gr", "sp"), TP),
            P(("gr", "sp"), TP),
        ),
        check_vma=False,
    )
```

```python
import jax
import jax.numpy as jnp
from jax import lax
from jax.experimental import pallas as pl
from jax.experimental.pallas import tpu as pltpu
from jax.sharding import Mesh
from jax.sharding import PartitionSpec as P


TP = ("tp_0", "tp_1")
BF = jnp.bfloat16
F32 = jnp.float32
SP = 16
OWN = 8
POS = 16
ROWS = OWN * POS
HD = 128
D = 1024
SEND = 2 * ROWS + 8
ROW = 4
TPX = 4


def dot(a, b, dims=((1,), (0,))):
    return lax.dot_general(a, b, (dims, ((), ())), preferred_element_type=F32)


def here():
    at = lax.axis_index("sp")
    return at // ROW, at % ROW


def take(x_ref, buf_ref, sem_ref, sem, blocks):
    z, y = here()
    copies = []
    for i, (dz, dy) in enumerate(blocks):
        dest = (z ^ dz) * ROW + (y + dy) % ROW
        copies.append(pltpu.make_async_copy(x_ref.at[pl.ds(dest * OWN, OWN)], buf_ref.at[i], sem_ref.at[sem + i]))
    for copy in copies:
        copy.start()
    return copies


def project_blocks(buf_ref, first, w, gates, outs):
    rows = buf_ref[first : first + ROW].reshape(ROW * ROWS, D)
    both = dot(rows, w).astype(BF)
    pre = dot(gates, rows, ((1,), (1,)))[:4]
    high = pre.astype(BF).astype(F32)
    coded = jnp.concatenate((high, pre - high), axis=0).astype(BF)
    for k, out in enumerate(outs):
        at = slice(k * ROWS, (k + 1) * ROWS)
        out[:ROWS, :] = both[at, :HD]
        out[ROWS : 2 * ROWS, :] = both[at, HD:]
        out[2 * ROWS :, :] = coded[:, at]


def near_kernel(x_ref, wk_ref, wv_ref, wi_ref, wf_ref, mirror_ref, w_ref, g_ref, rest_ref, buf_ref, wi_buf, wf_buf, sem_ref):
    key_copy = pltpu.make_async_copy(wk_ref, w_ref.at[:, :HD], sem_ref.at[SP])
    value_copy = pltpu.make_async_copy(wv_ref, w_ref.at[:, HD:], sem_ref.at[SP + 1])
    gate_copies = [
        pltpu.make_async_copy(wi_ref, wi_buf, sem_ref.at[SP + 2]),
        pltpu.make_async_copy(wf_ref, wf_buf, sem_ref.at[SP + 3]),
    ]
    for copy in (*gate_copies, key_copy, value_copy):
        copy.start()
    copies = take(x_ref, buf_ref, sem_ref, 0, [(3, dy) for dy in range(ROW)])
    later = take(x_ref, rest_ref, sem_ref, ROW, [(dz, dy) for dz in (1, 2, 0) for dy in range(ROW)])
    for copy in gate_copies:
        copy.wait()
    gates = jnp.concatenate((wi_buf[...].astype(F32), wf_buf[...].astype(F32), jnp.zeros((4, D), F32)), axis=0)
    g_ref[...] = gates.astype(BF)
    key_copy.wait()
    value_copy.wait()
    for copy in copies:
        copy.wait()
    project_blocks(buf_ref, 0, w_ref[...], g_ref[...], [mirror_ref.at[k] for k in range(ROW)])
    for copy in later:
        copy.wait()


def second_kernel(rest_ref, w_ref, g_ref, twin_ref):
    project_blocks(rest_ref, 0, w_ref[...], g_ref[...], [twin_ref.at[k] for k in range(ROW)])


def third_kernel(rest_ref, w_ref, g_ref, c1_ref, c2_ref, c3_ref, far_ref, own0_ref, own3_ref):
    project_blocks(rest_ref, ROW, w_ref[...], g_ref[...], [far_ref, c1_ref.at[0], c2_ref.at[0], c3_ref])
    project_blocks(rest_ref, 2 * ROW, w_ref[...], g_ref[...], [own0_ref, c1_ref.at[1], c2_ref.at[1], own3_ref])


ANY = pl.BlockSpec(memory_space=pl.ANY)
VM = pl.BlockSpec(memory_space=pltpu.VMEM)


def vm(array):
    return pltpu.with_memory_space_constraint(array, pltpu.VMEM)


def grant(mib):
    return pltpu.CompilerParams(vmem_limit_bytes=mib << 20)


def block(*lead):
    return pltpu.VMEM((*lead, SEND, HD), BF)


def run(kernel, out_shape, args, mib=16, scratch=()):
    specs = jax.tree.map(lambda _: VM, out_shape, is_leaf=lambda s: hasattr(s, "shape"))
    return pl.pallas_call(
        kernel,
        in_specs=[VM] * len(args),
        out_specs=specs,
        out_shape=out_shape,
        scratch_shapes=list(scratch),
        compiler_params=grant(mib),
    )(*[vm(a) for a in args])


def project_near(*args):
    return pl.pallas_call(
        near_kernel,
        in_specs=[ANY] * 5,
        out_specs=[VM] * 4,
        out_shape=(
            block(ROW), pltpu.VMEM((D, 2 * HD), BF), pltpu.VMEM((8, D), BF), pltpu.VMEM((3 * ROW, OWN, POS, D), BF)
        ),
        scratch_shapes=[
            pltpu.VMEM((ROW, OWN, POS, D), BF), pltpu.VMEM((2, D), BF), pltpu.VMEM((2, D), BF),
            pltpu.SemaphoreType.DMA((SP + 4,)),
        ],
        compiler_params=grant(16),
        name="near",
    )(*[pltpu.with_memory_space_constraint(a, pltpu.HBM) for a in args])


def gather_kernel(a_ref, b_ref, c_ref, d_ref, out_ref):
    out_ref[0] = a_ref[...]
    out_ref[1] = b_ref[0]
    out_ref[2] = c_ref[0]
    out_ref[3] = d_ref[...]


def legs_kernel(a_ref, b_ref, own3_ref, *outs):
    for k, out in enumerate(outs):
        out[0] = a_ref[k + 1]
        out[1] = b_ref[k + 1]
    outs[2][2] = own3_ref[...]


def three_parts(a):
    first = a.astype(BF)
    rest = a - first.astype(F32)
    second = rest.astype(BF)
    return first, second, (rest - second.astype(F32)).astype(BF)


def group_max(a, lane):
    for k in (1, 2, 4, 8):
        inside = (lane % POS) + k < POS
        a = jnp.maximum(a, jnp.where(inside, pltpu.roll(a, HD - k, 1), pltpu.roll(a, POS - k, 1)))
    return a


def log_sigmoid(a):
    return jnp.minimum(a, 0.0) - jnp.log1p(jnp.exp(-jnp.abs(a)))


def landed(refs):
    own0, c1, c2, mirror, twin, s1, s2, s3, far = refs
    own = [own0, c1.at[1], c2.at[1], s3.at[2]]
    from_mirror, from_twin = [
        [kept.at[0]] + [s.at[i] for s in (s1, s2, s3)] for i, kept in enumerate((mirror, twin))
    ]
    return own + from_twin + [far.at[k] for k in range(ROW)] + from_mirror


def rows_mine():
    row = lax.broadcasted_iota(jnp.int32, (OWN, HD), 0)
    lane = lax.broadcasted_iota(jnp.int32, (OWN, HD), 1)
    return row, lane, (lane // POS) == row


def two_parts(a):
    high = a.astype(BF)
    return jnp.concatenate((high, (a - high.astype(F32)).astype(BF)), axis=0)


def read_kernel(*refs):
    blocks = landed(refs[:9])
    q_ref, wo_ref, ib_ref, fb_ref, keep_ref, send_ref, weight_ref, turned_ref, stab_ref = refs[9:]
    scale = HD ** -0.5
    row, lane8, mine = rows_mine()
    query = q_ref[...]
    scores = [jnp.where(mine, dot(query, blk[:ROWS, :], ((1,), (1,))), 0.0) for blk in blocks]

    gates = jnp.stack([blk[2 * ROWS :, :].astype(F32) for blk in blocks])
    part = lambda c: gates[:, c, :] + gates[:, c + 4, :]
    in_pre = [part(g) + ib_ref[0:1, g : g + 1] for g in range(2)]
    forget = [log_sigmoid(part(2 + g) + fb_ref[0:1, g : g + 1]) for g in range(2)]

    z, y = here()
    place = lambda j: (z ^ (j // ROW)) * ROW + ((y - j % ROW) & 3)
    r = lax.broadcasted_iota(jnp.int32, (HD, HD), 0)
    c = lax.broadcasted_iota(jnp.int32, (HD, HD), 1)
    same = (r // POS) == (c // POS)
    ones = lambda m: jnp.where(m, 1.0, 0.0).astype(BF)
    jr = lax.broadcasted_iota(jnp.int32, (2 * SP, SP), 0)
    jc = lax.broadcasted_iota(jnp.int32, (2 * SP, SP), 1)
    lane = lax.broadcasted_iota(jnp.int32, (1, HD), 1)
    log_weight = []
    total = []
    for g in range(2):
        order = (r > c) if g == 0 else (r < c)
        inside = jnp.concatenate((ones(same & order), ones(same)), axis=1)
        sums = sum(dot(p, inside) for p in three_parts(forget[g]))
        block = sums[:, HD:]
        across = ones(((place(jc) > place(jr)) if g == 0 else (place(jc) < place(jr))) | (jr >= SP))
        outside = sum(dot(across, p) for p in three_parts(block))
        log_weight.append(in_pre[g] + sums[:, :HD] + outside[:SP])
        total.append(outside[SP : SP + 1])
    stab = [
        jnp.maximum(total[g], group_max(jnp.max(log_weight[g], axis=0, keepdims=True), lane)) for g in range(2)
    ]
    weight = jnp.concatenate([jnp.exp(log_weight[g] - stab[g]) for g in range(2)], axis=0)
    weight_ref[...] = weight
    turned_ref[...] = weight.T

    shares = jnp.zeros((2 * OWN, HD), F32)
    numerator = jnp.zeros((4 * OWN, HD), F32)
    for j, blk in enumerate(blocks):
        share = jnp.concatenate([scores[j] * weight[g * SP + j : g * SP + j + 1] for g in range(2)], axis=0)
        shares += share
        numerator += dot(two_parts(share), blk[ROWS : 2 * ROWS, :])
    numerator = (numerator[: 2 * OWN] + numerator[2 * OWN :]) * scale
    denominator = jnp.sum(shares, axis=1, keepdims=True) * scale
    hidden = jnp.zeros((OWN, HD), F32)
    for g in range(2):
        at = slice(g * OWN, (g + 1) * OWN)
        column = jnp.max(jnp.where(mine, stab[g], -jnp.inf), axis=1, keepdims=True)
        stab_ref[g] = jnp.sum(jnp.where(lane8 == row, column, 0.0), axis=0, keepdims=True)[:, :OWN]
        hidden += numerator[at] / jnp.maximum(jnp.maximum(jnp.abs(denominator[at]), jnp.exp(-column)), 1.0)
    hidden = hidden.astype(BF)
    x = lax.axis_index("tp_0")
    core = lax.axis_index("tp_1")
    for k in range(TPX):
        first = ((x + k) % TPX) * 2
        for out_ref, which in ((keep_ref, core), (send_ref, 1 - core)):
            at = pl.multiple_of((first + which) * HD, HD)
            out_ref[k] = dot(hidden, wo_ref[:, pl.ds(at, HD)])


def weigh_kernel(*refs):
    blocks = landed(refs[:9])
    weight_ref, turned_ref, vw_ref, norm_ref = refs[9:]
    _, _, mine = rows_mine()
    norm = jnp.zeros((4 * OWN, HD), F32)
    for j, blk in enumerate(blocks):
        spread = [jnp.where(mine, weight_ref[g * SP + j : g * SP + j + 1, :], 0.0) for g in range(2)]
        norm += dot(two_parts(jnp.concatenate(spread, axis=0)), blk[:ROWS, :])
        value = blk[ROWS : 2 * ROWS, :].astype(F32)
        for g in range(2):
            k = g * SP + j
            vw_ref[j, :, g * HD : (g + 1) * HD] = (value * turned_ref[:, k : k + 1]).astype(BF)
    norm_ref[...] = (norm[: 2 * OWN] + norm[2 * OWN :]) * (HD ** -0.5)


def memory_kernel(*refs):
    blocks = landed(refs[:9])
    vw_ref, mem_ref = refs[9:]
    for s in range(OWN):
        at = slice(s * POS, (s + 1) * POS)
        keys = jnp.concatenate([blk[at, :] for blk in blocks], axis=0)
        values = vw_ref[:, at, :].reshape(SP * POS, 2 * HD)
        memory = (dot(keys, values, ((0,), (0,))) * (HD ** -0.5)).astype(BF)
        mem_ref[0, s] = memory[:, :HD]
        mem_ref[1, s] = memory[:, HD:]


def join_kernel(keep_ref, got_ref, *outs):
    for k, out in enumerate(outs):
        out[...] = keep_ref[k] + got_ref[k]


def sum_kernel(a_ref, b_ref, c_ref, d_ref, out_ref):
    out_ref[...] = ((a_ref[...] + b_ref[...]) + (c_ref[...] + d_ref[...])).astype(BF)


def shift(array, dz, dy):
    spots = [(z, y) for z in range(ROW) for y in range(ROW)]
    pairs = [(z * ROW + y, (z ^ dz) * ROW + (y + dy) % ROW) for z, y in spots]
    return lax.ppermute(array, "sp", pairs)


def across(array, axis, hop):
    size = lax.axis_size(axis)
    return lax.ppermute(array, axis, [(i, (i + hop) % size) for i in range(size)])


def step(prompt, w_key, w_value, w_in_gate, w_forget_gate, in_bias, forget_bias, query, w_out):
    hops = range(1, ROW)
    mirror, w, gates, later = project_near(
        prompt, w_key.reshape(D, HD), w_value.reshape(D, HD), w_in_gate.reshape(2, D), w_forget_gate.reshape(2, D)
    )
    mirror = shift(mirror, 3, 0)
    twin = run(second_kernel, block(ROW), (later, w, gates))
    twin = shift(twin, 1, 0)
    *cross, far, own0, own3 = run(
        third_kernel, (block(2), block(2), block(), block(), block(), block()), (later, w, gates)
    )
    cross = [shift(blocks, 0, k) for k, blocks in zip(hops, cross)]
    far = run(gather_kernel, block(ROW), (far, *cross), 4)
    far = shift(far, 2, 0)
    side = run(legs_kernel, (block(2), block(2), block(3)), (mirror, twin, own3), 4)
    side = [shift(blocks, 0, k) for k, blocks in zip(hops, side)]
    blocks = (own0, cross[0], cross[1], mirror, twin, *side, far)
    half = pltpu.VMEM((TPX, OWN, HD), F32)
    keep, send, weight, turned, stab = run(
        read_kernel,
        (half, half, pltpu.VMEM((2 * SP, HD), F32), pltpu.VMEM((HD, 2 * SP), F32),
         jax.ShapeDtypeStruct((2, 1, OWN), F32)),
        (*blocks, query.reshape(OWN, HD), w_out.reshape(HD, D), in_bias.reshape(1, 2), forget_bias.reshape(1, 2)),
    )
    got = across(send, "tp_1", 1)
    values, norm = run(
        weigh_kernel,
        (pltpu.VMEM((SP, ROWS, 2 * HD), BF), jax.ShapeDtypeStruct((2 * OWN, HD), F32)),
        (*blocks, weight, turned),
    )
    terms = run(join_kernel, (pltpu.VMEM((OWN, HD), F32),) * TPX, (keep, got), 4)
    terms = [terms[0]] + [across(terms[k], "tp_0", k) for k in range(1, TPX)]
    memory = run(memory_kernel, jax.ShapeDtypeStruct((2, OWN, HD, HD), BF), (*blocks, values))
    read = run(sum_kernel, jax.ShapeDtypeStruct((OWN, HD), BF), terms, 4)
    return (
        memory.reshape(2, OWN, 1, HD, HD),
        norm.reshape(2, OWN, 1, HD),
        stab.reshape(2, OWN, 1),
        read,
    )


def solution(mesh):
    torus = Mesh(
        mesh.devices.reshape(mesh.shape["gr"], mesh.shape["sp"], 4, 2), ("gr", "sp", "tp_0", "tp_1")
    )
    return jax.shard_map(
        step,
        mesh=torus,
        in_specs=(
            P("gr", "sp", None),
            P(None, TP, None),
            P(None, TP, None),
            P(None, None, TP),
            P(None, None, TP),
            P(None, TP),
            P(None, TP),
            P(("gr", "sp"), TP, None),
            P(TP, None, None),
        ),
        out_specs=(
            P(None, ("gr", "sp"), TP, None, None),
            P(None, ("gr", "sp"), TP, None),
            P(None, ("gr", "sp"), TP),
            P(("gr", "sp"), TP),
        ),
        check_vma=False,
    )
```

```python
import jax
import jax.numpy as jnp
from jax import lax
from jax.experimental import pallas as pl
from jax.experimental.pallas import tpu as pltpu
from jax.sharding import Mesh
from jax.sharding import PartitionSpec as P


TP = ("tp_0", "tp_1")
BF = jnp.bfloat16
F32 = jnp.float32
SP = 16
OWN = 8
POS = 16
ROWS = OWN * POS
HD = 128
D = 1024
SEND = 2 * ROWS + 8
ROW = 4
TPX = 4


def dot(a, b, dims=((1,), (0,))):
    return lax.dot_general(a, b, (dims, ((), ())), preferred_element_type=F32)


def here():
    at = lax.axis_index("sp")
    return at // ROW, at % ROW


def take(x_ref, buf_ref, sem_ref, sem, blocks):
    z, y = here()
    copies = []
    for i, (dz, dy) in enumerate(blocks):
        dest = (z ^ dz) * ROW + (y + dy) % ROW
        copies.append(pltpu.make_async_copy(x_ref.at[pl.ds(dest * OWN, OWN)], buf_ref.at[i], sem_ref.at[sem + i]))
    for copy in copies:
        copy.start()
    return copies


def project_blocks(buf_ref, first, w, gates, outs):
    rows = buf_ref[first : first + ROW].reshape(ROW * ROWS, D)
    both = dot(rows, w).astype(BF)
    pre = dot(gates, rows, ((1,), (1,)))[:4]
    high = pre.astype(BF).astype(F32)
    coded = jnp.concatenate((high, pre - high), axis=0).astype(BF)
    for k, out in enumerate(outs):
        at = slice(k * ROWS, (k + 1) * ROWS)
        out[:ROWS, :] = both[at, :HD]
        out[ROWS : 2 * ROWS, :] = both[at, HD:]
        out[2 * ROWS :, :] = coded[:, at]


def near_kernel(x_ref, wk_ref, wv_ref, wi_ref, wf_ref, mirror_ref, w_ref, g_ref, rest_ref, buf_ref, wi_buf, wf_buf, sem_ref):
    key_copy = pltpu.make_async_copy(wk_ref, w_ref.at[:, :HD], sem_ref.at[SP])
    value_copy = pltpu.make_async_copy(wv_ref, w_ref.at[:, HD:], sem_ref.at[SP + 1])
    gate_copies = [
        pltpu.make_async_copy(wi_ref, wi_buf, sem_ref.at[SP + 2]),
        pltpu.make_async_copy(wf_ref, wf_buf, sem_ref.at[SP + 3]),
    ]
    for copy in (*gate_copies, key_copy, value_copy):
        copy.start()
    copies = take(x_ref, buf_ref, sem_ref, 0, [(3, dy) for dy in range(ROW)])
    later = take(x_ref, rest_ref, sem_ref, ROW, [(dz, dy) for dz in (1, 2, 0) for dy in range(ROW)])
    for copy in gate_copies:
        copy.wait()
    gates = jnp.concatenate((wi_buf[...].astype(F32), wf_buf[...].astype(F32), jnp.zeros((4, D), F32)), axis=0)
    g_ref[...] = gates.astype(BF)
    key_copy.wait()
    value_copy.wait()
    for copy in copies:
        copy.wait()
    project_blocks(buf_ref, 0, w_ref[...], g_ref[...], [mirror_ref.at[k] for k in range(ROW)])
    for copy in later:
        copy.wait()


def second_kernel(rest_ref, w_ref, g_ref, twin_ref):
    project_blocks(rest_ref, 0, w_ref[...], g_ref[...], [twin_ref.at[k] for k in range(ROW)])


def third_kernel(rest_ref, w_ref, g_ref, *outs):
    project_blocks(rest_ref, ROW, w_ref[...], g_ref[...], outs[:ROW])
    project_blocks(rest_ref, 2 * ROW, w_ref[...], g_ref[...], outs[ROW:])


ANY = pl.BlockSpec(memory_space=pl.ANY)
VM = pl.BlockSpec(memory_space=pltpu.VMEM)


def vm(array):
    return pltpu.with_memory_space_constraint(array, pltpu.VMEM)


def grant(mib):
    return pltpu.CompilerParams(vmem_limit_bytes=mib << 20)


def block(*lead):
    return pltpu.VMEM((*lead, SEND, HD), BF)


def run(kernel, out_shape, args, mib=16, scratch=()):
    specs = jax.tree.map(lambda _: VM, out_shape, is_leaf=lambda s: hasattr(s, "shape"))
    return pl.pallas_call(
        kernel,
        in_specs=[VM] * len(args),
        out_specs=specs,
        out_shape=out_shape,
        scratch_shapes=list(scratch),
        compiler_params=grant(mib),
    )(*[vm(a) for a in args])


def project_near(*args):
    return pl.pallas_call(
        near_kernel,
        in_specs=[ANY] * 5,
        out_specs=[VM] * 4,
        out_shape=(
            block(ROW), pltpu.VMEM((D, 2 * HD), BF), pltpu.VMEM((8, D), BF), pltpu.VMEM((3 * ROW, OWN, POS, D), BF)
        ),
        scratch_shapes=[
            pltpu.VMEM((ROW, OWN, POS, D), BF), pltpu.VMEM((2, D), BF), pltpu.VMEM((2, D), BF),
            pltpu.SemaphoreType.DMA((SP + 4,)),
        ],
        compiler_params=grant(16),
        name="near",
    )(*[pltpu.with_memory_space_constraint(a, pltpu.HBM) for a in args])


def gather_kernel(*refs):
    for i in range(ROW):
        refs[ROW][i] = refs[i][...]


def legs_kernel(a_ref, b_ref, *outs):
    for k, out in enumerate(outs):
        out[0] = a_ref[k + 1]
        out[1] = b_ref[k + 1]


def three_parts(a):
    first = a.astype(BF)
    rest = a - first.astype(F32)
    second = rest.astype(BF)
    return first, second, (rest - second.astype(F32)).astype(BF)


def group_max(a, lane):
    for k in (1, 2, 4, 8):
        inside = (lane % POS) + k < POS
        a = jnp.maximum(a, jnp.where(inside, pltpu.roll(a, HD - k, 1), pltpu.roll(a, POS - k, 1)))
    return a


def log_sigmoid(a):
    return jnp.minimum(a, 0.0) - jnp.log1p(jnp.exp(-jnp.abs(a)))


def landed(refs):
    own, (mirror, twin, s1, s2, s3, far) = list(refs[:ROW]), refs[ROW:]
    from_mirror, from_twin = [
        [kept.at[0]] + [s.at[i] for s in (s1, s2, s3)] for i, kept in enumerate((mirror, twin))
    ]
    return own + from_twin + [far.at[k] for k in range(ROW)] + from_mirror


def rows_mine():
    row = lax.broadcasted_iota(jnp.int32, (OWN, HD), 0)
    lane = lax.broadcasted_iota(jnp.int32, (OWN, HD), 1)
    return row, lane, (lane // POS) == row


def two_parts(a):
    high = a.astype(BF)
    return jnp.concatenate((high, (a - high.astype(F32)).astype(BF)), axis=0)


def read_kernel(*refs):
    blocks = landed(refs[:10])
    q_ref, wo_ref, ib_ref, fb_ref, keep_ref, send_ref, weight_ref, turned_ref, stab_ref = refs[10:]
    scale = HD ** -0.5
    row, lane8, mine = rows_mine()
    query = q_ref[...]
    scores = [jnp.where(mine, dot(query, blk[:ROWS, :], ((1,), (1,))), 0.0) for blk in blocks]

    gates = jnp.stack([blk[2 * ROWS :, :].astype(F32) for blk in blocks])
    part = lambda c: gates[:, c, :] + gates[:, c + 4, :]
    in_pre = [part(g) + ib_ref[0:1, g : g + 1] for g in range(2)]
    forget = [log_sigmoid(part(2 + g) + fb_ref[0:1, g : g + 1]) for g in range(2)]

    z, y = here()
    place = lambda j: (z ^ (j // ROW)) * ROW + ((y - j % ROW) & 3)
    r = lax.broadcasted_iota(jnp.int32, (HD, HD), 0)
    c = lax.broadcasted_iota(jnp.int32, (HD, HD), 1)
    same = (r // POS) == (c // POS)
    ones = lambda m: jnp.where(m, 1.0, 0.0).astype(BF)
    jr = lax.broadcasted_iota(jnp.int32, (2 * SP, SP), 0)
    jc = lax.broadcasted_iota(jnp.int32, (2 * SP, SP), 1)
    lane = lax.broadcasted_iota(jnp.int32, (1, HD), 1)
    log_weight = []
    total = []
    for g in range(2):
        order = (r > c) if g == 0 else (r < c)
        inside = jnp.concatenate((ones(same & order), ones(same)), axis=1)
        sums = sum(dot(p, inside) for p in three_parts(forget[g]))
        block = sums[:, HD:]
        across = ones(((place(jc) > place(jr)) if g == 0 else (place(jc) < place(jr))) | (jr >= SP))
        outside = sum(dot(across, p) for p in three_parts(block))
        log_weight.append(in_pre[g] + sums[:, :HD] + outside[:SP])
        total.append(outside[SP : SP + 1])
    stab = [
        jnp.maximum(total[g], group_max(jnp.max(log_weight[g], axis=0, keepdims=True), lane)) for g in range(2)
    ]
    weight = jnp.concatenate([jnp.exp(log_weight[g] - stab[g]) for g in range(2)], axis=0)
    weight_ref[...] = weight
    turned_ref[...] = weight.T

    shares = jnp.zeros((2 * OWN, HD), F32)
    numerator = jnp.zeros((4 * OWN, HD), F32)
    for j, blk in enumerate(blocks):
        share = jnp.concatenate([scores[j] * weight[g * SP + j : g * SP + j + 1] for g in range(2)], axis=0)
        shares += share
        numerator += dot(two_parts(share), blk[ROWS : 2 * ROWS, :])
    numerator = (numerator[: 2 * OWN] + numerator[2 * OWN :]) * scale
    denominator = jnp.sum(shares, axis=1, keepdims=True) * scale
    hidden = jnp.zeros((OWN, HD), F32)
    for g in range(2):
        at = slice(g * OWN, (g + 1) * OWN)
        column = jnp.max(jnp.where(mine, stab[g], -jnp.inf), axis=1, keepdims=True)
        stab_ref[g] = jnp.sum(jnp.where(lane8 == row, column, 0.0), axis=0, keepdims=True)[:, :OWN]
        hidden += numerator[at] / jnp.maximum(jnp.maximum(jnp.abs(denominator[at]), jnp.exp(-column)), 1.0)
    hidden = hidden.astype(BF)
    x = lax.axis_index("tp_0")
    core = lax.axis_index("tp_1")
    for k in range(TPX):
        first = ((x + k) % TPX) * 2
        for out_ref, which in ((keep_ref, core), (send_ref, 1 - core)):
            at = pl.multiple_of((first + which) * HD, HD)
            out_ref[k] = dot(hidden, wo_ref[:, pl.ds(at, HD)])


def weigh_kernel(*refs):
    blocks = landed(refs[:10])
    weight_ref, turned_ref, vw_ref, norm_ref = refs[10:]
    _, _, mine = rows_mine()
    norm = jnp.zeros((4 * OWN, HD), F32)
    for j, blk in enumerate(blocks):
        spread = [jnp.where(mine, weight_ref[g * SP + j : g * SP + j + 1, :], 0.0) for g in range(2)]
        norm += dot(two_parts(jnp.concatenate(spread, axis=0)), blk[:ROWS, :])
        value = blk[ROWS : 2 * ROWS, :].astype(F32)
        for g in range(2):
            k = g * SP + j
            vw_ref[j, :, g * HD : (g + 1) * HD] = (value * turned_ref[:, k : k + 1]).astype(BF)
    norm_ref[...] = (norm[: 2 * OWN] + norm[2 * OWN :]) * (HD ** -0.5)


def memory_kernel(*refs):
    blocks = landed(refs[:10])
    vw_ref, mem_ref = refs[10:]
    for s in range(OWN):
        at = slice(s * POS, (s + 1) * POS)
        keys = jnp.concatenate([blk[at, :] for blk in blocks], axis=0)
        values = vw_ref[:, at, :].reshape(SP * POS, 2 * HD)
        memory = (dot(keys, values, ((0,), (0,))) * (HD ** -0.5)).astype(BF)
        mem_ref[0, s] = memory[:, :HD]
        mem_ref[1, s] = memory[:, HD:]


def join_kernel(keep_ref, got_ref, *outs):
    for k, out in enumerate(outs):
        out[...] = keep_ref[k] + got_ref[k]


def sum_kernel(a_ref, b_ref, c_ref, d_ref, out_ref):
    out_ref[...] = ((a_ref[...] + b_ref[...]) + (c_ref[...] + d_ref[...])).astype(BF)


def shift(array, dz, dy):
    spots = [(z, y) for z in range(ROW) for y in range(ROW)]
    pairs = [(z * ROW + y, (z ^ dz) * ROW + (y + dy) % ROW) for z, y in spots]
    return lax.ppermute(array, "sp", pairs)


def across(array, axis, hop):
    size = lax.axis_size(axis)
    return lax.ppermute(array, axis, [(i, (i + hop) % size) for i in range(size)])


def step(prompt, w_key, w_value, w_in_gate, w_forget_gate, in_bias, forget_bias, query, w_out):
    hops = range(1, ROW)
    mirror, w, gates, later = project_near(
        prompt, w_key.reshape(D, HD), w_value.reshape(D, HD), w_in_gate.reshape(2, D), w_forget_gate.reshape(2, D)
    )
    mirror = shift(mirror, 3, 0)
    twin = run(second_kernel, block(ROW), (later, w, gates))
    twin = shift(twin, 1, 0)
    made = run(third_kernel, (block(),) * (2 * ROW), (later, w, gates))
    cross = [made[0]] + [shift(made[k], 0, k) for k in hops]
    own = [made[ROW]] + [shift(made[ROW + k], 0, k) for k in hops]
    far = run(gather_kernel, block(ROW), cross, 4)
    far = shift(far, 2, 0)
    side = run(legs_kernel, (block(2),) * 3, (mirror, twin), 4)
    side = [shift(blocks, 0, k) for k, blocks in zip(hops, side)]
    blocks = (*own, mirror, twin, *side, far)
    half = pltpu.VMEM((TPX, OWN, HD), F32)
    keep, send, weight, turned, stab = run(
        read_kernel,
        (half, half, pltpu.VMEM((2 * SP, HD), F32), pltpu.VMEM((HD, 2 * SP), F32),
         jax.ShapeDtypeStruct((2, 1, OWN), F32)),
        (*blocks, query.reshape(OWN, HD), w_out.reshape(HD, D), in_bias.reshape(1, 2), forget_bias.reshape(1, 2)),
    )
    got = across(send, "tp_1", 1)
    values, norm = run(
        weigh_kernel,
        (pltpu.VMEM((SP, ROWS, 2 * HD), BF), jax.ShapeDtypeStruct((2 * OWN, HD), F32)),
        (*blocks, weight, turned),
    )
    terms = run(join_kernel, (pltpu.VMEM((OWN, HD), F32),) * TPX, (keep, got), 4)
    terms = [terms[0]] + [across(terms[k], "tp_0", k) for k in range(1, TPX)]
    memory = run(memory_kernel, jax.ShapeDtypeStruct((2, OWN, HD, HD), BF), (*blocks, values))
    read = run(sum_kernel, jax.ShapeDtypeStruct((OWN, HD), BF), terms, 4)
    return (
        memory.reshape(2, OWN, 1, HD, HD),
        norm.reshape(2, OWN, 1, HD),
        stab.reshape(2, OWN, 1),
        read,
    )


def solution(mesh):
    torus = Mesh(
        mesh.devices.reshape(mesh.shape["gr"], mesh.shape["sp"], 4, 2), ("gr", "sp", "tp_0", "tp_1")
    )
    return jax.shard_map(
        step,
        mesh=torus,
        in_specs=(
            P("gr", "sp", None),
            P(None, TP, None),
            P(None, TP, None),
            P(None, None, TP),
            P(None, None, TP),
            P(None, TP),
            P(None, TP),
            P(("gr", "sp"), TP, None),
            P(TP, None, None),
        ),
        out_specs=(
            P(None, ("gr", "sp"), TP, None, None),
            P(None, ("gr", "sp"), TP, None),
            P(None, ("gr", "sp"), TP),
            P(("gr", "sp"), TP),
        ),
        check_vma=False,
    )
```

```python
import jax
import jax.numpy as jnp
from jax import lax
from jax.experimental import pallas as pl
from jax.experimental.pallas import tpu as pltpu
from jax.sharding import Mesh
from jax.sharding import PartitionSpec as P


TP = ("tp_0", "tp_1")
BF = jnp.bfloat16
F32 = jnp.float32
SP = 16
OWN = 8
POS = 16
ROWS = OWN * POS
HD = 128
D = 1024
SEND = 2 * ROWS + 8
ROW = 4
TPX = 4


def dot(a, b, dims=((1,), (0,))):
    return lax.dot_general(a, b, (dims, ((), ())), preferred_element_type=F32)


def here():
    at = lax.axis_index("sp")
    return at // ROW, at % ROW


def take(x_ref, buf_ref, sem_ref, sem, blocks):
    z, y = here()
    copies = []
    for i, (dz, dy) in enumerate(blocks):
        dest = (z ^ dz) * ROW + (y + dy) % ROW
        copies.append(pltpu.make_async_copy(x_ref.at[pl.ds(dest * OWN, OWN)], buf_ref.at[i], sem_ref.at[sem + i]))
    for copy in copies:
        copy.start()
    return copies


def project_blocks(buf_ref, first, w, gates, outs):
    rows = buf_ref[first : first + ROW].reshape(ROW * ROWS, D)
    both = dot(rows, w).astype(BF)
    pre = dot(gates, rows, ((1,), (1,)))[:4]
    high = pre.astype(BF).astype(F32)
    coded = jnp.concatenate((high, pre - high), axis=0).astype(BF)
    for k, out in enumerate(outs):
        at = slice(k * ROWS, (k + 1) * ROWS)
        out[:ROWS, :] = both[at, :HD]
        out[ROWS : 2 * ROWS, :] = both[at, HD:]
        out[2 * ROWS :, :] = coded[:, at]


def near_kernel(x_ref, wk_ref, wv_ref, wi_ref, wf_ref, mirror_ref, w_ref, g_ref, buf_ref, wi_buf, wf_buf, sem_ref):
    key_copy = pltpu.make_async_copy(wk_ref, w_ref.at[:, :HD], sem_ref.at[ROW])
    value_copy = pltpu.make_async_copy(wv_ref, w_ref.at[:, HD:], sem_ref.at[ROW + 1])
    gate_copies = [
        pltpu.make_async_copy(wi_ref, wi_buf, sem_ref.at[ROW + 2]),
        pltpu.make_async_copy(wf_ref, wf_buf, sem_ref.at[ROW + 3]),
    ]
    for copy in (*gate_copies, key_copy, value_copy):
        copy.start()
    copies = take(x_ref, buf_ref, sem_ref, 0, [(3, dy) for dy in range(ROW)])
    for copy in gate_copies:
        copy.wait()
    gates = jnp.concatenate((wi_buf[...].astype(F32), wf_buf[...].astype(F32), jnp.zeros((4, D), F32)), axis=0)
    g_ref[...] = gates.astype(BF)
    key_copy.wait()
    value_copy.wait()
    for copy in copies:
        copy.wait()
    project_blocks(buf_ref, 0, w_ref[...], g_ref[...], [mirror_ref.at[k] for k in range(ROW)])


def cross_kernel(x_ref, w_ref, g_ref, *refs):
    outs, (rest_ref, buf_ref, sem_ref) = refs[:ROW], refs[ROW:]
    copies = take(x_ref, buf_ref, sem_ref, 0, [(2, dy) for dy in range(ROW)])
    later = take(x_ref, rest_ref, sem_ref, ROW, [(dz, dy) for dz in (1, 0) for dy in range(ROW)])
    for copy in copies:
        copy.wait()
    project_blocks(buf_ref, 0, w_ref[...], g_ref[...], outs)
    for copy in later:
        copy.wait()


def twin_kernel(rest_ref, w_ref, g_ref, twin_ref):
    project_blocks(rest_ref, 0, w_ref[...], g_ref[...], [twin_ref.at[k] for k in range(ROW)])


def own_kernel(rest_ref, w_ref, g_ref, *outs):
    project_blocks(rest_ref, ROW, w_ref[...], g_ref[...], outs)


ANY = pl.BlockSpec(memory_space=pl.ANY)
VM = pl.BlockSpec(memory_space=pltpu.VMEM)


def vm(array):
    return pltpu.with_memory_space_constraint(array, pltpu.VMEM)


def grant(mib):
    return pltpu.CompilerParams(vmem_limit_bytes=mib << 20)


def block(*lead):
    return pltpu.VMEM((*lead, SEND, HD), BF)


def run(kernel, out_shape, args, mib=16, scratch=()):
    specs = jax.tree.map(lambda _: VM, out_shape, is_leaf=lambda s: hasattr(s, "shape"))
    return pl.pallas_call(
        kernel,
        in_specs=[VM] * len(args),
        out_specs=specs,
        out_shape=out_shape,
        scratch_shapes=list(scratch),
        compiler_params=grant(mib),
    )(*[vm(a) for a in args])


def project_near(*args):
    return pl.pallas_call(
        near_kernel,
        in_specs=[ANY] * 5,
        out_specs=[VM] * 3,
        out_shape=(
            block(ROW), pltpu.VMEM((D, 2 * HD), BF), pltpu.VMEM((8, D), BF)
        ),
        scratch_shapes=[
            pltpu.VMEM((ROW, OWN, POS, D), BF), pltpu.VMEM((2, D), BF), pltpu.VMEM((2, D), BF),
            pltpu.SemaphoreType.DMA((ROW + 4,)),
        ],
        compiler_params=grant(16),
        name="near",
    )(*[pltpu.with_memory_space_constraint(a, pltpu.HBM) for a in args])


def project_cross(prompt, w, gates):
    return pl.pallas_call(
        cross_kernel,
        in_specs=[ANY, VM, VM],
        out_specs=[VM] * (ROW + 1),
        out_shape=(block(),) * ROW + (pltpu.VMEM((2 * ROW, OWN, POS, D), BF),),
        scratch_shapes=[pltpu.VMEM((ROW, OWN, POS, D), BF), pltpu.SemaphoreType.DMA((3 * ROW,))],
        compiler_params=grant(16),
        name="cross",
    )(pltpu.with_memory_space_constraint(prompt, pltpu.HBM), vm(w), vm(gates))


def gather_kernel(*refs):
    for i in range(ROW):
        refs[ROW][i] = refs[i][...]


def legs_kernel(a_ref, b_ref, *outs):
    for k, out in enumerate(outs):
        out[0] = a_ref[k + 1]
        out[1] = b_ref[k + 1]


def three_parts(a):
    first = a.astype(BF)
    rest = a - first.astype(F32)
    second = rest.astype(BF)
    return first, second, (rest - second.astype(F32)).astype(BF)


def group_max(a, lane):
    for k in (1, 2, 4, 8):
        inside = (lane % POS) + k < POS
        a = jnp.maximum(a, jnp.where(inside, pltpu.roll(a, HD - k, 1), pltpu.roll(a, POS - k, 1)))
    return a


def log_sigmoid(a):
    return jnp.minimum(a, 0.0) - jnp.log1p(jnp.exp(-jnp.abs(a)))


def landed(refs):
    own, (mirror, twin, s1, s2, s3, far) = list(refs[:ROW]), refs[ROW:]
    from_mirror, from_twin = [
        [kept.at[0]] + [s.at[i] for s in (s1, s2, s3)] for i, kept in enumerate((mirror, twin))
    ]
    return own + from_twin + [far.at[k] for k in range(ROW)] + from_mirror


def rows_mine():
    row = lax.broadcasted_iota(jnp.int32, (OWN, HD), 0)
    lane = lax.broadcasted_iota(jnp.int32, (OWN, HD), 1)
    return row, lane, (lane // POS) == row


def two_parts(a):
    high = a.astype(BF)
    return jnp.concatenate((high, (a - high.astype(F32)).astype(BF)), axis=0)


def read_kernel(*refs):
    blocks = landed(refs[:10])
    q_ref, wo_ref, ib_ref, fb_ref, keep_ref, send_ref, weight_ref, turned_ref, stab_ref = refs[10:]
    scale = HD ** -0.5
    row, lane8, mine = rows_mine()
    query = q_ref[...]
    scores = [jnp.where(mine, dot(query, blk[:ROWS, :], ((1,), (1,))), 0.0) for blk in blocks]

    gates = jnp.stack([blk[2 * ROWS :, :].astype(F32) for blk in blocks])
    part = lambda c: gates[:, c, :] + gates[:, c + 4, :]
    in_pre = [part(g) + ib_ref[0:1, g : g + 1] for g in range(2)]
    forget = [log_sigmoid(part(2 + g) + fb_ref[0:1, g : g + 1]) for g in range(2)]

    z, y = here()
    place = lambda j: (z ^ (j // ROW)) * ROW + ((y - j % ROW) & 3)
    r = lax.broadcasted_iota(jnp.int32, (HD, HD), 0)
    c = lax.broadcasted_iota(jnp.int32, (HD, HD), 1)
    same = (r // POS) == (c // POS)
    ones = lambda m: jnp.where(m, 1.0, 0.0).astype(BF)
    jr = lax.broadcasted_iota(jnp.int32, (2 * SP, SP), 0)
    jc = lax.broadcasted_iota(jnp.int32, (2 * SP, SP), 1)
    lane = lax.broadcasted_iota(jnp.int32, (1, HD), 1)
    log_weight = []
    total = []
    for g in range(2):
        order = (r > c) if g == 0 else (r < c)
        inside = jnp.concatenate((ones(same & order), ones(same)), axis=1)
        sums = sum(dot(p, inside) for p in three_parts(forget[g]))
        block = sums[:, HD:]
        across = ones(((place(jc) > place(jr)) if g == 0 else (place(jc) < place(jr))) | (jr >= SP))
        outside = sum(dot(across, p) for p in three_parts(block))
        log_weight.append(in_pre[g] + sums[:, :HD] + outside[:SP])
        total.append(outside[SP : SP + 1])
    stab = [
        jnp.maximum(total[g], group_max(jnp.max(log_weight[g], axis=0, keepdims=True), lane)) for g in range(2)
    ]
    weight = jnp.concatenate([jnp.exp(log_weight[g] - stab[g]) for g in range(2)], axis=0)
    weight_ref[...] = weight
    turned_ref[...] = weight.T

    shares = jnp.zeros((2 * OWN, HD), F32)
    numerator = jnp.zeros((4 * OWN, HD), F32)
    for j, blk in enumerate(blocks):
        share = jnp.concatenate([scores[j] * weight[g * SP + j : g * SP + j + 1] for g in range(2)], axis=0)
        shares += share
        numerator += dot(two_parts(share), blk[ROWS : 2 * ROWS, :])
    numerator = (numerator[: 2 * OWN] + numerator[2 * OWN :]) * scale
    denominator = jnp.sum(shares, axis=1, keepdims=True) * scale
    hidden = jnp.zeros((OWN, HD), F32)
    for g in range(2):
        at = slice(g * OWN, (g + 1) * OWN)
        column = jnp.max(jnp.where(mine, stab[g], -jnp.inf), axis=1, keepdims=True)
        stab_ref[g] = jnp.sum(jnp.where(lane8 == row, column, 0.0), axis=0, keepdims=True)[:, :OWN]
        hidden += numerator[at] / jnp.maximum(jnp.maximum(jnp.abs(denominator[at]), jnp.exp(-column)), 1.0)
    hidden = hidden.astype(BF)
    x = lax.axis_index("tp_0")
    core = lax.axis_index("tp_1")
    for k in range(TPX):
        first = ((x + k) % TPX) * 2
        for out_ref, which in ((keep_ref, core), (send_ref, 1 - core)):
            at = pl.multiple_of((first + which) * HD, HD)
            out_ref[k] = dot(hidden, wo_ref[:, pl.ds(at, HD)])


def weigh_kernel(*refs):
    blocks = landed(refs[:10])
    weight_ref, turned_ref, vw_ref, norm_ref = refs[10:]
    _, _, mine = rows_mine()
    norm = jnp.zeros((4 * OWN, HD), F32)
    for j, blk in enumerate(blocks):
        spread = [jnp.where(mine, weight_ref[g * SP + j : g * SP + j + 1, :], 0.0) for g in range(2)]
        norm += dot(two_parts(jnp.concatenate(spread, axis=0)), blk[:ROWS, :])
        value = blk[ROWS : 2 * ROWS, :].astype(F32)
        for g in range(2):
            k = g * SP + j
            vw_ref[j, :, g * HD : (g + 1) * HD] = (value * turned_ref[:, k : k + 1]).astype(BF)
    norm_ref[...] = (norm[: 2 * OWN] + norm[2 * OWN :]) * (HD ** -0.5)


def memory_kernel(*refs):
    blocks = landed(refs[:10])
    vw_ref, mem_ref = refs[10:]
    for s in range(OWN):
        at = slice(s * POS, (s + 1) * POS)
        keys = jnp.concatenate([blk[at, :] for blk in blocks], axis=0)
        values = vw_ref[:, at, :].reshape(SP * POS, 2 * HD)
        memory = (dot(keys, values, ((0,), (0,))) * (HD ** -0.5)).astype(BF)
        mem_ref[0, s] = memory[:, :HD]
        mem_ref[1, s] = memory[:, HD:]


def join_kernel(keep_ref, got_ref, *outs):
    for k, out in enumerate(outs):
        out[...] = keep_ref[k] + got_ref[k]


def sum_kernel(a_ref, b_ref, c_ref, d_ref, out_ref):
    out_ref[...] = ((a_ref[...] + b_ref[...]) + (c_ref[...] + d_ref[...])).astype(BF)


def shift(array, dz, dy):
    spots = [(z, y) for z in range(ROW) for y in range(ROW)]
    pairs = [(z * ROW + y, (z ^ dz) * ROW + (y + dy) % ROW) for z, y in spots]
    return lax.ppermute(array, "sp", pairs)


def across(array, axis, hop):
    size = lax.axis_size(axis)
    return lax.ppermute(array, axis, [(i, (i + hop) % size) for i in range(size)])


def step(prompt, w_key, w_value, w_in_gate, w_forget_gate, in_bias, forget_bias, query, w_out):
    hops = range(1, ROW)
    mirror, w, gates = project_near(
        prompt, w_key.reshape(D, HD), w_value.reshape(D, HD), w_in_gate.reshape(2, D), w_forget_gate.reshape(2, D)
    )
    mirror = shift(mirror, 3, 0)
    *cross, later = project_cross(prompt, w, gates)
    cross = [cross[0]] + [shift(cross[k], 0, k) for k in hops]
    twin = run(twin_kernel, block(ROW), (later, w, gates))
    twin = shift(twin, 1, 0)
    far = run(gather_kernel, block(ROW), cross, 4)
    far = shift(far, 2, 0)
    own = run(own_kernel, (block(),) * ROW, (later, w, gates))
    own = [own[0]] + [shift(own[k], 0, k) for k in hops]
    side = run(legs_kernel, (block(2),) * 3, (mirror, twin), 4)
    side = [shift(blocks, 0, k) for k, blocks in zip(hops, side)]
    blocks = (*own, mirror, twin, *side, far)
    half = pltpu.VMEM((TPX, OWN, HD), F32)
    keep, send, weight, turned, stab = run(
        read_kernel,
        (half, half, pltpu.VMEM((2 * SP, HD), F32), pltpu.VMEM((HD, 2 * SP), F32),
         jax.ShapeDtypeStruct((2, 1, OWN), F32)),
        (*blocks, query.reshape(OWN, HD), w_out.reshape(HD, D), in_bias.reshape(1, 2), forget_bias.reshape(1, 2)),
    )
    got = across(send, "tp_1", 1)
    values, norm = run(
        weigh_kernel,
        (pltpu.VMEM((SP, ROWS, 2 * HD), BF), jax.ShapeDtypeStruct((2 * OWN, HD), F32)),
        (*blocks, weight, turned),
    )
    terms = run(join_kernel, (pltpu.VMEM((OWN, HD), F32),) * TPX, (keep, got), 4)
    terms = [terms[0]] + [across(terms[k], "tp_0", k) for k in range(1, TPX)]
    memory = run(memory_kernel, jax.ShapeDtypeStruct((2, OWN, HD, HD), BF), (*blocks, values))
    read = run(sum_kernel, jax.ShapeDtypeStruct((OWN, HD), BF), terms, 4)
    return (
        memory.reshape(2, OWN, 1, HD, HD),
        norm.reshape(2, OWN, 1, HD),
        stab.reshape(2, OWN, 1),
        read,
    )


def solution(mesh):
    torus = Mesh(
        mesh.devices.reshape(mesh.shape["gr"], mesh.shape["sp"], 4, 2), ("gr", "sp", "tp_0", "tp_1")
    )
    return jax.shard_map(
        step,
        mesh=torus,
        in_specs=(
            P("gr", "sp", None),
            P(None, TP, None),
            P(None, TP, None),
            P(None, None, TP),
            P(None, None, TP),
            P(None, TP),
            P(None, TP),
            P(("gr", "sp"), TP, None),
            P(TP, None, None),
        ),
        out_specs=(
            P(None, ("gr", "sp"), TP, None, None),
            P(None, ("gr", "sp"), TP, None),
            P(None, ("gr", "sp"), TP),
            P(("gr", "sp"), TP),
        ),
        check_vma=False,
    )
```

```python
import jax
import jax.numpy as jnp
from jax import lax
from jax.experimental import pallas as pl
from jax.experimental.pallas import tpu as pltpu
from jax.sharding import Mesh
from jax.sharding import PartitionSpec as P


TP = ("tp_0", "tp_1")
BF = jnp.bfloat16
F32 = jnp.float32
SP = 16
OWN = 8
POS = 16
ROWS = OWN * POS
HD = 128
D = 1024
SEND = 2 * ROWS + 8
ROW = 4
TPX = 4


def dot(a, b, dims=((1,), (0,))):
    return lax.dot_general(a, b, (dims, ((), ())), preferred_element_type=F32)


def here():
    at = lax.axis_index("sp")
    return at // ROW, at % ROW


def take(x_ref, buf_ref, sem_ref, sem, blocks):
    z, y = here()
    copies = []
    for i, (dz, dy) in enumerate(blocks):
        dest = (z ^ dz) * ROW + (y + dy) % ROW
        copies.append(pltpu.make_async_copy(x_ref.at[pl.ds(dest * OWN, OWN)], buf_ref.at[i], sem_ref.at[sem + i]))
    for copy in copies:
        copy.start()
    return copies


def project_blocks(buf_ref, first, w, gates, outs):
    rows = buf_ref[first : first + ROW].reshape(ROW * ROWS, D)
    both = dot(rows, w).astype(BF)
    pre = dot(gates, rows, ((1,), (1,)))[:4]
    high = pre.astype(BF).astype(F32)
    coded = jnp.concatenate((high, pre - high), axis=0).astype(BF)
    for k, out in enumerate(outs):
        at = slice(k * ROWS, (k + 1) * ROWS)
        out[:ROWS, :] = both[at, :HD]
        out[ROWS : 2 * ROWS, :] = both[at, HD:]
        out[2 * ROWS :, :] = coded[:, at]


def near_kernel(x_ref, wk_ref, wv_ref, wi_ref, wf_ref, mirror_ref, w_ref, g_ref, rest_ref, buf_ref, wi_buf, wf_buf, sem_ref):
    key_copy = pltpu.make_async_copy(wk_ref, w_ref.at[:, :HD], sem_ref.at[SP])
    value_copy = pltpu.make_async_copy(wv_ref, w_ref.at[:, HD:], sem_ref.at[SP + 1])
    gate_copies = [
        pltpu.make_async_copy(wi_ref, wi_buf, sem_ref.at[SP + 2]),
        pltpu.make_async_copy(wf_ref, wf_buf, sem_ref.at[SP + 3]),
    ]
    for copy in (*gate_copies, key_copy, value_copy):
        copy.start()
    copies = take(x_ref, buf_ref, sem_ref, 0, [(3, dy) for dy in range(ROW)])
    later = take(x_ref, rest_ref, sem_ref, ROW, [(dz, dy) for dz in (1, 2, 0) for dy in range(ROW)])
    for copy in gate_copies:
        copy.wait()
    gates = jnp.concatenate((wi_buf[...].astype(F32), wf_buf[...].astype(F32), jnp.zeros((4, D), F32)), axis=0)
    g_ref[...] = gates.astype(BF)
    key_copy.wait()
    value_copy.wait()
    for copy in copies:
        copy.wait()
    project_blocks(buf_ref, 0, w_ref[...], g_ref[...], [mirror_ref.at[k] for k in range(ROW)])
    for copy in later:
        copy.wait()


def second_kernel(rest_ref, w_ref, g_ref, twin_ref):
    project_blocks(rest_ref, 0, w_ref[...], g_ref[...], [twin_ref.at[k] for k in range(ROW)])


def third_kernel(rest_ref, w_ref, g_ref, *outs):
    project_blocks(rest_ref, ROW, w_ref[...], g_ref[...], outs)


def own_kernel(rest_ref, w_ref, g_ref, *outs):
    project_blocks(rest_ref, 2 * ROW, w_ref[...], g_ref[...], outs)


ANY = pl.BlockSpec(memory_space=pl.ANY)
VM = pl.BlockSpec(memory_space=pltpu.VMEM)


def vm(array):
    return pltpu.with_memory_space_constraint(array, pltpu.VMEM)


def grant(mib):
    return pltpu.CompilerParams(vmem_limit_bytes=mib << 20)


def block(*lead):
    return pltpu.VMEM((*lead, SEND, HD), BF)


def run(kernel, out_shape, args, mib=16, scratch=()):
    specs = jax.tree.map(lambda _: VM, out_shape, is_leaf=lambda s: hasattr(s, "shape"))
    return pl.pallas_call(
        kernel,
        in_specs=[VM] * len(args),
        out_specs=specs,
        out_shape=out_shape,
        scratch_shapes=list(scratch),
        compiler_params=grant(mib),
    )(*[vm(a) for a in args])


def project_near(*args):
    return pl.pallas_call(
        near_kernel,
        in_specs=[ANY] * 5,
        out_specs=[VM] * 4,
        out_shape=(
            block(ROW), pltpu.VMEM((D, 2 * HD), BF), pltpu.VMEM((8, D), BF), pltpu.VMEM((3 * ROW, OWN, POS, D), BF)
        ),
        scratch_shapes=[
            pltpu.VMEM((ROW, OWN, POS, D), BF), pltpu.VMEM((2, D), BF), pltpu.VMEM((2, D), BF),
            pltpu.SemaphoreType.DMA((SP + 4,)),
        ],
        compiler_params=grant(16),
        name="near",
    )(*[pltpu.with_memory_space_constraint(a, pltpu.HBM) for a in args])


def gather_kernel(*refs):
    for i in range(ROW):
        refs[ROW][i] = refs[i][...]


def legs_kernel(inner_ref, outer_ref, twin_ref, mirror0_ref, *outs):
    z, _ = here()
    edge = (z == 0) | (z == ROW - 1)

    def fill(mirror_ref):
        mirror0_ref[...] = mirror_ref[0]
        for k, out in enumerate(outs):
            out[0] = mirror_ref[k + 1]
            out[1] = twin_ref[k + 1]

    @pl.when(edge)
    def _():
        fill(outer_ref)

    @pl.when(jnp.logical_not(edge))
    def _():
        fill(inner_ref)


def three_parts(a):
    first = a.astype(BF)
    rest = a - first.astype(F32)
    second = rest.astype(BF)
    return first, second, (rest - second.astype(F32)).astype(BF)


def group_max(a, lane):
    for k in (1, 2, 4, 8):
        inside = (lane % POS) + k < POS
        a = jnp.maximum(a, jnp.where(inside, pltpu.roll(a, HD - k, 1), pltpu.roll(a, POS - k, 1)))
    return a


def log_sigmoid(a):
    return jnp.minimum(a, 0.0) - jnp.log1p(jnp.exp(-jnp.abs(a)))


def landed(refs):
    own, (mirror, twin, s1, s2, s3, far) = list(refs[:ROW]), refs[ROW:]
    sides = (s1, s2, s3)
    from_mirror = [mirror] + [s.at[0] for s in sides]
    from_twin = [twin.at[0]] + [s.at[1] for s in sides]
    return own + from_twin + [far.at[k] for k in range(ROW)] + from_mirror


def rows_mine():
    row = lax.broadcasted_iota(jnp.int32, (OWN, HD), 0)
    lane = lax.broadcasted_iota(jnp.int32, (OWN, HD), 1)
    return row, lane, (lane // POS) == row


def two_parts(a):
    high = a.astype(BF)
    return jnp.concatenate((high, (a - high.astype(F32)).astype(BF)), axis=0)


def read_kernel(*refs):
    blocks = landed(refs[:10])
    q_ref, wo_ref, ib_ref, fb_ref, keep_ref, send_ref, weight_ref, turned_ref, stab_ref = refs[10:]
    scale = HD ** -0.5
    row, lane8, mine = rows_mine()
    query = q_ref[...]
    scores = [jnp.where(mine, dot(query, blk[:ROWS, :], ((1,), (1,))), 0.0) for blk in blocks]

    gates = jnp.stack([blk[2 * ROWS :, :].astype(F32) for blk in blocks])
    part = lambda c: gates[:, c, :] + gates[:, c + 4, :]
    in_pre = [part(g) + ib_ref[0:1, g : g + 1] for g in range(2)]
    forget = [log_sigmoid(part(2 + g) + fb_ref[0:1, g : g + 1]) for g in range(2)]

    z, y = here()
    place = lambda j: (z ^ (j // ROW)) * ROW + ((y - j % ROW) & 3)
    r = lax.broadcasted_iota(jnp.int32, (HD, HD), 0)
    c = lax.broadcasted_iota(jnp.int32, (HD, HD), 1)
    same = (r // POS) == (c // POS)
    ones = lambda m: jnp.where(m, 1.0, 0.0).astype(BF)
    jr = lax.broadcasted_iota(jnp.int32, (2 * SP, SP), 0)
    jc = lax.broadcasted_iota(jnp.int32, (2 * SP, SP), 1)
    lane = lax.broadcasted_iota(jnp.int32, (1, HD), 1)
    log_weight = []
    total = []
    for g in range(2):
        order = (r > c) if g == 0 else (r < c)
        inside = jnp.concatenate((ones(same & order), ones(same)), axis=1)
        sums = sum(dot(p, inside) for p in three_parts(forget[g]))
        block = sums[:, HD:]
        across = ones(((place(jc) > place(jr)) if g == 0 else (place(jc) < place(jr))) | (jr >= SP))
        outside = sum(dot(across, p) for p in three_parts(block))
        log_weight.append(in_pre[g] + sums[:, :HD] + outside[:SP])
        total.append(outside[SP : SP + 1])
    stab = [
        jnp.maximum(total[g], group_max(jnp.max(log_weight[g], axis=0, keepdims=True), lane)) for g in range(2)
    ]
    weight = jnp.concatenate([jnp.exp(log_weight[g] - stab[g]) for g in range(2)], axis=0)
    weight_ref[...] = weight
    turned_ref[...] = weight.T

    shares = jnp.zeros((2 * OWN, HD), F32)
    numerator = jnp.zeros((4 * OWN, HD), F32)
    for j, blk in enumerate(blocks):
        share = jnp.concatenate([scores[j] * weight[g * SP + j : g * SP + j + 1] for g in range(2)], axis=0)
        shares += share
        numerator += dot(two_parts(share), blk[ROWS : 2 * ROWS, :])
    numerator = (numerator[: 2 * OWN] + numerator[2 * OWN :]) * scale
    denominator = jnp.sum(shares, axis=1, keepdims=True) * scale
    hidden = jnp.zeros((OWN, HD), F32)
    for g in range(2):
        at = slice(g * OWN, (g + 1) * OWN)
        column = jnp.max(jnp.where(mine, stab[g], -jnp.inf), axis=1, keepdims=True)
        stab_ref[g] = jnp.sum(jnp.where(lane8 == row, column, 0.0), axis=0, keepdims=True)[:, :OWN]
        hidden += numerator[at] / jnp.maximum(jnp.maximum(jnp.abs(denominator[at]), jnp.exp(-column)), 1.0)
    hidden = hidden.astype(BF)
    x = lax.axis_index("tp_0")
    core = lax.axis_index("tp_1")
    for k in range(TPX):
        first = ((x + k) % TPX) * 2
        for out_ref, which in ((keep_ref, core), (send_ref, 1 - core)):
            at = pl.multiple_of((first + which) * HD, HD)
            out_ref[k] = dot(hidden, wo_ref[:, pl.ds(at, HD)])


def weigh_kernel(*refs):
    blocks = landed(refs[:10])
    weight_ref, turned_ref, vw_ref, norm_ref = refs[10:]
    _, _, mine = rows_mine()
    norm = jnp.zeros((4 * OWN, HD), F32)
    for j, blk in enumerate(blocks):
        spread = [jnp.where(mine, weight_ref[g * SP + j : g * SP + j + 1, :], 0.0) for g in range(2)]
        norm += dot(two_parts(jnp.concatenate(spread, axis=0)), blk[:ROWS, :])
        value = blk[ROWS : 2 * ROWS, :].astype(F32)
        for g in range(2):
            k = g * SP + j
            vw_ref[j, :, g * HD : (g + 1) * HD] = (value * turned_ref[:, k : k + 1]).astype(BF)
    norm_ref[...] = (norm[: 2 * OWN] + norm[2 * OWN :]) * (HD ** -0.5)


def memory_kernel(*refs):
    blocks = landed(refs[:10])
    vw_ref, mem_ref = refs[10:]
    for s in range(OWN):
        at = slice(s * POS, (s + 1) * POS)
        keys = jnp.concatenate([blk[at, :] for blk in blocks], axis=0)
        values = vw_ref[:, at, :].reshape(SP * POS, 2 * HD)
        memory = (dot(keys, values, ((0,), (0,))) * (HD ** -0.5)).astype(BF)
        mem_ref[0, s] = memory[:, :HD]
        mem_ref[1, s] = memory[:, HD:]


def join_kernel(keep_ref, got_ref, *outs):
    for k, out in enumerate(outs):
        out[...] = keep_ref[k] + got_ref[k]


def sum_kernel(a_ref, b_ref, c_ref, d_ref, out_ref):
    out_ref[...] = ((a_ref[...] + b_ref[...]) + (c_ref[...] + d_ref[...])).astype(BF)


def shift(array, dz, dy, rows=range(ROW)):
    spots = [(z, y) for z in rows for y in range(ROW)]
    pairs = [(z * ROW + y, (z ^ dz) * ROW + (y + dy) % ROW) for z, y in spots]
    return lax.ppermute(array, "sp", pairs)


def across(array, axis, hop):
    size = lax.axis_size(axis)
    return lax.ppermute(array, axis, [(i, (i + hop) % size) for i in range(size)])


def step(prompt, w_key, w_value, w_in_gate, w_forget_gate, in_bias, forget_bias, query, w_out):
    hops = range(1, ROW)
    mirror, w, gates, later = project_near(
        prompt, w_key.reshape(D, HD), w_value.reshape(D, HD), w_in_gate.reshape(2, D), w_forget_gate.reshape(2, D)
    )
    inner = shift(mirror, 3, 0, (1, 2))
    outer = shift(mirror, 3, 0, (0, 3))
    twin = run(second_kernel, block(ROW), (later, w, gates))
    twin = shift(twin, 1, 0)
    cross = run(third_kernel, (block(),) * ROW, (later, w, gates))
    cross = [cross[0]] + [shift(cross[k], 0, k) for k in hops]
    own = run(own_kernel, (block(),) * ROW, (later, w, gates))
    own = [own[0]] + [shift(own[k], 0, k) for k in hops]
    far = run(gather_kernel, block(ROW), cross, 4)
    far = shift(far, 2, 0)
    mirror, *side = run(legs_kernel, (block(),) + (block(2),) * 3, (inner, outer, twin), 4)
    side = [shift(blocks, 0, k) for k, blocks in zip(hops, side)]
    blocks = (*own, mirror, twin, *side, far)
    half = pltpu.VMEM((TPX, OWN, HD), F32)
    keep, send, weight, turned, stab = run(
        read_kernel,
        (half, half, pltpu.VMEM((2 * SP, HD), F32), pltpu.VMEM((HD, 2 * SP), F32),
         jax.ShapeDtypeStruct((2, 1, OWN), F32)),
        (*blocks, query.reshape(OWN, HD), w_out.reshape(HD, D), in_bias.reshape(1, 2), forget_bias.reshape(1, 2)),
    )
    got = across(send, "tp_1", 1)
    values, norm = run(
        weigh_kernel,
        (pltpu.VMEM((SP, ROWS, 2 * HD), BF), jax.ShapeDtypeStruct((2 * OWN, HD), F32)),
        (*blocks, weight, turned),
    )
    terms = run(join_kernel, (pltpu.VMEM((OWN, HD), F32),) * TPX, (keep, got), 4)
    terms = [terms[0]] + [across(terms[k], "tp_0", k) for k in range(1, TPX)]
    memory = run(memory_kernel, jax.ShapeDtypeStruct((2, OWN, HD, HD), BF), (*blocks, values))
    read = run(sum_kernel, jax.ShapeDtypeStruct((OWN, HD), BF), terms, 4)
    return (
        memory.reshape(2, OWN, 1, HD, HD),
        norm.reshape(2, OWN, 1, HD),
        stab.reshape(2, OWN, 1),
        read,
    )


def solution(mesh):
    torus = Mesh(
        mesh.devices.reshape(mesh.shape["gr"], mesh.shape["sp"], 4, 2), ("gr", "sp", "tp_0", "tp_1")
    )
    return jax.shard_map(
        step,
        mesh=torus,
        in_specs=(
            P("gr", "sp", None),
            P(None, TP, None),
            P(None, TP, None),
            P(None, None, TP),
            P(None, None, TP),
            P(None, TP),
            P(None, TP),
            P(("gr", "sp"), TP, None),
            P(TP, None, None),
        ),
        out_specs=(
            P(None, ("gr", "sp"), TP, None, None),
            P(None, ("gr", "sp"), TP, None),
            P(None, ("gr", "sp"), TP),
            P(("gr", "sp"), TP),
        ),
        check_vma=False,
    )
```

```python
import jax
import jax.numpy as jnp
from jax import lax
from jax.experimental import pallas as pl
from jax.experimental.pallas import tpu as pltpu
from jax.sharding import Mesh
from jax.sharding import PartitionSpec as P


TP = ("tp_0", "tp_1")
BF = jnp.bfloat16
F32 = jnp.float32
SP = 16
OWN = 8
POS = 16
ROWS = OWN * POS
HD = 128
D = 1024
SEND = 2 * ROWS + 8
ROW = 4
TPX = 4


def dot(a, b, dims=((1,), (0,))):
    return lax.dot_general(a, b, (dims, ((), ())), preferred_element_type=F32)


def here():
    at = lax.axis_index("sp")
    return at // ROW, at % ROW


def take(x_ref, buf_ref, sem_ref, sem, blocks):
    z, y = here()
    copies = []
    for i, (dz, dy) in enumerate(blocks):
        dest = (z ^ dz) * ROW + (y + dy) % ROW
        copies.append(pltpu.make_async_copy(x_ref.at[pl.ds(dest * OWN, OWN)], buf_ref.at[i], sem_ref.at[sem + i]))
    for copy in copies:
        copy.start()
    return copies


def project_blocks(buf_ref, first, w, gates, outs):
    rows = buf_ref[first : first + ROW].reshape(ROW * ROWS, D)
    both = dot(rows, w).astype(BF)
    pre = dot(gates, rows, ((1,), (1,)))[:4]
    high = pre.astype(BF).astype(F32)
    coded = jnp.concatenate((high, pre - high), axis=0).astype(BF)
    for k, out in enumerate(outs):
        at = slice(k * ROWS, (k + 1) * ROWS)
        out[:ROWS, :] = both[at, :HD]
        out[ROWS : 2 * ROWS, :] = both[at, HD:]
        out[2 * ROWS :, :] = coded[:, at]


def near_kernel(x_ref, wk_ref, wv_ref, wi_ref, wf_ref, mirror_ref, w_ref, g_ref, rest_ref, buf_ref, wi_buf, wf_buf, sem_ref):
    key_copy = pltpu.make_async_copy(wk_ref, w_ref.at[:, :HD], sem_ref.at[SP])
    value_copy = pltpu.make_async_copy(wv_ref, w_ref.at[:, HD:], sem_ref.at[SP + 1])
    gate_copies = [
        pltpu.make_async_copy(wi_ref, wi_buf, sem_ref.at[SP + 2]),
        pltpu.make_async_copy(wf_ref, wf_buf, sem_ref.at[SP + 3]),
    ]
    for copy in (*gate_copies, key_copy, value_copy):
        copy.start()
    copies = take(x_ref, buf_ref, sem_ref, 0, [(3, dy) for dy in range(ROW)])
    later = take(x_ref, rest_ref, sem_ref, ROW, [(dz, dy) for dz in (2, 1, 0) for dy in range(ROW)])
    for copy in gate_copies:
        copy.wait()
    gates = jnp.concatenate((wi_buf[...].astype(F32), wf_buf[...].astype(F32), jnp.zeros((4, D), F32)), axis=0)
    g_ref[...] = gates.astype(BF)
    key_copy.wait()
    value_copy.wait()
    for copy in copies:
        copy.wait()
    project_blocks(buf_ref, 0, w_ref[...], g_ref[...], [mirror_ref.at[k] for k in range(ROW)])
    for copy in later:
        copy.wait()


def third_kernel(rest_ref, w_ref, g_ref, *outs):
    project_blocks(rest_ref, 0, w_ref[...], g_ref[...], outs)


def twin_kernel(rest_ref, w_ref, g_ref, twin_ref):
    project_blocks(rest_ref, ROW, w_ref[...], g_ref[...], [twin_ref.at[k] for k in range(ROW)])


def own_kernel(rest_ref, w_ref, g_ref, *refs):
    project_blocks(rest_ref, 2 * ROW, w_ref[...], g_ref[...], refs[:ROW])
    fill_masks(*refs[ROW:])


ANY = pl.BlockSpec(memory_space=pl.ANY)
VM = pl.BlockSpec(memory_space=pltpu.VMEM)


def vm(array):
    return pltpu.with_memory_space_constraint(array, pltpu.VMEM)


def grant(mib):
    return pltpu.CompilerParams(vmem_limit_bytes=mib << 20)


def block(*lead):
    return pltpu.VMEM((*lead, SEND, HD), BF)


def run(kernel, out_shape, args, mib=16, scratch=()):
    specs = jax.tree.map(lambda _: VM, out_shape, is_leaf=lambda s: hasattr(s, "shape"))
    return pl.pallas_call(
        kernel,
        in_specs=[VM] * len(args),
        out_specs=specs,
        out_shape=out_shape,
        scratch_shapes=list(scratch),
        compiler_params=grant(mib),
    )(*[vm(a) for a in args])


def project_near(*args):
    return pl.pallas_call(
        near_kernel,
        in_specs=[ANY] * 5,
        out_specs=[VM] * 4,
        out_shape=(
            block(ROW), pltpu.VMEM((D, 2 * HD), BF), pltpu.VMEM((8, D), BF), pltpu.VMEM((3 * ROW, OWN, POS, D), BF)
        ),
        scratch_shapes=[
            pltpu.VMEM((ROW, OWN, POS, D), BF), pltpu.VMEM((2, D), BF), pltpu.VMEM((2, D), BF),
            pltpu.SemaphoreType.DMA((SP + 4,)),
        ],
        compiler_params=grant(16),
        name="near",
    )(*[pltpu.with_memory_space_constraint(a, pltpu.HBM) for a in args])


def gather_kernel(*refs):
    for i in range(ROW):
        refs[ROW][i] = refs[i][...]


def legs_kernel(a_ref, b_ref, *outs):
    for k, out in enumerate(outs):
        out[0] = a_ref[k + 1]
        out[1] = b_ref[k + 1]


def fill_masks(inside_ref, across_ref):
    z, y = here()
    place = lambda j: (z ^ (j // ROW)) * ROW + ((y - j % ROW) & 3)
    r = lax.broadcasted_iota(jnp.int32, (HD, HD), 0)
    c = lax.broadcasted_iota(jnp.int32, (HD, HD), 1)
    same = (r // POS) == (c // POS)
    ones = lambda m: jnp.where(m, 1.0, 0.0).astype(BF)
    jr = lax.broadcasted_iota(jnp.int32, (2 * SP, SP), 0)
    jc = lax.broadcasted_iota(jnp.int32, (2 * SP, SP), 1)
    for g in range(2):
        inside_ref[g, :, :HD] = ones(same & ((r > c) if g == 0 else (r < c)))
        inside_ref[g, :, HD:] = ones(same)
        across_ref[g] = ones(((place(jc) > place(jr)) if g == 0 else (place(jc) < place(jr))) | (jr >= SP))


def three_parts(a):
    first = a.astype(BF)
    rest = a - first.astype(F32)
    second = rest.astype(BF)
    return first, second, (rest - second.astype(F32)).astype(BF)


def group_max(a, lane):
    for k in (1, 2, 4, 8):
        inside = (lane % POS) + k < POS
        a = jnp.maximum(a, jnp.where(inside, pltpu.roll(a, HD - k, 1), pltpu.roll(a, POS - k, 1)))
    return a


def log_sigmoid(a):
    return jnp.minimum(a, 0.0) - jnp.log1p(jnp.exp(-jnp.abs(a)))


def landed(refs):
    own, (mirror, twin, s1, s2, s3, far) = list(refs[:ROW]), refs[ROW:]
    from_mirror, from_twin = [
        [kept.at[0]] + [s.at[i] for s in (s1, s2, s3)] for i, kept in enumerate((mirror, twin))
    ]
    return own + from_twin + [far.at[k] for k in range(ROW)] + from_mirror


def rows_mine():
    row = lax.broadcasted_iota(jnp.int32, (OWN, HD), 0)
    lane = lax.broadcasted_iota(jnp.int32, (OWN, HD), 1)
    return row, lane, (lane // POS) == row


def two_parts(a):
    high = a.astype(BF)
    return jnp.concatenate((high, (a - high.astype(F32)).astype(BF)), axis=0)


def read_kernel(*refs):
    blocks = landed(refs[:10])
    q_ref, wo_ref, ib_ref, fb_ref, inside_ref, across_ref, keep_ref, send_ref, weight_ref, turned_ref, stab_ref = refs[10:]
    scale = HD ** -0.5
    row, lane8, mine = rows_mine()
    query = q_ref[...]
    scores = [jnp.where(mine, dot(query, blk[:ROWS, :], ((1,), (1,))), 0.0) for blk in blocks]

    gates = jnp.stack([blk[2 * ROWS :, :].astype(F32) for blk in blocks])
    part = lambda c: gates[:, c, :] + gates[:, c + 4, :]
    in_pre = [part(g) + ib_ref[0:1, g : g + 1] for g in range(2)]
    forget = [log_sigmoid(part(2 + g) + fb_ref[0:1, g : g + 1]) for g in range(2)]

    lane = lax.broadcasted_iota(jnp.int32, (1, HD), 1)
    log_weight = []
    total = []
    for g in range(2):
        sums = sum(dot(p, inside_ref[g]) for p in three_parts(forget[g]))
        block = sums[:, HD:]
        outside = sum(dot(across_ref[g], p) for p in three_parts(block))
        log_weight.append(in_pre[g] + sums[:, :HD] + outside[:SP])
        total.append(outside[SP : SP + 1])
    stab = [
        jnp.maximum(total[g], group_max(jnp.max(log_weight[g], axis=0, keepdims=True), lane)) for g in range(2)
    ]
    weight = jnp.concatenate([jnp.exp(log_weight[g] - stab[g]) for g in range(2)], axis=0)
    weight_ref[...] = weight
    turned_ref[...] = weight.T

    shares = jnp.zeros((2 * OWN, HD), F32)
    numerator = jnp.zeros((4 * OWN, HD), F32)
    for j, blk in enumerate(blocks):
        share = jnp.concatenate([scores[j] * weight[g * SP + j : g * SP + j + 1] for g in range(2)], axis=0)
        shares += share
        numerator += dot(two_parts(share), blk[ROWS : 2 * ROWS, :])
    numerator = (numerator[: 2 * OWN] + numerator[2 * OWN :]) * scale
    denominator = jnp.sum(shares, axis=1, keepdims=True) * scale
    hidden = jnp.zeros((OWN, HD), F32)
    for g in range(2):
        at = slice(g * OWN, (g + 1) * OWN)
        column = jnp.max(jnp.where(mine, stab[g], -jnp.inf), axis=1, keepdims=True)
        stab_ref[g] = jnp.sum(jnp.where(lane8 == row, column, 0.0), axis=0, keepdims=True)[:, :OWN]
        hidden += numerator[at] / jnp.maximum(jnp.maximum(jnp.abs(denominator[at]), jnp.exp(-column)), 1.0)
    hidden = hidden.astype(BF)
    x = lax.axis_index("tp_0")
    core = lax.axis_index("tp_1")
    for k in range(TPX):
        first = ((x + k) % TPX) * 2
        for out_ref, which in ((keep_ref, core), (send_ref, 1 - core)):
            at = pl.multiple_of((first + which) * HD, HD)
            out_ref[k] = dot(hidden, wo_ref[:, pl.ds(at, HD)])


def weigh_kernel(*refs):
    blocks = landed(refs[:10])
    weight_ref, turned_ref, vw_ref, norm_ref = refs[10:]
    _, _, mine = rows_mine()
    norm = jnp.zeros((4 * OWN, HD), F32)
    for j, blk in enumerate(blocks):
        spread = [jnp.where(mine, weight_ref[g * SP + j : g * SP + j + 1, :], 0.0) for g in range(2)]
        norm += dot(two_parts(jnp.concatenate(spread, axis=0)), blk[:ROWS, :])
        value = blk[ROWS : 2 * ROWS, :].astype(F32)
        for g in range(2):
            k = g * SP + j
            vw_ref[j, :, g * HD : (g + 1) * HD] = (value * turned_ref[:, k : k + 1]).astype(BF)
    norm_ref[...] = (norm[: 2 * OWN] + norm[2 * OWN :]) * (HD ** -0.5)


def memory_kernel(*refs):
    blocks = landed(refs[:10])
    vw_ref, mem_ref = refs[10:]
    for s in range(OWN):
        at = slice(s * POS, (s + 1) * POS)
        keys = jnp.concatenate([blk[at, :] for blk in blocks], axis=0)
        values = vw_ref[:, at, :].reshape(SP * POS, 2 * HD)
        memory = (dot(keys, values, ((0,), (0,))) * (HD ** -0.5)).astype(BF)
        mem_ref[0, s] = memory[:, :HD]
        mem_ref[1, s] = memory[:, HD:]


def join_kernel(keep_ref, got_ref, *outs):
    for k, out in enumerate(outs):
        out[...] = keep_ref[k] + got_ref[k]


def sum_kernel(a_ref, b_ref, c_ref, d_ref, out_ref):
    out_ref[...] = ((a_ref[...] + b_ref[...]) + (c_ref[...] + d_ref[...])).astype(BF)


def shift(array, dz, dy):
    spots = [(z, y) for z in range(ROW) for y in range(ROW)]
    pairs = [(z * ROW + y, (z ^ dz) * ROW + (y + dy) % ROW) for z, y in spots]
    return lax.ppermute(array, "sp", pairs)


def across(array, axis, hop):
    size = lax.axis_size(axis)
    return lax.ppermute(array, axis, [(i, (i + hop) % size) for i in range(size)])


def step(prompt, w_key, w_value, w_in_gate, w_forget_gate, in_bias, forget_bias, query, w_out):
    hops = range(1, ROW)
    mirror, w, gates, later = project_near(
        prompt, w_key.reshape(D, HD), w_value.reshape(D, HD), w_in_gate.reshape(2, D), w_forget_gate.reshape(2, D)
    )
    mirror = shift(mirror, 3, 0)
    cross = run(third_kernel, (block(),) * ROW, (later, w, gates))
    cross = [cross[0]] + [shift(cross[k], 0, k) for k in hops]
    twin = run(twin_kernel, block(ROW), (later, w, gates))
    twin = shift(twin, 1, 0)
    far = run(gather_kernel, block(ROW), cross, 4)
    far = shift(far, 2, 0)
    masks = (pltpu.VMEM((2, HD, 2 * HD), BF), pltpu.VMEM((2, 2 * SP, SP), BF))
    *own, inside, outside = run(own_kernel, (block(),) * ROW + masks, (later, w, gates))
    masks = (inside, outside)
    own = [own[0]] + [shift(own[k], 0, k) for k in hops]
    side = run(legs_kernel, (block(2),) * 3, (mirror, twin), 4)
    side = [shift(blocks, 0, k) for k, blocks in zip(hops, side)]
    blocks = (*own, mirror, twin, *side, far)
    half = pltpu.VMEM((TPX, OWN, HD), F32)
    keep, send, weight, turned, stab = run(
        read_kernel,
        (half, half, pltpu.VMEM((2 * SP, HD), F32), pltpu.VMEM((HD, 2 * SP), F32),
         jax.ShapeDtypeStruct((2, 1, OWN), F32)),
        (*blocks, query.reshape(OWN, HD), w_out.reshape(HD, D), in_bias.reshape(1, 2), forget_bias.reshape(1, 2),
         *masks),
    )
    got = across(send, "tp_1", 1)
    values, norm = run(
        weigh_kernel,
        (pltpu.VMEM((SP, ROWS, 2 * HD), BF), jax.ShapeDtypeStruct((2 * OWN, HD), F32)),
        (*blocks, weight, turned),
    )
    terms = run(join_kernel, (pltpu.VMEM((OWN, HD), F32),) * TPX, (keep, got), 4)
    terms = [terms[0]] + [across(terms[k], "tp_0", k) for k in range(1, TPX)]
    memory = run(memory_kernel, jax.ShapeDtypeStruct((2, OWN, HD, HD), BF), (*blocks, values))
    read = run(sum_kernel, jax.ShapeDtypeStruct((OWN, HD), BF), terms, 4)
    return (
        memory.reshape(2, OWN, 1, HD, HD),
        norm.reshape(2, OWN, 1, HD),
        stab.reshape(2, OWN, 1),
        read,
    )


def solution(mesh):
    torus = Mesh(
        mesh.devices.reshape(mesh.shape["gr"], mesh.shape["sp"], 4, 2), ("gr", "sp", "tp_0", "tp_1")
    )
    return jax.shard_map(
        step,
        mesh=torus,
        in_specs=(
            P("gr", "sp", None),
            P(None, TP, None),
            P(None, TP, None),
            P(None, None, TP),
            P(None, None, TP),
            P(None, TP),
            P(None, TP),
            P(("gr", "sp"), TP, None),
            P(TP, None, None),
        ),
        out_specs=(
            P(None, ("gr", "sp"), TP, None, None),
            P(None, ("gr", "sp"), TP, None),
            P(None, ("gr", "sp"), TP),
            P(("gr", "sp"), TP),
        ),
        check_vma=False,
    )
```

```python
import jax
import jax.numpy as jnp
from jax import lax
from jax.experimental import pallas as pl
from jax.experimental.pallas import tpu as pltpu
from jax.sharding import Mesh
from jax.sharding import PartitionSpec as P


TP = ("tp_0", "tp_1")
BF = jnp.bfloat16
F32 = jnp.float32
SP = 16
OWN = 8
POS = 16
ROWS = OWN * POS
HD = 128
D = 1024
SEND = 2 * ROWS + 8
ROW = 4
TPX = 4


def dot(a, b, dims=((1,), (0,))):
    return lax.dot_general(a, b, (dims, ((), ())), preferred_element_type=F32)


def here():
    at = lax.axis_index("sp")
    return at // ROW, at % ROW


def take(x_ref, buf_ref, sem_ref, sem, blocks):
    z, y = here()
    copies = []
    for i, (dz, dy) in enumerate(blocks):
        dest = (z ^ dz) * ROW + (y + dy) % ROW
        copies.append(pltpu.make_async_copy(x_ref.at[pl.ds(dest * OWN, OWN)], buf_ref.at[i], sem_ref.at[sem + i]))
    for copy in copies:
        copy.start()
    return copies


def project_blocks(buf_ref, first, w, gates, outs):
    rows = buf_ref[first : first + ROW].reshape(ROW * ROWS, D)
    both = dot(rows, w).astype(BF)
    pre = dot(gates, rows, ((1,), (1,)))[:4]
    high = pre.astype(BF).astype(F32)
    coded = jnp.concatenate((high, pre - high), axis=0).astype(BF)
    for k, out in enumerate(outs):
        at = slice(k * ROWS, (k + 1) * ROWS)
        out[:ROWS, :] = both[at, :HD]
        out[ROWS : 2 * ROWS, :] = both[at, HD:]
        out[2 * ROWS :, :] = coded[:, at]


def near_kernel(x_ref, wk_ref, wv_ref, wi_ref, wf_ref, mirror_ref, w_ref, g_ref, rest_ref, buf_ref, wi_buf, wf_buf, sem_ref):
    key_copy = pltpu.make_async_copy(wk_ref, w_ref.at[:, :HD], sem_ref.at[SP])
    value_copy = pltpu.make_async_copy(wv_ref, w_ref.at[:, HD:], sem_ref.at[SP + 1])
    gate_copies = [
        pltpu.make_async_copy(wi_ref, wi_buf, sem_ref.at[SP + 2]),
        pltpu.make_async_copy(wf_ref, wf_buf, sem_ref.at[SP + 3]),
    ]
    for copy in (*gate_copies, key_copy, value_copy):
        copy.start()
    copies = take(x_ref, buf_ref, sem_ref, 0, [(3, dy) for dy in range(ROW)])
    later = take(x_ref, rest_ref, sem_ref, ROW, [(dz, dy) for dz in (1, 2, 0) for dy in range(ROW)])
    for copy in gate_copies:
        copy.wait()
    gates = jnp.concatenate((wi_buf[...].astype(F32), wf_buf[...].astype(F32), jnp.zeros((4, D), F32)), axis=0)
    g_ref[...] = gates.astype(BF)
    key_copy.wait()
    value_copy.wait()
    for copy in copies:
        copy.wait()
    project_blocks(buf_ref, 0, w_ref[...], g_ref[...], [mirror_ref.at[k] for k in range(ROW)])
    for copy in later:
        copy.wait()


def second_kernel(rest_ref, w_ref, g_ref, twin_ref):
    project_blocks(rest_ref, 0, w_ref[...], g_ref[...], [twin_ref.at[k] for k in range(ROW)])


def third_kernel(rest_ref, w_ref, g_ref, *outs):
    project_blocks(rest_ref, ROW, w_ref[...], g_ref[...], outs)


def own_kernel(rest_ref, w_ref, g_ref, *outs):
    project_blocks(rest_ref, 2 * ROW, w_ref[...], g_ref[...], outs)


ANY = pl.BlockSpec(memory_space=pl.ANY)
VM = pl.BlockSpec(memory_space=pltpu.VMEM)


def vm(array):
    return pltpu.with_memory_space_constraint(array, pltpu.VMEM)


def grant(mib):
    return pltpu.CompilerParams(vmem_limit_bytes=mib << 20)


def block(*lead):
    return pltpu.VMEM((*lead, SEND, HD), BF)


def run(kernel, out_shape, args, mib=16, scratch=()):
    specs = jax.tree.map(lambda _: VM, out_shape, is_leaf=lambda s: hasattr(s, "shape"))
    return pl.pallas_call(
        kernel,
        in_specs=[VM] * len(args),
        out_specs=specs,
        out_shape=out_shape,
        scratch_shapes=list(scratch),
        compiler_params=grant(mib),
    )(*[vm(a) for a in args])


def project_near(*args):
    return pl.pallas_call(
        near_kernel,
        in_specs=[ANY] * 5,
        out_specs=[VM] * 4,
        out_shape=(
            block(ROW), pltpu.VMEM((D, 2 * HD), BF), pltpu.VMEM((8, D), BF), pltpu.VMEM((3 * ROW, OWN, POS, D), BF)
        ),
        scratch_shapes=[
            pltpu.VMEM((ROW, OWN, POS, D), BF), pltpu.VMEM((2, D), BF), pltpu.VMEM((2, D), BF),
            pltpu.SemaphoreType.DMA((SP + 4,)),
        ],
        compiler_params=grant(16),
        name="near",
    )(*[pltpu.with_memory_space_constraint(a, pltpu.HBM) for a in args])


def gather_kernel(*refs):
    for i in range(ROW):
        refs[ROW][i] = refs[i][...]


def legs_kernel(a_ref, b_ref, own3_ref, *outs):
    for k, out in enumerate(outs):
        out[0] = a_ref[k + 1]
        out[1] = b_ref[k + 1]
    outs[2][2] = own3_ref[...]


def three_parts(a):
    first = a.astype(BF)
    rest = a - first.astype(F32)
    second = rest.astype(BF)
    return first, second, (rest - second.astype(F32)).astype(BF)


def group_max(a, lane):
    for k in (1, 2, 4, 8):
        inside = (lane % POS) + k < POS
        a = jnp.maximum(a, jnp.where(inside, pltpu.roll(a, HD - k, 1), pltpu.roll(a, POS - k, 1)))
    return a


def log_sigmoid(a):
    return jnp.minimum(a, 0.0) - jnp.log1p(jnp.exp(-jnp.abs(a)))


def landed(refs):
    own0, o1, o2, mirror, twin, s1, s2, s3, far = refs
    own = [own0, o1, o2, s3.at[2]]
    from_mirror, from_twin = [
        [kept.at[0]] + [s.at[i] for s in (s1, s2, s3)] for i, kept in enumerate((mirror, twin))
    ]
    return own + from_twin + [far.at[k] for k in range(ROW)] + from_mirror


def rows_mine():
    row = lax.broadcasted_iota(jnp.int32, (OWN, HD), 0)
    lane = lax.broadcasted_iota(jnp.int32, (OWN, HD), 1)
    return row, lane, (lane // POS) == row


def two_parts(a):
    high = a.astype(BF)
    return jnp.concatenate((high, (a - high.astype(F32)).astype(BF)), axis=0)


def read_kernel(*refs):
    blocks = landed(refs[:9])
    q_ref, wo_ref, ib_ref, fb_ref, keep_ref, send_ref, weight_ref, turned_ref, stab_ref = refs[9:]
    scale = HD ** -0.5
    row, lane8, mine = rows_mine()
    query = q_ref[...]
    scores = [jnp.where(mine, dot(query, blk[:ROWS, :], ((1,), (1,))), 0.0) for blk in blocks]

    gates = jnp.stack([blk[2 * ROWS :, :].astype(F32) for blk in blocks])
    part = lambda c: gates[:, c, :] + gates[:, c + 4, :]
    in_pre = [part(g) + ib_ref[0:1, g : g + 1] for g in range(2)]
    forget = [log_sigmoid(part(2 + g) + fb_ref[0:1, g : g + 1]) for g in range(2)]

    z, y = here()
    place = lambda j: (z ^ (j // ROW)) * ROW + ((y - j % ROW) & 3)
    r = lax.broadcasted_iota(jnp.int32, (HD, HD), 0)
    c = lax.broadcasted_iota(jnp.int32, (HD, HD), 1)
    same = (r // POS) == (c // POS)
    ones = lambda m: jnp.where(m, 1.0, 0.0).astype(BF)
    jr = lax.broadcasted_iota(jnp.int32, (2 * SP, SP), 0)
    jc = lax.broadcasted_iota(jnp.int32, (2 * SP, SP), 1)
    lane = lax.broadcasted_iota(jnp.int32, (1, HD), 1)
    log_weight = []
    total = []
    for g in range(2):
        order = (r > c) if g == 0 else (r < c)
        inside = jnp.concatenate((ones(same & order), ones(same)), axis=1)
        sums = sum(dot(p, inside) for p in three_parts(forget[g]))
        block = sums[:, HD:]
        across = ones(((place(jc) > place(jr)) if g == 0 else (place(jc) < place(jr))) | (jr >= SP))
        outside = sum(dot(across, p) for p in three_parts(block))
        log_weight.append(in_pre[g] + sums[:, :HD] + outside[:SP])
        total.append(outside[SP : SP + 1])
    stab = [
        jnp.maximum(total[g], group_max(jnp.max(log_weight[g], axis=0, keepdims=True), lane)) for g in range(2)
    ]
    weight = jnp.concatenate([jnp.exp(log_weight[g] - stab[g]) for g in range(2)], axis=0)
    weight_ref[...] = weight
    turned_ref[...] = weight.T

    shares = jnp.zeros((2 * OWN, HD), F32)
    numerator = jnp.zeros((4 * OWN, HD), F32)
    for j, blk in enumerate(blocks):
        share = jnp.concatenate([scores[j] * weight[g * SP + j : g * SP + j + 1] for g in range(2)], axis=0)
        shares += share
        numerator += dot(two_parts(share), blk[ROWS : 2 * ROWS, :])
    numerator = (numerator[: 2 * OWN] + numerator[2 * OWN :]) * scale
    denominator = jnp.sum(shares, axis=1, keepdims=True) * scale
    hidden = jnp.zeros((OWN, HD), F32)
    for g in range(2):
        at = slice(g * OWN, (g + 1) * OWN)
        column = jnp.max(jnp.where(mine, stab[g], -jnp.inf), axis=1, keepdims=True)
        stab_ref[g] = jnp.sum(jnp.where(lane8 == row, column, 0.0), axis=0, keepdims=True)[:, :OWN]
        hidden += numerator[at] / jnp.maximum(jnp.maximum(jnp.abs(denominator[at]), jnp.exp(-column)), 1.0)
    hidden = hidden.astype(BF)
    x = lax.axis_index("tp_0")
    core = lax.axis_index("tp_1")
    for k in range(TPX):
        first = ((x + k) % TPX) * 2
        for out_ref, which in ((keep_ref, core), (send_ref, 1 - core)):
            at = pl.multiple_of((first + which) * HD, HD)
            out_ref[k] = dot(hidden, wo_ref[:, pl.ds(at, HD)])


def weigh_kernel(*refs):
    blocks = landed(refs[:9])
    weight_ref, turned_ref, vw_ref, norm_ref = refs[9:]
    _, _, mine = rows_mine()
    norm = jnp.zeros((4 * OWN, HD), F32)
    for j, blk in enumerate(blocks):
        spread = [jnp.where(mine, weight_ref[g * SP + j : g * SP + j + 1, :], 0.0) for g in range(2)]
        norm += dot(two_parts(jnp.concatenate(spread, axis=0)), blk[:ROWS, :])
        value = blk[ROWS : 2 * ROWS, :].astype(F32)
        for g in range(2):
            k = g * SP + j
            vw_ref[j, :, g * HD : (g + 1) * HD] = (value * turned_ref[:, k : k + 1]).astype(BF)
    norm_ref[...] = (norm[: 2 * OWN] + norm[2 * OWN :]) * (HD ** -0.5)


def memory_kernel(*refs):
    blocks = landed(refs[:9])
    vw_ref, mem_ref = refs[9:]
    for s in range(OWN):
        at = slice(s * POS, (s + 1) * POS)
        keys = jnp.concatenate([blk[at, :] for blk in blocks], axis=0)
        values = vw_ref[:, at, :].reshape(SP * POS, 2 * HD)
        memory = (dot(keys, values, ((0,), (0,))) * (HD ** -0.5)).astype(BF)
        mem_ref[0, s] = memory[:, :HD]
        mem_ref[1, s] = memory[:, HD:]


def join_kernel(keep_ref, got_ref, *outs):
    for k, out in enumerate(outs):
        out[...] = keep_ref[k] + got_ref[k]


def sum_kernel(a_ref, b_ref, c_ref, d_ref, out_ref):
    out_ref[...] = ((a_ref[...] + b_ref[...]) + (c_ref[...] + d_ref[...])).astype(BF)


def shift(array, dz, dy):
    spots = [(z, y) for z in range(ROW) for y in range(ROW)]
    pairs = [(z * ROW + y, (z ^ dz) * ROW + (y + dy) % ROW) for z, y in spots]
    return lax.ppermute(array, "sp", pairs)


def across(array, axis, hop):
    size = lax.axis_size(axis)
    return lax.ppermute(array, axis, [(i, (i + hop) % size) for i in range(size)])


def step(prompt, w_key, w_value, w_in_gate, w_forget_gate, in_bias, forget_bias, query, w_out):
    hops = range(1, ROW)
    mirror, w, gates, later = project_near(
        prompt, w_key.reshape(D, HD), w_value.reshape(D, HD), w_in_gate.reshape(2, D), w_forget_gate.reshape(2, D)
    )
    mirror = shift(mirror, 3, 0)
    twin = run(second_kernel, block(ROW), (later, w, gates))
    twin = shift(twin, 1, 0)
    cross = run(third_kernel, (block(),) * ROW, (later, w, gates))
    cross = [cross[0]] + [shift(cross[k], 0, k) for k in hops]
    far = run(gather_kernel, block(ROW), cross, 4)
    far = shift(far, 2, 0)
    *own, own3 = run(own_kernel, (block(),) * ROW, (later, w, gates))
    own = [own[0]] + [shift(own[k], 0, k) for k in (1, 2)]
    side = run(legs_kernel, (block(2), block(2), block(3)), (mirror, twin, own3), 4)
    side = [shift(blocks, 0, k) for k, blocks in zip(hops, side)]
    blocks = (*own, mirror, twin, *side, far)
    half = pltpu.VMEM((TPX, OWN, HD), F32)
    keep, send, weight, turned, stab = run(
        read_kernel,
        (half, half, pltpu.VMEM((2 * SP, HD), F32), pltpu.VMEM((HD, 2 * SP), F32),
         jax.ShapeDtypeStruct((2, 1, OWN), F32)),
        (*blocks, query.reshape(OWN, HD), w_out.reshape(HD, D), in_bias.reshape(1, 2), forget_bias.reshape(1, 2)),
    )
    got = across(send, "tp_1", 1)
    values, norm = run(
        weigh_kernel,
        (pltpu.VMEM((SP, ROWS, 2 * HD), BF), jax.ShapeDtypeStruct((2 * OWN, HD), F32)),
        (*blocks, weight, turned),
    )
    terms = run(join_kernel, (pltpu.VMEM((OWN, HD), F32),) * TPX, (keep, got), 4)
    terms = [terms[0]] + [across(terms[k], "tp_0", k) for k in range(1, TPX)]
    memory = run(memory_kernel, jax.ShapeDtypeStruct((2, OWN, HD, HD), BF), (*blocks, values))
    read = run(sum_kernel, jax.ShapeDtypeStruct((OWN, HD), BF), terms, 4)
    return (
        memory.reshape(2, OWN, 1, HD, HD),
        norm.reshape(2, OWN, 1, HD),
        stab.reshape(2, OWN, 1),
        read,
    )


def solution(mesh):
    torus = Mesh(
        mesh.devices.reshape(mesh.shape["gr"], mesh.shape["sp"], 4, 2), ("gr", "sp", "tp_0", "tp_1")
    )
    return jax.shard_map(
        step,
        mesh=torus,
        in_specs=(
            P("gr", "sp", None),
            P(None, TP, None),
            P(None, TP, None),
            P(None, None, TP),
            P(None, None, TP),
            P(None, TP),
            P(None, TP),
            P(("gr", "sp"), TP, None),
            P(TP, None, None),
        ),
        out_specs=(
            P(None, ("gr", "sp"), TP, None, None),
            P(None, ("gr", "sp"), TP, None),
            P(None, ("gr", "sp"), TP),
            P(("gr", "sp"), TP),
        ),
        check_vma=False,
    )
```

```python
import jax
import jax.numpy as jnp
from jax import lax
from jax.experimental import pallas as pl
from jax.experimental.pallas import tpu as pltpu
from jax.sharding import Mesh
from jax.sharding import PartitionSpec as P


TP = ("tp_0", "tp_1")
BF = jnp.bfloat16
F32 = jnp.float32
SP = 16
OWN = 8
POS = 16
ROWS = OWN * POS
HD = 128
D = 1024
SEND = 2 * ROWS + 8
ROW = 4
TPX = 4


def dot(a, b, dims=((1,), (0,))):
    return lax.dot_general(a, b, (dims, ((), ())), preferred_element_type=F32)


def here():
    at = lax.axis_index("sp")
    return at // ROW, at % ROW


def take(x_ref, buf_ref, sem_ref, sem, blocks):
    z, y = here()
    copies = []
    for i, (dz, dy) in enumerate(blocks):
        dest = (z ^ dz) * ROW + (y + dy) % ROW
        copies.append(pltpu.make_async_copy(x_ref.at[pl.ds(dest * OWN, OWN)], buf_ref.at[i], sem_ref.at[sem + i]))
    for copy in copies:
        copy.start()
    return copies


def project_blocks(buf_ref, first, w, gates, outs):
    rows = buf_ref[first : first + ROW].reshape(ROW * ROWS, D)
    both = dot(rows, w).astype(BF)
    pre = dot(gates, rows, ((1,), (1,)))[:4]
    high = pre.astype(BF).astype(F32)
    coded = jnp.concatenate((high, pre - high), axis=0).astype(BF)
    for k, out in enumerate(outs):
        at = slice(k * ROWS, (k + 1) * ROWS)
        out[:ROWS, :] = both[at, :HD]
        out[ROWS : 2 * ROWS, :] = both[at, HD:]
        out[2 * ROWS :, :] = coded[:, at]


def near_kernel(x_ref, wk_ref, wv_ref, wi_ref, wf_ref, mirror_ref, w_ref, g_ref, rest_ref, buf_ref, wi_buf, wf_buf, sem_ref):
    key_copy = pltpu.make_async_copy(wk_ref, w_ref.at[:, :HD], sem_ref.at[SP])
    value_copy = pltpu.make_async_copy(wv_ref, w_ref.at[:, HD:], sem_ref.at[SP + 1])
    gate_copies = [
        pltpu.make_async_copy(wi_ref, wi_buf, sem_ref.at[SP + 2]),
        pltpu.make_async_copy(wf_ref, wf_buf, sem_ref.at[SP + 3]),
    ]
    for copy in (*gate_copies, key_copy, value_copy):
        copy.start()
    copies = take(x_ref, buf_ref, sem_ref, 0, [(3, dy) for dy in range(ROW)])
    later = take(x_ref, rest_ref, sem_ref, ROW, [(dz, dy) for dz in (1, 2, 0) for dy in range(ROW)])
    for copy in gate_copies:
        copy.wait()
    gates = jnp.concatenate((wi_buf[...].astype(F32), wf_buf[...].astype(F32), jnp.zeros((4, D), F32)), axis=0)
    g_ref[...] = gates.astype(BF)
    key_copy.wait()
    value_copy.wait()
    for copy in copies:
        copy.wait()
    project_blocks(buf_ref, 0, w_ref[...], g_ref[...], [mirror_ref.at[k] for k in range(ROW)])
    for copy in later:
        copy.wait()


def second_kernel(rest_ref, w_ref, g_ref, twin_ref):
    project_blocks(rest_ref, 0, w_ref[...], g_ref[...], [twin_ref.at[k] for k in range(ROW)])


def third_kernel(rest_ref, w_ref, g_ref, *outs):
    project_blocks(rest_ref, ROW, w_ref[...], g_ref[...], outs)


def own_kernel(rest_ref, w_ref, g_ref, *outs):
    project_blocks(rest_ref, 2 * ROW, w_ref[...], g_ref[...], outs)


ANY = pl.BlockSpec(memory_space=pl.ANY)
VM = pl.BlockSpec(memory_space=pltpu.VMEM)


def vm(array):
    return pltpu.with_memory_space_constraint(array, pltpu.VMEM)


def grant(mib):
    return pltpu.CompilerParams(vmem_limit_bytes=mib << 20)


def block(*lead):
    return pltpu.VMEM((*lead, SEND, HD), BF)


def run(kernel, out_shape, args, mib=16, scratch=()):
    specs = jax.tree.map(lambda _: VM, out_shape, is_leaf=lambda s: hasattr(s, "shape"))
    return pl.pallas_call(
        kernel,
        in_specs=[VM] * len(args),
        out_specs=specs,
        out_shape=out_shape,
        scratch_shapes=list(scratch),
        compiler_params=grant(mib),
    )(*[vm(a) for a in args])


def project_near(*args):
    return pl.pallas_call(
        near_kernel,
        in_specs=[ANY] * 5,
        out_specs=[VM] * 4,
        out_shape=(
            block(ROW), pltpu.VMEM((D, 2 * HD), BF), pltpu.VMEM((8, D), BF), pltpu.VMEM((3 * ROW, OWN, POS, D), BF)
        ),
        scratch_shapes=[
            pltpu.VMEM((ROW, OWN, POS, D), BF), pltpu.VMEM((2, D), BF), pltpu.VMEM((2, D), BF),
            pltpu.SemaphoreType.DMA((SP + 4,)),
        ],
        compiler_params=grant(16),
        name="near",
    )(*[pltpu.with_memory_space_constraint(a, pltpu.HBM) for a in args])


def gather_kernel(*refs):
    for i in range(ROW):
        refs[ROW][i] = refs[i][...]


def pair_kernel(a_ref, b_ref, *outs):
    for k, out in enumerate(outs):
        out[0] = a_ref[k + 1]
        out[1] = b_ref[k + 1]


def three_parts(a):
    first = a.astype(BF)
    rest = a - first.astype(F32)
    second = rest.astype(BF)
    return first, second, (rest - second.astype(F32)).astype(BF)


def group_max(a, lane):
    for k in (1, 2, 4, 8):
        inside = (lane % POS) + k < POS
        a = jnp.maximum(a, jnp.where(inside, pltpu.roll(a, HD - k, 1), pltpu.roll(a, POS - k, 1)))
    return a


def log_sigmoid(a):
    return jnp.minimum(a, 0.0) - jnp.log1p(jnp.exp(-jnp.abs(a)))


def landed(refs):
    own, (mirror, twin, s1, s2, s3, far) = list(refs[:ROW]), refs[ROW:]
    from_mirror = [mirror.at[0]] + [s.at[0] for s in (s1, s2, s3)]
    from_twin = [twin.at[0]] + [s.at[1] for s in (s1, s2, s3)]
    return own + from_twin + [far.at[k] for k in range(ROW)] + from_mirror


def rows_mine():
    row = lax.broadcasted_iota(jnp.int32, (OWN, HD), 0)
    lane = lax.broadcasted_iota(jnp.int32, (OWN, HD), 1)
    return row, lane, (lane // POS) == row


def two_parts(a):
    high = a.astype(BF)
    return jnp.concatenate((high, (a - high.astype(F32)).astype(BF)), axis=0)


def read_kernel(*refs):
    blocks = landed(refs[:10])
    q_ref, wo_ref, ib_ref, fb_ref, keep_ref, send_ref, weight_ref, turned_ref, stab_ref = refs[10:]
    scale = HD ** -0.5
    row, lane8, mine = rows_mine()
    query = q_ref[...]
    scores = [jnp.where(mine, dot(query, blk[:ROWS, :], ((1,), (1,))), 0.0) for blk in blocks]

    gates = jnp.stack([blk[2 * ROWS :, :].astype(F32) for blk in blocks])
    part = lambda c: gates[:, c, :] + gates[:, c + 4, :]
    in_pre = [part(g) + ib_ref[0:1, g : g + 1] for g in range(2)]
    forget = [log_sigmoid(part(2 + g) + fb_ref[0:1, g : g + 1]) for g in range(2)]

    z, y = here()
    place = lambda j: (z ^ (j // ROW)) * ROW + ((y - j % ROW) & 3)
    r = lax.broadcasted_iota(jnp.int32, (HD, HD), 0)
    c = lax.broadcasted_iota(jnp.int32, (HD, HD), 1)
    same = (r // POS) == (c // POS)
    ones = lambda m: jnp.where(m, 1.0, 0.0).astype(BF)
    jr = lax.broadcasted_iota(jnp.int32, (2 * SP, SP), 0)
    jc = lax.broadcasted_iota(jnp.int32, (2 * SP, SP), 1)
    lane = lax.broadcasted_iota(jnp.int32, (1, HD), 1)
    log_weight = []
    total = []
    for g in range(2):
        order = (r > c) if g == 0 else (r < c)
        inside = jnp.concatenate((ones(same & order), ones(same)), axis=1)
        sums = sum(dot(p, inside) for p in three_parts(forget[g]))
        block = sums[:, HD:]
        across = ones(((place(jc) > place(jr)) if g == 0 else (place(jc) < place(jr))) | (jr >= SP))
        outside = sum(dot(across, p) for p in three_parts(block))
        log_weight.append(in_pre[g] + sums[:, :HD] + outside[:SP])
        total.append(outside[SP : SP + 1])
    stab = [
        jnp.maximum(total[g], group_max(jnp.max(log_weight[g], axis=0, keepdims=True), lane)) for g in range(2)
    ]
    weight = jnp.concatenate([jnp.exp(log_weight[g] - stab[g]) for g in range(2)], axis=0)
    weight_ref[...] = weight
    turned_ref[...] = weight.T

    shares = jnp.zeros((2 * OWN, HD), F32)
    numerator = jnp.zeros((4 * OWN, HD), F32)
    for j, blk in enumerate(blocks):
        share = jnp.concatenate([scores[j] * weight[g * SP + j : g * SP + j + 1] for g in range(2)], axis=0)
        shares += share
        numerator += dot(two_parts(share), blk[ROWS : 2 * ROWS, :])
    numerator = (numerator[: 2 * OWN] + numerator[2 * OWN :]) * scale
    denominator = jnp.sum(shares, axis=1, keepdims=True) * scale
    hidden = jnp.zeros((OWN, HD), F32)
    for g in range(2):
        at = slice(g * OWN, (g + 1) * OWN)
        column = jnp.max(jnp.where(mine, stab[g], -jnp.inf), axis=1, keepdims=True)
        stab_ref[g] = jnp.sum(jnp.where(lane8 == row, column, 0.0), axis=0, keepdims=True)[:, :OWN]
        hidden += numerator[at] / jnp.maximum(jnp.maximum(jnp.abs(denominator[at]), jnp.exp(-column)), 1.0)
    hidden = hidden.astype(BF)
    x = lax.axis_index("tp_0")
    core = lax.axis_index("tp_1")
    for k in range(TPX):
        first = ((x + k) % TPX) * 2
        for out_ref, which in ((keep_ref, core), (send_ref, 1 - core)):
            at = pl.multiple_of((first + which) * HD, HD)
            out_ref[k] = dot(hidden, wo_ref[:, pl.ds(at, HD)])


def weigh_kernel(*refs):
    blocks = landed(refs[:10])
    weight_ref, turned_ref, vw_ref, norm_ref = refs[10:]
    _, _, mine = rows_mine()
    norm = jnp.zeros((4 * OWN, HD), F32)
    for j, blk in enumerate(blocks):
        spread = [jnp.where(mine, weight_ref[g * SP + j : g * SP + j + 1, :], 0.0) for g in range(2)]
        norm += dot(two_parts(jnp.concatenate(spread, axis=0)), blk[:ROWS, :])
        value = blk[ROWS : 2 * ROWS, :].astype(F32)
        for g in range(2):
            k = g * SP + j
            vw_ref[j, :, g * HD : (g + 1) * HD] = (value * turned_ref[:, k : k + 1]).astype(BF)
    norm_ref[...] = (norm[: 2 * OWN] + norm[2 * OWN :]) * (HD ** -0.5)


def memory_kernel(*refs):
    blocks = landed(refs[:10])
    vw_ref, mem_ref = refs[10:]
    for s in range(OWN):
        at = slice(s * POS, (s + 1) * POS)
        keys = jnp.concatenate([blk[at, :] for blk in blocks], axis=0)
        values = vw_ref[:, at, :].reshape(SP * POS, 2 * HD)
        memory = (dot(keys, values, ((0,), (0,))) * (HD ** -0.5)).astype(BF)
        mem_ref[0, s] = memory[:, :HD]
        mem_ref[1, s] = memory[:, HD:]


def join_kernel(keep_ref, got_ref, *outs):
    for k, out in enumerate(outs):
        out[...] = keep_ref[k] + got_ref[k]


def sum_kernel(a_ref, b_ref, c_ref, d_ref, out_ref):
    out_ref[...] = ((a_ref[...] + b_ref[...]) + (c_ref[...] + d_ref[...])).astype(BF)


def shift(array, dz, dy):
    spots = [(z, y) for z in range(ROW) for y in range(ROW)]
    pairs = [(z * ROW + y, (z ^ dz) * ROW + (y + dy) % ROW) for z, y in spots]
    return lax.ppermute(array, "sp", pairs)


def across(array, axis, hop):
    size = lax.axis_size(axis)
    return lax.ppermute(array, axis, [(i, (i + hop) % size) for i in range(size)])


def step(prompt, w_key, w_value, w_in_gate, w_forget_gate, in_bias, forget_bias, query, w_out):
    hops = range(1, ROW)
    mirror, w, gates, later = project_near(
        prompt, w_key.reshape(D, HD), w_value.reshape(D, HD), w_in_gate.reshape(2, D), w_forget_gate.reshape(2, D)
    )
    mirror = shift(mirror, 3, 0)
    twin = run(second_kernel, block(ROW), (later, w, gates))
    twin = shift(twin, 1, 0)
    cross = run(third_kernel, (block(),) * ROW, (later, w, gates))
    cross = [cross[0]] + [shift(cross[k], 0, k) for k in hops]
    far = run(gather_kernel, block(ROW), cross, 4)
    far = shift(far, 2, 0)
    own = run(own_kernel, (block(),) * ROW, (later, w, gates))
    own = [own[0]] + [shift(own[k], 0, k) for k in hops]
    side = run(pair_kernel, (block(2),) * 3, (mirror, twin), 4)
    side = [shift(blocks, 0, k) for k, blocks in zip(hops, side)]
    blocks = (*own, mirror, twin, *side, far)
    half = pltpu.VMEM((TPX, OWN, HD), F32)
    keep, send, weight, turned, stab = run(
        read_kernel,
        (half, half, pltpu.VMEM((2 * SP, HD), F32), pltpu.VMEM((HD, 2 * SP), F32),
         jax.ShapeDtypeStruct((2, 1, OWN), F32)),
        (*blocks, query.reshape(OWN, HD), w_out.reshape(HD, D), in_bias.reshape(1, 2), forget_bias.reshape(1, 2)),
    )
    got = across(send, "tp_1", 1)
    values, norm = run(
        weigh_kernel,
        (pltpu.VMEM((SP, ROWS, 2 * HD), BF), jax.ShapeDtypeStruct((2 * OWN, HD), F32)),
        (*blocks, weight, turned),
    )
    terms = run(join_kernel, (pltpu.VMEM((OWN, HD), F32),) * TPX, (keep, got), 4)
    terms = [terms[0]] + [across(terms[k], "tp_0", k) for k in range(1, TPX)]
    memory = run(memory_kernel, jax.ShapeDtypeStruct((2, OWN, HD, HD), BF), (*blocks, values))
    read = run(sum_kernel, jax.ShapeDtypeStruct((OWN, HD), BF), terms, 4)
    return (
        memory.reshape(2, OWN, 1, HD, HD),
        norm.reshape(2, OWN, 1, HD),
        stab.reshape(2, OWN, 1),
        read,
    )


def solution(mesh):
    torus = Mesh(
        mesh.devices.reshape(mesh.shape["gr"], mesh.shape["sp"], 4, 2), ("gr", "sp", "tp_0", "tp_1")
    )
    return jax.shard_map(
        step,
        mesh=torus,
        in_specs=(
            P("gr", "sp", None),
            P(None, TP, None),
            P(None, TP, None),
            P(None, None, TP),
            P(None, None, TP),
            P(None, TP),
            P(None, TP),
            P(("gr", "sp"), TP, None),
            P(TP, None, None),
        ),
        out_specs=(
            P(None, ("gr", "sp"), TP, None, None),
            P(None, ("gr", "sp"), TP, None),
            P(None, ("gr", "sp"), TP),
            P(("gr", "sp"), TP),
        ),
        check_vma=False,
    )
```

```python
import jax
import jax.numpy as jnp
from jax import lax
from jax.experimental import pallas as pl
from jax.experimental.pallas import tpu as pltpu
from jax.sharding import Mesh
from jax.sharding import PartitionSpec as P


TP = ("tp_0", "tp_1")
BF = jnp.bfloat16
F32 = jnp.float32
SP = 16
OWN = 8
POS = 16
ROWS = OWN * POS
HD = 128
D = 1024
SEND = 2 * ROWS + 8
ROW = 4
TPX = 4


def dot(a, b, dims=((1,), (0,))):
    return lax.dot_general(a, b, (dims, ((), ())), preferred_element_type=F32)


def here():
    at = lax.axis_index("sp")
    return at // ROW, at % ROW


def take(x_ref, buf_ref, sem_ref, sem, blocks):
    z, y = here()
    copies = []
    for i, (dz, dy) in enumerate(blocks):
        dest = (z ^ dz) * ROW + (y + dy) % ROW
        copies.append(pltpu.make_async_copy(x_ref.at[pl.ds(dest * OWN, OWN)], buf_ref.at[i], sem_ref.at[sem + i]))
    for copy in copies:
        copy.start()
    return copies


def project_blocks(buf_ref, first, w, gates, outs):
    rows = buf_ref[first : first + ROW].reshape(ROW * ROWS, D)
    both = dot(rows, w).astype(BF)
    pre = dot(gates, rows, ((1,), (1,)))[:4]
    high = pre.astype(BF).astype(F32)
    coded = jnp.concatenate((high, pre - high), axis=0).astype(BF)
    for k, out in enumerate(outs):
        at = slice(k * ROWS, (k + 1) * ROWS)
        out[:ROWS, :] = both[at, :HD]
        out[ROWS : 2 * ROWS, :] = both[at, HD:]
        out[2 * ROWS :, :] = coded[:, at]


def near_kernel(x_ref, wk_ref, wv_ref, wi_ref, wf_ref, mirror_ref, w_ref, g_ref, rest_ref, buf_ref, wi_buf, wf_buf, sem_ref):
    key_copy = pltpu.make_async_copy(wk_ref, w_ref.at[:, :HD], sem_ref.at[SP])
    value_copy = pltpu.make_async_copy(wv_ref, w_ref.at[:, HD:], sem_ref.at[SP + 1])
    gate_copies = [
        pltpu.make_async_copy(wi_ref, wi_buf, sem_ref.at[SP + 2]),
        pltpu.make_async_copy(wf_ref, wf_buf, sem_ref.at[SP + 3]),
    ]
    for copy in (*gate_copies, key_copy, value_copy):
        copy.start()
    copies = take(x_ref, buf_ref, sem_ref, 0, [(3, dy) for dy in range(ROW)])
    later = take(x_ref, rest_ref, sem_ref, ROW, [(dz, dy) for dz in (1, 2) for dy in range(ROW)])
    for copy in gate_copies:
        copy.wait()
    gates = jnp.concatenate((wi_buf[...].astype(F32), wf_buf[...].astype(F32), jnp.zeros((4, D), F32)), axis=0)
    g_ref[...] = gates.astype(BF)
    key_copy.wait()
    value_copy.wait()
    for copy in copies:
        copy.wait()
    project_blocks(buf_ref, 0, w_ref[...], g_ref[...], [mirror_ref.at[k] for k in range(ROW)])
    for copy in later:
        copy.wait()


def second_kernel(rest_ref, w_ref, g_ref, twin_ref):
    project_blocks(rest_ref, 0, w_ref[...], g_ref[...], [twin_ref.at[k] for k in range(ROW)])


def third_kernel(rest_ref, w_ref, g_ref, *outs):
    project_blocks(rest_ref, ROW, w_ref[...], g_ref[...], outs)


def own_kernel(x_ref, w_ref, g_ref, *refs):
    outs, (buf_ref, sem_ref) = refs[:ROW], refs[ROW:]
    for copy in take(x_ref, buf_ref, sem_ref, 0, [(0, dy) for dy in range(ROW)]):
        copy.wait()
    project_blocks(buf_ref, 0, w_ref[...], g_ref[...], outs)


ANY = pl.BlockSpec(memory_space=pl.ANY)
VM = pl.BlockSpec(memory_space=pltpu.VMEM)


def vm(array):
    return pltpu.with_memory_space_constraint(array, pltpu.VMEM)


def grant(mib):
    return pltpu.CompilerParams(vmem_limit_bytes=mib << 20)


def block(*lead):
    return pltpu.VMEM((*lead, SEND, HD), BF)


def run(kernel, out_shape, args, mib=16, scratch=()):
    specs = jax.tree.map(lambda _: VM, out_shape, is_leaf=lambda s: hasattr(s, "shape"))
    return pl.pallas_call(
        kernel,
        in_specs=[VM] * len(args),
        out_specs=specs,
        out_shape=out_shape,
        scratch_shapes=list(scratch),
        compiler_params=grant(mib),
    )(*[vm(a) for a in args])


def project_near(*args):
    return pl.pallas_call(
        near_kernel,
        in_specs=[ANY] * 5,
        out_specs=[VM] * 4,
        out_shape=(
            block(ROW), pltpu.VMEM((D, 2 * HD), BF), pltpu.VMEM((8, D), BF), pltpu.VMEM((2 * ROW, OWN, POS, D), BF)
        ),
        scratch_shapes=[
            pltpu.VMEM((ROW, OWN, POS, D), BF), pltpu.VMEM((2, D), BF), pltpu.VMEM((2, D), BF),
            pltpu.SemaphoreType.DMA((SP + 4,)),
        ],
        compiler_params=grant(16),
        name="near",
    )(*[pltpu.with_memory_space_constraint(a, pltpu.HBM) for a in args])


def project_own(prompt, w, gates):
    return pl.pallas_call(
        own_kernel,
        in_specs=[ANY, VM, VM],
        out_specs=[VM] * ROW,
        out_shape=(block(),) * ROW,
        scratch_shapes=[pltpu.VMEM((ROW, OWN, POS, D), BF), pltpu.SemaphoreType.DMA((ROW,))],
        compiler_params=grant(16),
        name="own",
    )(pltpu.with_memory_space_constraint(prompt, pltpu.HBM), vm(w), vm(gates))


def gather_kernel(*refs):
    for i in range(ROW):
        refs[ROW][i] = refs[i][...]


def pair_kernel(a_ref, b_ref, *outs):
    for k, out in enumerate(outs):
        out[0] = a_ref[k + 1]
        out[1] = b_ref[k + 1]


def three_parts(a):
    first = a.astype(BF)
    rest = a - first.astype(F32)
    second = rest.astype(BF)
    return first, second, (rest - second.astype(F32)).astype(BF)


def group_max(a, lane):
    for k in (1, 2, 4, 8):
        inside = (lane % POS) + k < POS
        a = jnp.maximum(a, jnp.where(inside, pltpu.roll(a, HD - k, 1), pltpu.roll(a, POS - k, 1)))
    return a


def log_sigmoid(a):
    return jnp.minimum(a, 0.0) - jnp.log1p(jnp.exp(-jnp.abs(a)))


def landed(refs):
    own, (mirror, twin, s1, s2, s3, far) = list(refs[:ROW]), refs[ROW:]
    from_mirror = [mirror.at[0]] + [s.at[0] for s in (s1, s2, s3)]
    from_twin = [twin.at[0]] + [s.at[1] for s in (s1, s2, s3)]
    return own + from_twin + [far.at[k] for k in range(ROW)] + from_mirror


def rows_mine():
    row = lax.broadcasted_iota(jnp.int32, (OWN, HD), 0)
    lane = lax.broadcasted_iota(jnp.int32, (OWN, HD), 1)
    return row, lane, (lane // POS) == row


def two_parts(a):
    high = a.astype(BF)
    return jnp.concatenate((high, (a - high.astype(F32)).astype(BF)), axis=0)


def read_kernel(*refs):
    blocks = landed(refs[:10])
    q_ref, wo_ref, ib_ref, fb_ref, keep_ref, send_ref, weight_ref, turned_ref, stab_ref = refs[10:]
    scale = HD ** -0.5
    row, lane8, mine = rows_mine()
    query = q_ref[...]
    scores = []
    for a, b in zip(blocks[::2], blocks[1::2]):
        both = dot(query, jnp.concatenate((a[:ROWS, :], b[:ROWS, :]), axis=0), ((1,), (1,)))
        scores += [jnp.where(mine, both[:, :HD], 0.0), jnp.where(mine, both[:, HD:], 0.0)]

    gates = jnp.stack([blk[2 * ROWS :, :].astype(F32) for blk in blocks])
    part = lambda c: gates[:, c, :] + gates[:, c + 4, :]
    in_pre = [part(g) + ib_ref[0:1, g : g + 1] for g in range(2)]
    forget = [log_sigmoid(part(2 + g) + fb_ref[0:1, g : g + 1]) for g in range(2)]

    z, y = here()
    place = lambda j: (z ^ (j // ROW)) * ROW + ((y - j % ROW) & 3)
    r = lax.broadcasted_iota(jnp.int32, (HD, HD), 0)
    c = lax.broadcasted_iota(jnp.int32, (HD, HD), 1)
    same = (r // POS) == (c // POS)
    ones = lambda m: jnp.where(m, 1.0, 0.0).astype(BF)
    jr = lax.broadcasted_iota(jnp.int32, (2 * SP, SP), 0)
    jc = lax.broadcasted_iota(jnp.int32, (2 * SP, SP), 1)
    lane = lax.broadcasted_iota(jnp.int32, (1, HD), 1)
    log_weight = []
    total = []
    for g in range(2):
        order = (r > c) if g == 0 else (r < c)
        inside = jnp.concatenate((ones(same & order), ones(same)), axis=1)
        sums = sum(dot(p, inside) for p in three_parts(forget[g]))
        block = sums[:, HD:]
        across = ones(((place(jc) > place(jr)) if g == 0 else (place(jc) < place(jr))) | (jr >= SP))
        outside = sum(dot(across, p) for p in three_parts(block))
        log_weight.append(in_pre[g] + sums[:, :HD] + outside[:SP])
        total.append(outside[SP : SP + 1])
    stab = [
        jnp.maximum(total[g], group_max(jnp.max(log_weight[g], axis=0, keepdims=True), lane)) for g in range(2)
    ]
    weight = jnp.concatenate([jnp.exp(log_weight[g] - stab[g]) for g in range(2)], axis=0)
    weight_ref[...] = weight
    turned_ref[...] = weight.T

    shares = jnp.zeros((2 * OWN, HD), F32)
    numerator = jnp.zeros((4 * OWN, HD), F32)
    for j in range(0, SP, 2):
        pair = [
            jnp.concatenate([scores[i] * weight[g * SP + i : g * SP + i + 1] for g in range(2)], axis=0)
            for i in (j, j + 1)
        ]
        shares += pair[0] + pair[1]
        values = jnp.concatenate([blocks[i][ROWS : 2 * ROWS, :] for i in (j, j + 1)], axis=0)
        numerator += dot(jnp.concatenate([two_parts(share) for share in pair], axis=1), values)
    numerator = (numerator[: 2 * OWN] + numerator[2 * OWN :]) * scale
    denominator = jnp.sum(shares, axis=1, keepdims=True) * scale
    hidden = jnp.zeros((OWN, HD), F32)
    for g in range(2):
        at = slice(g * OWN, (g + 1) * OWN)
        column = jnp.max(jnp.where(mine, stab[g], -jnp.inf), axis=1, keepdims=True)
        stab_ref[g] = jnp.sum(jnp.where(lane8 == row, column, 0.0), axis=0, keepdims=True)[:, :OWN]
        hidden += numerator[at] / jnp.maximum(jnp.maximum(jnp.abs(denominator[at]), jnp.exp(-column)), 1.0)
    hidden = hidden.astype(BF)
    x = lax.axis_index("tp_0")
    core = lax.axis_index("tp_1")
    for k in range(TPX):
        first = ((x + k) % TPX) * 2
        for out_ref, which in ((keep_ref, core), (send_ref, 1 - core)):
            at = pl.multiple_of((first + which) * HD, HD)
            out_ref[k] = dot(hidden, wo_ref[:, pl.ds(at, HD)])


def weigh_kernel(*refs):
    blocks = landed(refs[:10])
    weight_ref, turned_ref, vw_ref, norm_ref = refs[10:]
    _, _, mine = rows_mine()
    norm = jnp.zeros((4 * OWN, HD), F32)
    for j, blk in enumerate(blocks):
        spread = [jnp.where(mine, weight_ref[g * SP + j : g * SP + j + 1, :], 0.0) for g in range(2)]
        norm += dot(two_parts(jnp.concatenate(spread, axis=0)), blk[:ROWS, :])
        value = blk[ROWS : 2 * ROWS, :].astype(F32)
        for g in range(2):
            k = g * SP + j
            vw_ref[j, :, g * HD : (g + 1) * HD] = (value * turned_ref[:, k : k + 1]).astype(BF)
    norm_ref[...] = (norm[: 2 * OWN] + norm[2 * OWN :]) * (HD ** -0.5)


def memory_kernel(*refs):
    blocks = landed(refs[:10])
    vw_ref, mem_ref = refs[10:]
    for s in range(OWN):
        at = slice(s * POS, (s + 1) * POS)
        keys = jnp.concatenate([blk[at, :] for blk in blocks], axis=0)
        values = vw_ref[:, at, :].reshape(SP * POS, 2 * HD)
        memory = (dot(keys, values, ((0,), (0,))) * (HD ** -0.5)).astype(BF)
        mem_ref[0, s] = memory[:, :HD]
        mem_ref[1, s] = memory[:, HD:]


def join_kernel(keep_ref, got_ref, *outs):
    for k, out in enumerate(outs):
        out[...] = keep_ref[k] + got_ref[k]


def sum_kernel(a_ref, b_ref, c_ref, d_ref, out_ref):
    out_ref[...] = ((a_ref[...] + b_ref[...]) + (c_ref[...] + d_ref[...])).astype(BF)


def shift(array, dz, dy):
    spots = [(z, y) for z in range(ROW) for y in range(ROW)]
    pairs = [(z * ROW + y, (z ^ dz) * ROW + (y + dy) % ROW) for z, y in spots]
    return lax.ppermute(array, "sp", pairs)


def across(array, axis, hop):
    size = lax.axis_size(axis)
    return lax.ppermute(array, axis, [(i, (i + hop) % size) for i in range(size)])


def step(prompt, w_key, w_value, w_in_gate, w_forget_gate, in_bias, forget_bias, query, w_out):
    hops = range(1, ROW)
    mirror, w, gates, later = project_near(
        prompt, w_key.reshape(D, HD), w_value.reshape(D, HD), w_in_gate.reshape(2, D), w_forget_gate.reshape(2, D)
    )
    mirror = shift(mirror, 3, 0)
    twin = run(second_kernel, block(ROW), (later, w, gates))
    twin = shift(twin, 1, 0)
    cross = run(third_kernel, (block(),) * ROW, (later, w, gates))
    cross = [cross[0]] + [shift(cross[k], 0, k) for k in hops]
    far = run(gather_kernel, block(ROW), cross, 4)
    far = shift(far, 2, 0)
    own = project_own(prompt, w, gates)
    own = [own[0]] + [shift(own[k], 0, k) for k in hops]
    side = run(pair_kernel, (block(2),) * 3, (mirror, twin), 4)
    side = [shift(blocks, 0, k) for k, blocks in zip(hops, side)]
    blocks = (*own, mirror, twin, *side, far)
    half = pltpu.VMEM((TPX, OWN, HD), F32)
    keep, send, weight, turned, stab = run(
        read_kernel,
        (half, half, pltpu.VMEM((2 * SP, HD), F32), pltpu.VMEM((HD, 2 * SP), F32),
         jax.ShapeDtypeStruct((2, 1, OWN), F32)),
        (*blocks, query.reshape(OWN, HD), w_out.reshape(HD, D), in_bias.reshape(1, 2), forget_bias.reshape(1, 2)),
    )
    got = across(send, "tp_1", 1)
    values, norm = run(
        weigh_kernel,
        (pltpu.VMEM((SP, ROWS, 2 * HD), BF), jax.ShapeDtypeStruct((2 * OWN, HD), F32)),
        (*blocks, weight, turned),
    )
    terms = run(join_kernel, (pltpu.VMEM((OWN, HD), F32),) * TPX, (keep, got), 4)
    terms = [terms[0]] + [across(terms[k], "tp_0", k) for k in range(1, TPX)]
    memory = run(memory_kernel, jax.ShapeDtypeStruct((2, OWN, HD, HD), BF), (*blocks, values))
    read = run(sum_kernel, jax.ShapeDtypeStruct((OWN, HD), BF), terms, 4)
    return (
        memory.reshape(2, OWN, 1, HD, HD),
        norm.reshape(2, OWN, 1, HD),
        stab.reshape(2, OWN, 1),
        read,
    )


def solution(mesh):
    torus = Mesh(
        mesh.devices.reshape(mesh.shape["gr"], mesh.shape["sp"], 4, 2), ("gr", "sp", "tp_0", "tp_1")
    )
    return jax.shard_map(
        step,
        mesh=torus,
        in_specs=(
            P("gr", "sp", None),
            P(None, TP, None),
            P(None, TP, None),
            P(None, None, TP),
            P(None, None, TP),
            P(None, TP),
            P(None, TP),
            P(("gr", "sp"), TP, None),
            P(TP, None, None),
        ),
        out_specs=(
            P(None, ("gr", "sp"), TP, None, None),
            P(None, ("gr", "sp"), TP, None),
            P(None, ("gr", "sp"), TP),
            P(("gr", "sp"), TP),
        ),
        check_vma=False,
    )
```
